32 devices in a mesh: ep: 8 (over z, y), tp: 4 (over x, core).
Axes of the slice: x: 2, y: 2, z: 4, core: 2. Of those that a mesh axis runs over, the one named last changes fastest.
Arguments:
- queries: bfloat16 [4096, 1536], P('ep', 'tp'), may hold values from -6 to 6
- keys: bfloat16 [4096, 1536], P('ep', 'tp'), may hold values from -6 to 6
- values: bfloat16 [4096, 1536], P('ep', 'tp'), may hold values from -6 to 6
- decay_gate_logits: float32 [4096, 12], P('ep', 'tp'), may hold values from -6 to 6
- correction_logits: bfloat16 [4096, 12], P('ep', 'tp'), may hold values from -6 to 6
- head_decay_speed: float32 [12], P('tp'), may hold values from 0 to 1
- position_log_decay: float32 [4096, 12], P('ep', 'tp'), may hold values from -1 to 0
- head_output_gain: float32 [128], replicated, may hold values from 0.1 to 1.9
- mixer_output_weight: bfloat16 [1536, 2048], P('tp'), may hold values from -0.15625 to 0.15625
- expert_input_tokens: bfloat16 [4096, 2048], P(('ep', 'tp')), may hold values from -6 to 6
- expert_norm_gain: float32 [2048], replicated, may hold values from 0.1 to 1.9
- routes: int32 [4096, 2], P(('ep', 'tp')), may hold values from 0 to 7, all different within a row; in each aligned block of 128 rows (0 to 127, 128 to 255, ...) at most 48 rows name the same one
- chosen_expert_weight: float32 [4096, 2], P(('ep', 'tp')), may hold values from 0.25 to 2.5
- routed_gate_weight: bfloat16 [8, 2048, 1024], P('ep', None, 'tp'), may hold values from -0.125 to 0.125
- routed_up_weight: bfloat16 [8, 2048, 1024], P('ep', None, 'tp'), may hold values from -0.125 to 0.125
- routed_down_weight: bfloat16 [8, 1024, 2048], P('ep', 'tp'), may hold values from -0.1875 to 0.1875
- common_gate_weight: bfloat16 [2048, 1024], P(None, 'tp'), may hold values from -0.125 to 0.125
- common_up_weight: bfloat16 [2048, 1024], P(None, 'tp'), may hold values from -0.125 to 0.125
- common_down_weight: bfloat16 [1024, 2048], P('tp'), may hold values from -0.1875 to 0.1875
Outputs:
- mixer_out: bfloat16 [4096, 2048], P(('ep', 'tp'))
- moe_out: bfloat16 [4096, 2048], P(('ep', 'tp'))
The draws below stay inside these ranges and needn't reach their ends.
Inputs may be any that keep to these rules, and one draw needn't show every extreme that they name: `routes`: each row names 2 different experts; the rows of one device name no expert more than 48 times, and some device names some expert exactly 48 times.
All inputs are finite; a program needn't handle non-finite values.
Results may differ from the reference program's by a relative error of at most 0.017.
Values may be sent and summed in bfloat16 or wider, within the bound.
A program may use at most 128 MiB of HBM per device.

```python
import math
import jax
import jax.numpy as jnp
import numpy as np
from jax import lax

D = 2048
HEADS = 12
HEAD_DIM = 128
BLOCK = 64
EXPERT_FF = 1024
SHARED_FF = 1024
TOP_K = 2
TOK_DEV = 128
EXPERTS = 8
CAP = 48
GROUP_ROWS = 512
TOKENS_A = 4096
TOKENS_B = 4096
N_EP = 8
N_TP = 4


def gentle_heads(key):
    order = jax.random.permutation(jax.random.fold_in(key, 41), HEADS)
    return order < max(1, HEADS // 4)


def draw_head_decay_speed(key, part):
    fast_share = 0.5
    gentle = gentle_heads(key)
    fast_head = (jax.random.uniform(jax.random.fold_in(key, 11), (HEADS,)) < fast_share) & jnp.logical_not(gentle)
    quick_rate = jax.random.uniform(jax.random.fold_in(key, 12), (HEADS,), jnp.float32, 0.02, 0.06)
    slow_rate = jax.random.uniform(jax.random.fold_in(key, 13), (HEADS,), jnp.float32, 0.5, 1.5) / TOKENS_A
    return jnp.where(fast_head, quick_rate, slow_rate).astype(jnp.float32)


def draw_correction_logits(key, part):
    gentle = gentle_heads(key)
    rough = jnp.clip(jax.random.normal(jax.random.fold_in(key, 42), (TOKENS_A, HEADS), jnp.float32), -6.0, 6.0)
    weak = jax.random.uniform(jax.random.fold_in(key, 43), (TOKENS_A, HEADS), jnp.float32, -6.0, -5.0)
    return jnp.where(gentle[None, :], weak, rough).astype(jnp.bfloat16)


def draw_position_log_decay(key, part):
    hit_draw = jax.random.uniform(jax.random.fold_in(key, 21), (TOKENS_A, HEADS))
    depth = jax.random.uniform(jax.random.fold_in(key, 22), (TOKENS_A, HEADS), jnp.float32, 0.5, 0.8)
    return jnp.where(hit_draw < 4.0 / TOKENS_A, jnp.log(depth), 0.0).astype(jnp.float32)


def draw_decay_gate_logits(key, part):
    lower_end = -1.5
    upper_end = 1.5
    base_draw = jax.random.normal(jax.random.fold_in(key, 31), (TOKENS_A, HEADS), jnp.float32)
    shifts = jax.random.uniform(jax.random.fold_in(key, 32), (TOKENS_A // GROUP_ROWS, 1), jnp.float32, lower_end, upper_end)
    owner = jnp.arange(TOKENS_A) // GROUP_ROWS
    return jnp.clip(base_draw + shifts[owner], -6.0, 6.0).astype(jnp.float32)


def block_scale(own_key, dims, split, low, top_value):
    def one(position, blocks):
        heights = jax.random.uniform(jax.random.fold_in(jax.random.fold_in(own_key, 6), position), (blocks,), jnp.float32, low / len(split), top_value / len(split))
        return jnp.repeat(jnp.exp(heights), dims[position] // blocks).reshape((-1,) + (1,) * (len(dims) - position - 1))

    gain = one(*split[0])
    for cut in split[1:]:
        gain = gain * one(*cut)
    return gain


def deal_out(key, own, number, rows, count, top, reach, skew):
    sequence = jax.random.permutation(key, count)
    heavy_load, common = portions_of(count, rows * top, reach, skew, True), portions_of(count, rows * top, reach, skew, False)
    places = jnp.arange(count)

    def named(sizes, offset_by):
        used = int((sizes > 0).sum())
        fixed = max(1, used // 4)
        moved = fixed + (places - fixed + offset_by * (used - fixed)) % max(1, count - fixed)
        return jnp.zeros((count,), jnp.int32).at[sequence[jnp.where(places < fixed, places, moved)]].set(jnp.asarray(sizes, jnp.int32))

    sizes = jnp.where(number % 4 == 0, named(heavy_load, number // 4), named(common, number - number // 4 - 1))
    mixed = jax.random.permutation(jax.random.fold_in(own, 3), count)
    giver, taker = mixed[0:count // 2 * 2:2], mixed[1:count // 2 * 2:2]
    margin = jnp.minimum(sizes[giver] - 1, reach - sizes[taker]) // 2
    margin = jnp.where((giver == sequence[0]) | (taker == sequence[0]) | (sizes[taker] == 0), 0, jnp.maximum(margin, 0))
    moved = jax.random.randint(jax.random.fold_in(own, 4), (count // 2,), 0, 1 << 20) % (margin + 1)
    sizes = sizes.at[giver].add(-moved).at[taker].add(moved)
    members = jnp.searchsorted(jnp.cumsum(sizes), jnp.arange(rows * top), side="right").astype(jnp.int32)
    grid = members.reshape(top, rows).T
    grid = grid[jax.random.permutation(jax.random.fold_in(own, 1), rows)]
    offset_by = jax.random.randint(jax.random.fold_in(own, 2), (rows, 1), 0, top)
    return jnp.take_along_axis(grid, (jnp.arange(top)[None, :] + offset_by) % top, axis=1)


def portions_of(amount, total, most, lean, full):
    loads = [(1 << 20) // math.isqrt(standing ** lean) + 1 for standing in range(1, amount + 1)]
    largest = most if full else min(most, max(-(-total // amount), total * loads[0] // sum(loads)))
    least = 1 if total - largest >= amount - 1 else 0
    counts, spare = [largest] + [least] * (amount - 1), total - largest - least * (amount - 1)
    while spare > 0:
        candidates = [i for i in range(1, amount) if counts[i] < largest] or [i for i in range(1, amount) if counts[i] < most]
        whole, budget = sum([loads[i] for i in candidates]), spare
        for i in candidates:
            addition = min(most - counts[i], max(1, budget * loads[i] // whole), spare)
            counts[i] = counts[i] + addition
            spare = spare - addition
    return np.array(counts)


def gaussian(rng, extent, deviation, bound, cuts=(), kind=jnp.bfloat16):
    array = jax.random.normal(rng, extent, jnp.float32) * deviation
    if len(cuts) > 0:
        array = block_scale(rng, extent, cuts, -0.22, 0.18) * array
    return jnp.clip(array, min=-bound, max=bound).astype(kind)


def setup_inputs(seed: int = 0) -> dict:
    seeds = jax.random.split(jax.random.key(seed), 20)
    queries = gaussian(seeds[0], (TOKENS_A, HEADS * HEAD_DIM), 1.0, 6.0, ((0, 8), (1, 4)))
    keys = gaussian(seeds[1], (TOKENS_A, HEADS * HEAD_DIM), 1.0, 6.0, ((0, 8), (1, 4)))
    values = gaussian(seeds[2], (TOKENS_A, HEADS * HEAD_DIM), 1.0, 6.0, ((0, 8), (1, 4)))
    decay_gate_logits = draw_decay_gate_logits(jax.random.fold_in(seeds[19], 71), 0)
    correction_logits = draw_correction_logits(jax.random.fold_in(seeds[19], 71), 0)
    head_decay_speed = draw_head_decay_speed(jax.random.fold_in(seeds[19], 71), 0)
    position_log_decay = draw_position_log_decay(jax.random.fold_in(seeds[19], 71), 0)
    head_output_gain = jnp.clip(1.0 + 0.18 * jax.random.normal(seeds[7], (HEAD_DIM,), jnp.float32), 0.1, 1.9)
    mixer_output_weight = gaussian(seeds[8], (HEADS * HEAD_DIM, D), (HEADS * HEAD_DIM) ** -0.5, 0.15625, ((0, 4),))
    expert_input_tokens = gaussian(seeds[9], (TOKENS_B, D), 1.0, 6.0, ((0, 32),))
    expert_norm_gain = jnp.clip(1.0 + 0.18 * jax.random.normal(seeds[10], (D,), jnp.float32), 0.1, 1.9)
    routes_keys = jax.random.split(jax.random.fold_in(seeds[11], 1), TOKENS_B // TOK_DEV)
    routes_turns = jax.random.permutation(jax.random.fold_in(seeds[11], 3), TOKENS_B // TOK_DEV)
    routes = jax.vmap(lambda own, number: deal_out(jax.random.fold_in(seeds[11], 2), own, number, TOK_DEV, EXPERTS, TOP_K, CAP, 2))(routes_keys, routes_turns).reshape((TOKENS_B, TOP_K))
    chosen_expert_weight = jnp.clip(jnp.exp(math.log(2.5) - 2.3025851 * jax.random.uniform(seeds[12], (TOKENS_B, TOP_K), jnp.float32) ** block_scale(seeds[12], (TOKENS_B, TOP_K), ((0, 32),), -0.2, 0.2)), 0.25, 2.5)
    routed_gate_weight = gaussian(seeds[13], (EXPERTS, D, EXPERT_FF), D ** -0.5, 0.125, ((0, 8), (2, 4)))
    routed_up_weight = gaussian(seeds[14], (EXPERTS, D, EXPERT_FF), D ** -0.5, 0.125, ((0, 8), (2, 4)))
    routed_down_weight = gaussian(seeds[15], (EXPERTS, EXPERT_FF, D), EXPERT_FF ** -0.5, 0.1875, ((0, 8), (1, 4)))
    common_gate_weight = gaussian(seeds[16], (D, SHARED_FF), D ** -0.5, 0.125, ((1, 4),))
    common_up_weight = gaussian(seeds[17], (D, SHARED_FF), D ** -0.5, 0.125, ((1, 4),))
    common_down_weight = gaussian(seeds[18], (SHARED_FF, D), SHARED_FF ** -0.5, 0.1875, ((0, 4),))
    return {"queries": queries, "keys": keys, "values": values, "decay_gate_logits": decay_gate_logits, "correction_logits": correction_logits, "head_decay_speed": head_decay_speed, "position_log_decay": position_log_decay, "head_output_gain": head_output_gain, "mixer_output_weight": mixer_output_weight, "expert_input_tokens": expert_input_tokens, "expert_norm_gain": expert_norm_gain, "routes": routes, "chosen_expert_weight": chosen_expert_weight, "routed_gate_weight": routed_gate_weight, "routed_up_weight": routed_up_weight, "routed_down_weight": routed_down_weight, "common_gate_weight": common_gate_weight, "common_up_weight": common_up_weight, "common_down_weight": common_down_weight}


EPS = 1e-06
HIGH = lax.Precision.HIGHEST

def separate_heads(source, number_of_heads):
    row_count = source.shape[0]
    shaped = source.astype(jnp.float32).reshape(row_count // BLOCK, BLOCK, number_of_heads, source.shape[1] // number_of_heads)
    return jnp.transpose(shaped, (2, 0, 1, 3))

def block_contributions(queries, keys, values, decay_gate_logits, correction_logits, head_decay_speed, position_log_decay):
    number_of_heads = decay_gate_logits.shape[1]
    q_heads = separate_heads(queries, number_of_heads)
    k_heads = separate_heads(keys, number_of_heads)
    v_heads = separate_heads(values, number_of_heads)
    q_heads = q_heads * lax.rsqrt(lax.optimization_barrier(jnp.sum(q_heads * q_heads, axis=-1, keepdims=True)) + EPS) * q_heads.shape[-1] ** (-0.5)
    k_heads = k_heads * lax.rsqrt(lax.optimization_barrier(jnp.sum(k_heads * k_heads, axis=-1, keepdims=True)) + EPS)
    decay_speed_column = head_decay_speed.astype(jnp.float32)[:, None, None]
    log_gate_value = -decay_speed_column * jax.nn.softplus(separate_heads(decay_gate_logits, number_of_heads)[..., 0]) + separate_heads(position_log_decay, number_of_heads)[..., 0]
    beta_gate = jax.nn.sigmoid(separate_heads(correction_logits, number_of_heads)[..., 0])
    cum_gate = jnp.cumsum(log_gate_value, axis=-1)
    positions = jnp.arange(log_gate_value.shape[-1])
    causal = positions[:, None] >= positions[None, :]
    strict = positions[:, None] > positions[None, :]
    decay_mat = jnp.exp(jnp.where(causal, cum_gate[..., :, None] - cum_gate[..., None, :], -jnp.inf))
    keyed = k_heads * beta_gate[..., None]
    lower_part = jnp.where(strict, jnp.einsum('hnld,hnsd->hnls', keyed, k_heads, precision=HIGH) * decay_mat, 0.0)
    right_side = jnp.concatenate([v_heads * beta_gate[..., None], keyed * jnp.exp(cum_gate)[..., None]], axis=-1)
    solved = lax.linalg.triangular_solve(lower_part, right_side, left_side=True, lower=True, unit_diagonal=True)
    value_width = v_heads.shape[-1]
    new_values = solved[..., :value_width]
    corr_weights = solved[..., value_width:]
    scores = jnp.einsum('hnld,hnsd->hnls', q_heads, k_heads, precision=HIGH) * decay_mat
    carried_keys = k_heads * jnp.exp(cum_gate[..., -1:] - cum_gate)[..., None]
    q_scaled = q_heads * jnp.exp(cum_gate)[..., None]
    return (q_scaled, cum_gate[..., -1], scores, new_values, corr_weights, carried_keys)

def advance(state, inputs):
    q_blk, last_blk, score_blk, value_blk, weight_blk, carry_blk = inputs
    corrected = value_blk - jnp.einsum('hld,hde->hle', weight_blk, state, precision=HIGH)
    output = jnp.einsum('hld,hde->hle', q_blk, state, precision=HIGH) + jnp.einsum('hls,hse->hle', score_blk, corrected, precision=HIGH)
    state = state * jnp.exp(last_blk)[:, None, None] + jnp.einsum('hld,hle->hde', carry_blk, corrected, precision=HIGH)
    return (state, output)

def finish_heads(outputs, head_output_gain):
    normed = outputs * lax.rsqrt(lax.optimization_barrier(jnp.mean(outputs * outputs, axis=-1, keepdims=True)) + EPS) * head_output_gain.astype(jnp.float32)
    block_count, number_of_heads, span_len, value_width = normed.shape
    normed = jnp.transpose(normed, (0, 2, 1, 3)).reshape(block_count * span_len, number_of_heads * value_width)
    return normed.astype(jnp.bfloat16)

def norm_rows(expert_input_tokens, expert_norm_gain):
    rows_f = expert_input_tokens.astype(jnp.float32)
    scaled = rows_f * lax.rsqrt(lax.optimization_barrier(jnp.mean(rows_f * rows_f, axis=-1, keepdims=True)) + EPS) * expert_norm_gain.astype(jnp.float32)
    return scaled.astype(jnp.bfloat16)

def gated_hidden(rows_in, w_gate, w_up):
    gate_val = jnp.dot(rows_in.astype(jnp.float32), w_gate.astype(jnp.float32), preferred_element_type=jnp.float32)
    up_val = jnp.dot(rows_in.astype(jnp.float32), w_up.astype(jnp.float32), preferred_element_type=jnp.float32)
    return (jax.nn.silu(gate_val) * up_val).astype(jnp.bfloat16)

def mix_routes(chosen_expert_weight, copies, shared):
    running = shared
    for slot_k in range(chosen_expert_weight.shape[1]):
        running = running + chosen_expert_weight[:, slot_k:slot_k + 1] * copies[:, slot_k].astype(jnp.float32)
    return running.astype(jnp.bfloat16)

def reference(queries, keys, values, decay_gate_logits, correction_logits, head_decay_speed, position_log_decay, head_output_gain, mixer_output_weight, expert_input_tokens, expert_norm_gain, routes, chosen_expert_weight, routed_gate_weight, routed_up_weight, routed_down_weight, common_gate_weight, common_up_weight, common_down_weight):
    summands = block_contributions(queries, keys, values, decay_gate_logits, correction_logits, head_decay_speed, position_log_decay)
    number_of_heads = summands[0].shape[0]
    key_width = summands[0].shape[-1]
    value_width = summands[3].shape[-1]
    inputs = tuple((jnp.moveaxis(item, 1, 0) for item in summands))
    zero_state = jnp.zeros((number_of_heads, key_width, value_width), jnp.float32)
    _, outputs = lax.scan(advance, zero_state, inputs)
    normed = finish_heads(outputs, head_output_gain)
    part_width = HEADS // N_TP * HEAD_DIM
    running = jnp.zeros((normed.shape[0], mixer_output_weight.shape[1]), jnp.float32)
    for member in range(N_TP):
        part_sum = jnp.dot(normed[:, member * part_width:(member + 1) * part_width].astype(jnp.float32), mixer_output_weight[member * part_width:(member + 1) * part_width].astype(jnp.float32), preferred_element_type=jnp.float32).astype(jnp.bfloat16)
        running = running + part_sum.astype(jnp.float32)
    mixer_out = running.astype(jnp.bfloat16)
    normed_in = norm_rows(expert_input_tokens, expert_norm_gain)
    token_count, top_k = routes.shape
    flat_routes = routes.reshape(-1).astype(jnp.int32)
    copy_count = flat_routes.shape[0]
    row_limit = N_EP * N_TP * CAP
    unit_width = EXPERT_FF // N_TP

    def one_expert(results, expert):
        chosen = flat_routes == expert
        before = jnp.cumsum(chosen.astype(jnp.int32)) - 1
        target = jnp.where(chosen, before, row_limit).astype(jnp.int32)
        owners = jnp.zeros((row_limit + 1,), jnp.int32).at[target].set(jnp.arange(copy_count, dtype=jnp.int32))
        in_use = jnp.arange(row_limit, dtype=jnp.int32) < jnp.sum(chosen.astype(jnp.int32))
        picked = owners[:row_limit]
        picked_rows = normed_in[(picked // top_k).astype(jnp.int32)]
        hidden = gated_hidden(picked_rows, routed_gate_weight[expert], routed_up_weight[expert])
        running_e = jnp.zeros((row_limit, normed_in.shape[1]), jnp.float32)
        for member in range(N_TP):
            part_sum = jnp.dot(hidden[:, member * unit_width:(member + 1) * unit_width].astype(jnp.float32), routed_down_weight[expert, member * unit_width:(member + 1) * unit_width].astype(jnp.float32), preferred_element_type=jnp.float32).astype(jnp.bfloat16)
            running_e = running_e + part_sum.astype(jnp.float32)
        result = running_e.astype(jnp.bfloat16)
        spots = jnp.where(in_use, picked, copy_count).astype(jnp.int32)
        results = results.at[spots].set(result, mode='drop')
        return (results, None)
    start_rows = jnp.zeros((copy_count, normed_in.shape[1]), jnp.bfloat16)
    copies, _ = lax.scan(one_expert, start_rows, jnp.arange(EXPERTS, dtype=jnp.int32))
    shared_hidden = gated_hidden(normed_in, common_gate_weight, common_up_weight)
    shared_width = SHARED_FF // N_TP
    shared = jnp.zeros((token_count, normed_in.shape[1]), jnp.float32)
    for member in range(N_TP):
        part_sum = jnp.dot(shared_hidden[:, member * shared_width:(member + 1) * shared_width].astype(jnp.float32), common_down_weight[member * shared_width:(member + 1) * shared_width].astype(jnp.float32), preferred_element_type=jnp.float32).astype(jnp.bfloat16)
        shared = shared + part_sum.astype(jnp.float32)
    moe_out = mix_routes(chosen_expert_weight, copies.reshape(token_count, top_k, -1), shared)
    return (mixer_out, moe_out)
```

```python
import functools

import jax
import jax.numpy as jnp
from jax import lax
from jax.experimental import pallas as pl
from jax.experimental.pallas import tpu as pltpu
from jax.sharding import PartitionSpec as P


EPS = 1e-06


SPAN = 64


def halves(x):
    high = x.astype(jnp.bfloat16)
    return high, (x - high.astype(jnp.float32)).astype(jnp.bfloat16)


def product(left, right, numbers):
    left_high, left_low = halves(left)
    right_high, right_low = halves(right)

    def dot(x, y):
        return lax.dot_general(x, y, numbers, preferred_element_type=jnp.float32)

    return dot(left_high, right_high) + (dot(left_high, right_low) + dot(left_low, right_high))


def bmm(left, right, dims):
    return product(left, right, (dims, ((0,), (0,))))


def mm(left, right):
    return product(left, right, (((1,), (0,)), ((), ())))


def unit_lower_inverse(lower, rows, cols):
    inverse = jnp.where(rows == cols, 1.0, 0.0) - jnp.where(
        ((rows >> 1) == (cols >> 1)), lower, 0.0
    )
    level = 1
    while (1 << level) < SPAN:
        below = ((rows >> (level + 1)) == (cols >> (level + 1))) & (
            (rows >> level) != (cols >> level)
        )
        part = jnp.where(below, lower, 0.0)
        inverse = inverse - bmm(bmm(inverse, part, ((2,), (1,))), inverse, ((2,), (1,)))
        level += 1
    return inverse


def local_kernel(q_ref, k_ref, v_ref, ccol_ref, crow_ref, bcol_ref, g_ref, z_ref, total_ref):
    width = q_ref.shape[1]
    count = q_ref.shape[0] // SPAN
    shape = (count, SPAN, width)
    q = q_ref[...].astype(jnp.float32)
    k = k_ref[...].astype(jnp.float32)
    v = v_ref[...].astype(jnp.float32).reshape(shape)
    q = q * lax.rsqrt(jnp.sum(q * q, axis=-1, keepdims=True) + EPS) * width ** (-0.5)
    k = k * lax.rsqrt(jnp.sum(k * k, axis=-1, keepdims=True) + EPS)
    q = q.reshape(shape)
    k = k.reshape(shape)
    ccol = ccol_ref[0].reshape(count, SPAN, 1)
    crow = crow_ref[0]
    bcol = bcol_ref[0].reshape(count, SPAN, 1)
    rows = lax.broadcasted_iota(jnp.int32, (count, SPAN, SPAN), 1)
    cols = lax.broadcasted_iota(jnp.int32, (count, SPAN, SPAN), 2)
    decay = jnp.exp(jnp.where(rows >= cols, ccol - crow, -jnp.inf))
    keyed = k * bcol
    lower = jnp.where(rows > cols, bmm(keyed, k, ((2,), (2,))) * decay, 0.0)
    inverse = unit_lower_inverse(lower, rows, cols)
    grown = jnp.exp(ccol)
    solved = bmm(
        inverse, jnp.concatenate([keyed * grown, v * bcol], axis=-1), ((2,), (1,))
    )
    scores = bmm(q, k, ((2,), (2,))) * decay
    q_scaled = q * grown
    last = ccol[:, SPAN - 1 :, :]
    carried = k * jnp.exp(last - ccol)
    mixed = bmm(scores, solved, ((2,), (1,)))
    readout = q_scaled - mixed[:, :, :width]
    eye_r = lax.broadcasted_iota(jnp.int32, (width, width), 0)
    eye_c = lax.broadcasted_iota(jnp.int32, (width, width), 1)
    eye = jnp.where(eye_r == eye_c, 1.0, 0.0)
    state = jnp.concatenate([eye, jnp.zeros_like(eye)], axis=1)
    for n in range(count):
        seen = mm(readout[n], state)
        g_ref[0, n * SPAN : (n + 1) * SPAN, :] = seen[:, :width]
        z_ref[0, n * SPAN : (n + 1) * SPAN, :] = seen[:, width:] + mixed[n][:, width:]
        both = mm(carried[n].T, solved[n])
        trans = jnp.exp(last[n]) * eye - both[:, :width]
        state = mm(trans, state)
        state = jnp.concatenate([state[:, :width], state[:, width:] + both[:, width:]], axis=1)
    total_ref[0] = state.astype(jnp.bfloat16)


def finish_kernel(place_ref, gathered_ref, g_ref, z_ref, gain_ref, out_ref):
    width = g_ref.shape[2]

    def one(turn, state):
        both = gathered_ref[turn, 0].astype(jnp.float32)
        return mm(both[:, :width], state) + both[:, width:]

    state = lax.fori_loop(0, place_ref[0], one, jnp.zeros((width, width), jnp.float32))
    out = mm(g_ref[0], state) + z_ref[0]
    out = out * lax.rsqrt(jnp.mean(out * out, axis=-1, keepdims=True) + EPS) * gain_ref[...]
    out_ref[...] = out.astype(jnp.bfloat16)


def token_mixer_heads(
    queries,
    keys,
    values,
    decay_gate_logits,
    correction_logits,
    head_decay_speed,
    position_log_decay,
    head_output_gain,
):
    heads = decay_gate_logits.shape[1]
    length = queries.shape[0]
    width = queries.shape[1] // heads
    count = length // SPAN
    log_gate = -head_decay_speed * jax.nn.softplus(decay_gate_logits) + position_log_decay
    log_gate = log_gate.T.reshape(heads, count, SPAN)
    at = jnp.arange(SPAN)
    cum = jnp.sum(
        jnp.where(at[:, None] >= at[None, :], log_gate[:, :, None, :], 0.0), axis=-1
    )
    beta = jax.nn.sigmoid(correction_logits.astype(jnp.float32)).T.reshape(heads, length, 1)
    by_head = pl.BlockSpec((length, width), lambda h: (0, h))
    column = pl.BlockSpec((1, length, 1), lambda h: (h, 0, 0))
    whole = pl.BlockSpec((1, length, width), lambda h: (h, 0, 0))
    local_call = pl.pallas_call(
        local_kernel,
        grid=(heads,),
        in_specs=[
            by_head,
            by_head,
            by_head,
            column,
            pl.BlockSpec((1, count, 1, SPAN), lambda h: (h, 0, 0, 0)),
            column,
        ],
        out_specs=[whole, whole, pl.BlockSpec((1, width, 2 * width), lambda h: (h, 0, 0))],
        out_shape=[
            jax.ShapeDtypeStruct((heads, length, width), jnp.float32),
            jax.ShapeDtypeStruct((heads, length, width), jnp.float32),
            jax.ShapeDtypeStruct((heads, width, 2 * width), jnp.bfloat16),
        ],
        cost_estimate=pl.CostEstimate(
            flops=3_000_000_000, bytes_accessed=4_000_000, transcendentals=200_000
        ),
    )
    readout, local_out, total = local_call(
        queries,
        keys,
        values,
        cum.reshape(heads, length, 1),
        cum.reshape(heads, count, 1, SPAN),
        beta,
    )
    gathered = lax.all_gather(total, "ep")
    place = lax.axis_index("ep").astype(jnp.int32).reshape(1)
    devices = gathered.shape[0]
    return pl.pallas_call(
        finish_kernel,
        grid=(heads,),
        in_specs=[
            pl.BlockSpec(memory_space=pltpu.SMEM),
            pl.BlockSpec((devices, 1, width, 2 * width), lambda h: (0, h, 0, 0)),
            whole,
            whole,
            pl.BlockSpec((1, width), lambda h: (0, 0)),
        ],
        out_specs=by_head,
        out_shape=jax.ShapeDtypeStruct((length, heads * width), jnp.bfloat16),
        cost_estimate=pl.CostEstimate(
            flops=500_000_000, bytes_accessed=4_000_000, transcendentals=2_000
        ),
    )(place, gathered, readout, local_out, head_output_gain.reshape(1, width))


def norm_rows(expert_input_tokens, expert_norm_gain):
    rows_f = expert_input_tokens.astype(jnp.float32)
    scaled = (
        rows_f
        * lax.rsqrt(jnp.mean(rows_f * rows_f, axis=-1, keepdims=True) + EPS)
        * expert_norm_gain
    )
    return scaled.astype(jnp.bfloat16)


def gated_hidden(rows_in, w_gate, w_up):
    gate_val = jnp.dot(rows_in, w_gate, preferred_element_type=jnp.float32)
    up_val = jnp.dot(rows_in, w_up, preferred_element_type=jnp.float32)
    return (jax.nn.silu(gate_val) * up_val).astype(jnp.bfloat16)


def slot_layout(routes, capacity):
    flat = routes.reshape(-1)
    at = jnp.arange(flat.shape[0], dtype=jnp.int32)
    same = (flat[:, None] == flat[None, :]) & (at[None, :] < at[:, None])
    before = jnp.sum(same.astype(jnp.int32), axis=1)
    return (flat * capacity + before).reshape(routes.shape)


def plain_shards(
    queries,
    keys,
    values,
    decay_gate_logits,
    correction_logits,
    head_decay_speed,
    position_log_decay,
    head_output_gain,
    mixer_output_weight,
    expert_input_tokens,
    expert_norm_gain,
    routes,
    chosen_expert_weight,
    routed_gate_weight,
    routed_up_weight,
    routed_down_weight,
    common_gate_weight,
    common_up_weight,
    common_down_weight,
):
    normed = token_mixer_heads(
        queries,
        keys,
        values,
        decay_gate_logits,
        correction_logits,
        head_decay_speed,
        position_log_decay,
        head_output_gain,
    )
    mixer_out = lax.psum_scatter(
        jnp.dot(normed, mixer_output_weight, preferred_element_type=jnp.float32).astype(
            jnp.bfloat16
        ),
        "tp",
        scatter_dimension=0,
        tiled=True,
    )
    normed_in = norm_rows(expert_input_tokens, expert_norm_gain)
    tokens_own, top_k = routes.shape
    model_width = expert_input_tokens.shape[1]
    experts = lax.axis_size("ep")
    capacity = 3 * tokens_own * top_k // (2 * experts)
    slot_count = experts * capacity
    slots = slot_layout(routes, capacity)
    numbers = jnp.arange(slot_count, dtype=jnp.int32)
    sends = sum(
        (slots[None, :, k] == numbers[:, None]).astype(jnp.bfloat16) for k in range(top_k)
    )
    outgoing = jnp.dot(sends, normed_in, preferred_element_type=jnp.float32).astype(
        jnp.bfloat16
    )
    arrived = lax.all_to_all(
        outgoing.reshape(experts, capacity, model_width),
        "ep",
        split_axis=0,
        concat_axis=0,
        tiled=True,
    ).reshape(slot_count, model_width)
    gate_all = lax.all_gather(routed_gate_weight[0], "tp")
    up_all = lax.all_gather(routed_up_weight[0], "tp")
    down_all = lax.all_gather(routed_down_weight[0], "tp", axis=0, tiled=True)
    hidden = jnp.concatenate(
        [gated_hidden(arrived, gate_all[t], up_all[t]) for t in range(gate_all.shape[0])],
        axis=1,
    )
    slot_sums = jnp.dot(hidden, down_all, preferred_element_type=jnp.float32).astype(
        jnp.bfloat16
    )
    returned = lax.all_to_all(
        slot_sums.reshape(experts, capacity, model_width),
        "ep",
        split_axis=0,
        concat_axis=0,
        tiled=True,
    ).reshape(slot_count, model_width)
    shared_hidden = gated_hidden(
        lax.all_gather(normed_in, "tp", axis=0, tiled=True), common_gate_weight, common_up_weight
    )
    shared = lax.psum_scatter(
        jnp.dot(shared_hidden, common_down_weight, preferred_element_type=jnp.float32).astype(
            jnp.bfloat16
        ),
        "tp",
        scatter_dimension=0,
        tiled=True,
    ).astype(jnp.float32)
    weights = sum(
        jnp.where(
            slots[:, k : k + 1] == numbers[None, :], chosen_expert_weight[:, k : k + 1], 0.0
        )
        for k in range(top_k)
    )
    coarse = weights.astype(jnp.bfloat16)
    fine = (weights - coarse.astype(jnp.float32)).astype(jnp.bfloat16)
    routed = jnp.dot(coarse, returned, preferred_element_type=jnp.float32) + jnp.dot(
        fine, returned, preferred_element_type=jnp.float32
    )
    moe_out = (shared + routed).astype(jnp.bfloat16)
    return (mixer_out, moe_out)


MESH = pl.DeviceIdType.MESH
CUTS = 4
OWN, CORE, CROSS, FAR = range(4)


def scaled_rows(rows, gain):
    rows_f = rows.astype(jnp.float32)
    norm = lax.rsqrt(jnp.mean(rows_f * rows_f, axis=-1, keepdims=True) + EPS)
    return (rows_f * norm * gain).astype(jnp.bfloat16)


def silu_product(gate_val, up_val):
    return (gate_val / (1.0 + jnp.exp(-gate_val)) * up_val).astype(jnp.bfloat16)


def fused_kernel(
    devices,
    q_ref,
    k_ref,
    v_ref,
    decay_ref,
    correct_ref,
    speed_ref,
    log_ref,
    head_gain_ref,
    tok_ref,
    gain_ref,
    sends_ref,
    coarse_ref,
    fine_ref,
    mixw_hbm,
    rg_hbm,
    ru_hbm,
    rd_hbm,
    cg_hbm,
    cu_hbm,
    cd_hbm,
    mix_ref,
    moe_ref,
    wg,
    wu,
    wd,
    cg,
    cu,
    cd,
    mw,
    toks,
    outgoing,
    arrived,
    hid,
    slot_out,
    returned,
    sh_part,
    sh_in,
    sh_cross,
    sh_far,
    mx_part,
    mx_in,
    mx_cross,
    mx_far,
    ccol_s,
    crow_s,
    bcol_s,
    gs,
    zs,
    tot,
    tot_bf,
    pair_in,
    pair_tot,
    s_in,
    s_out,
    state_s,
    normed,
    local_sem,
    w_send,
    w_recv,
    d_send,
    d_recv,
    r_send,
    r_recv,
    r_local,
    rs_send,
    rs_recv,
    c_send,
    c_recv,
):
    e = lax.axis_index("ep")
    t = lax.axis_index("tp")
    heads = decay_ref.shape[1]
    width = q_ref.shape[1] // heads
    length = q_ref.shape[0]
    count = length // SPAN
    tokens, model = tok_ref.shape
    capacity = arrived.shape[1]
    slots = devices * capacity
    unit = wg.shape[2]
    cut = model // CUTS
    core_t = t + 1 - 2 * (t % 2)
    core = (e, core_t)
    cross = (e, (t + 2) % 4)

    def remote(src, dst, send, recv, peer):
        return pltpu.make_async_remote_copy(
            src_ref=src,
            dst_ref=dst,
            send_sem=send,
            recv_sem=recv,
            device_id=peer,
            device_id_type=MESH,
        )

    barrier = pltpu.get_barrier_semaphore()
    for o in range(1, devices):
        pl.semaphore_signal(
            barrier, inc=1, device_id=((e + o) % devices, t), device_id_type=MESH
        )
    for o in range(1, 4):
        pl.semaphore_signal(barrier, inc=1, device_id=(e, (t + o) % 4), device_id_type=MESH)
    pl.semaphore_wait(barrier, devices + 2)

    def cols(j):
        return pl.ds(pl.multiple_of(j * cut, cut), cut)

    def spread(i, src, place):
        remote(src, place(CROSS), w_send.at[i, 0], w_recv.at[i, 0], cross).start()
        remote(src, place(CORE), w_send.at[i, 1], w_recv.at[i, 1], core).start()

    def forward(i, place):
        remote(place(CROSS), place(CROSS), w_send.at[i, 0], w_recv.at[i, 0], cross).wait_recv()
        remote(place(CROSS), place(FAR), w_send.at[i, 2], w_recv.at[i, 2], core).start()

    def take(i, place):
        remote(place(CORE), place(CORE), w_send.at[i, 1], w_recv.at[i, 1], core).wait_recv()
        remote(place(FAR), place(FAR), w_send.at[i, 2], w_recv.at[i, 2], core).wait_recv()

    def sent(i, place):
        remote(place(CROSS), place(CROSS), w_send.at[i, 0], w_recv.at[i, 0], cross).wait_send()
        remote(place(CORE), place(CORE), w_send.at[i, 1], w_recv.at[i, 1], core).wait_send()
        remote(place(FAR), place(FAR), w_send.at[i, 2], w_recv.at[i, 2], core).wait_send()

    def tok_at(r):
        return toks.at[r]

    def gate_at(r):
        return wg.at[r]

    def up_at(r):
        return wu.at[r]

    def down_at(j):
        return lambda r: wd.at[r, :, cols(j)]

    spread(0, tok_ref, tok_at)
    spread(1, rg_hbm, gate_at)
    spread(2, ru_hbm, up_at)
    for j in range(CUTS):
        remote(
            rd_hbm.at[:, cols(j)], wd.at[CROSS, :, cols(j)], w_send.at[3 + j, 0], w_recv.at[3 + j, 0], cross
        ).start()
        remote(
            rd_hbm.at[:, cols(j)], wd.at[CORE, :, cols(j)], w_send.at[3 + j, 1], w_recv.at[3 + j, 1], core
        ).start()

    locals_ = [
        pltpu.make_async_copy(src, dst, local_sem.at[n])
        for n, (src, dst) in enumerate(
            (
                (cg_hbm, cg),
                (cu_hbm, cu),
                (cd_hbm, cd),
                (rg_hbm, wg.at[OWN]),
                (ru_hbm, wu.at[OWN]),
                (rd_hbm, wd.at[OWN]),
                (mixw_hbm, mw),
            )
        )
    ]
    for copy in locals_:
        copy.start()

    toks[OWN] = scaled_rows(tok_ref[...], gain_ref[...])
    outgoing[...] = (
        jnp.dot(sends_ref[...], toks[OWN], preferred_element_type=jnp.float32)
        .astype(jnp.bfloat16)
        .reshape(outgoing.shape)
    )

    softplus = jnp.maximum(decay_ref[...], 0.0) + jnp.log1p(jnp.exp(-jnp.abs(decay_ref[...])))
    log_gate = -speed_ref[...] * softplus + log_ref[...]
    beta = 1.0 / (1.0 + jnp.exp(-correct_ref[...].astype(jnp.float32)))
    rows = lax.broadcasted_iota(jnp.int32, (count, SPAN, SPAN), 1)
    cols_at = lax.broadcasted_iota(jnp.int32, (count, SPAN, SPAN), 2)
    for h in range(heads):
        one = log_gate[:, h : h + 1].reshape(count, SPAN, 1)
        crow = jnp.sum(jnp.where(rows <= cols_at, one, 0.0), axis=1, keepdims=True)
        crow_s[h] = crow
        ccol_s[h] = jnp.sum(jnp.where(rows == cols_at, crow, 0.0), axis=2, keepdims=True)
        bcol_s[h] = beta[:, h : h + 1].reshape(count, SPAN, 1)

    for o in range(1, devices):
        peer = (e + o) % devices
        remote(
            outgoing.at[peer], arrived.at[e], d_send.at[o - 1], d_recv.at[o - 1], (peer, t)
        ).start()
    own_rows = pltpu.make_async_copy(outgoing.at[e], arrived.at[e], local_sem.at[7])
    own_rows.start()

    def local_head(h, carry):
        at = pl.ds(pl.multiple_of(h * width, width), width)
        shape = (count, SPAN, width)
        q = q_ref[:, at].astype(jnp.float32)
        k = k_ref[:, at].astype(jnp.float32)
        v = v_ref[:, at].astype(jnp.float32).reshape(shape)
        q = q * lax.rsqrt(jnp.sum(q * q, axis=-1, keepdims=True) + EPS) * width ** (-0.5)
        k = k * lax.rsqrt(jnp.sum(k * k, axis=-1, keepdims=True) + EPS)
        q = q.reshape(shape)
        k = k.reshape(shape)
        ccol = ccol_s[h]
        crow = crow_s[h]
        bcol = bcol_s[h]
        decay = jnp.exp(jnp.where(rows >= cols_at, ccol - crow, -jnp.inf))
        keyed = k * bcol
        lower = jnp.where(rows > cols_at, bmm(keyed, k, ((2,), (2,))) * decay, 0.0)
        inverse = unit_lower_inverse(lower, rows, cols_at)
        grown = jnp.exp(ccol)
        solved = bmm(
            inverse, jnp.concatenate([keyed * grown, v * bcol], axis=-1), ((2,), (1,))
        )
        scores = bmm(q, k, ((2,), (2,))) * decay
        q_scaled = q * grown
        last = ccol[:, SPAN - 1 :, :]
        carried = k * jnp.exp(last - ccol)
        mixed = bmm(scores, solved, ((2,), (1,)))
        readout = q_scaled - mixed[:, :, :width]
        eye_r = lax.broadcasted_iota(jnp.int32, (width, width), 0)
        eye_c = lax.broadcasted_iota(jnp.int32, (width, width), 1)
        eye = jnp.where(eye_r == eye_c, 1.0, 0.0)
        state = jnp.concatenate([eye, jnp.zeros_like(eye)], axis=1)
        for n in range(count):
            seen = mm(readout[n], state)
            gs[h, n * SPAN : (n + 1) * SPAN, :] = seen[:, :width]
            zs[h, n * SPAN : (n + 1) * SPAN, :] = seen[:, width:] + mixed[n][:, width:]
            both = mm(carried[n].T, solved[n])
            trans = jnp.exp(last[n]) * eye - both[:, :width]
            state = mm(trans, state)
            state = jnp.concatenate([state[:, :width], state[:, width:] + both[:, width:]], axis=1)
        tot[h] = state
        tot_bf[h] = state.astype(jnp.bfloat16)
        return carry

    lax.fori_loop(0, heads, local_head, 0)

    odd = e % 2
    pair = e // 2
    pairs = devices // 2
    forward(0, tok_at)
    to_odd = remote(tot_bf, pair_in, c_send.at[0], c_recv.at[0], ((e + 1) % devices, t))

    @pl.when(odd == 0)
    def _():
        to_odd.start()

    take(0, tok_at)
    for n in range(3):
        locals_[n].wait()
    gain = gain_ref[...]
    for r in (CORE, CROSS, FAR):
        if r == CROSS:
            remote(tok_at(FAR), tok_at(FAR), w_send.at[0, 2], w_recv.at[0, 2], core).wait_send()
        toks[r] = scaled_rows(toks[r], gain)
    x_all = toks[...].reshape(4 * tokens, model)
    sh_hid = silu_product(
        jnp.dot(x_all, cg[...], preferred_element_type=jnp.float32),
        jnp.dot(x_all, cu[...], preferred_element_type=jnp.float32),
    )
    sh_part[...] = (
        jnp.dot(sh_hid, cd[...], preferred_element_type=jnp.float32)
        .astype(jnp.bfloat16)
        .reshape(sh_part.shape)
    )

    def reduce_start(n, part, inbox):
        for i, r in enumerate((FAR, CORE)):
            remote(
                part.at[r], inbox.at[1 - i], rs_send.at[n, i], rs_recv.at[n, i], core
            ).start()

    def reduce_cross(n, part, inbox, out, far):
        remote(part.at[FAR], inbox.at[1], rs_send.at[n, 0], rs_recv.at[n, 0], core).wait_recv()
        out[...] = (part[CROSS].astype(jnp.float32) + inbox[1].astype(jnp.float32)).astype(
            jnp.bfloat16
        )
        remote(out, far, rs_send.at[n, 2], rs_recv.at[n, 2], cross).start()

    def reduce_finish(n, part, inbox, out, far):
        remote(part.at[CORE], inbox.at[0], rs_send.at[n, 1], rs_recv.at[n, 1], core).wait_recv()
        remote(out, far, rs_send.at[n, 2], rs_recv.at[n, 2], cross).wait_recv()
        return (
            part[OWN].astype(jnp.float32)
            + inbox[0].astype(jnp.float32)
            + far[...].astype(jnp.float32)
        )

    def reduce_sent(n, part, inbox, out, far):
        remote(part.at[FAR], inbox.at[1], rs_send.at[n, 0], rs_recv.at[n, 0], core).wait_send()
        remote(part.at[CORE], inbox.at[0], rs_send.at[n, 1], rs_recv.at[n, 1], core).wait_send()
        remote(out, far, rs_send.at[n, 2], rs_recv.at[n, 2], cross).wait_send()

    reduce_start(0, sh_part, sh_in)

    @pl.when(odd == 1)
    def _():
        remote(tot_bf, pair_in, c_send.at[0], c_recv.at[0], ((e + 1) % devices, t)).wait_recv()
        for h in range(heads):
            both = mm(tot[h][:, :width], pair_in[h].astype(jnp.float32))
            pair_tot[h, :, :width] = both[:, :width]
            pair_tot[h, :, width:] = both[:, width:] + tot[h][:, width:]

    reduce_cross(0, sh_part, sh_in, sh_cross, sh_far)

    forward(1, gate_at)
    for n in range(3, 6):
        locals_[n].wait()
    for i in (1, 2):
        remote(
            wg.at[CORE], wg.at[CORE], w_send.at[i, 1], w_recv.at[i, 1], core
        ).wait_recv()
    own_rows.wait()
    for o in range(1, devices):
        remote(
            outgoing.at[e], arrived.at[e], d_send.at[o - 1], d_recv.at[o - 1], (e, core_t)
        ).wait_recv()

    def hidden_of(r, carry):
        rows_in = arrived[...].reshape(slots, model)
        hid[r] = silu_product(
            jnp.dot(rows_in, wg[r], preferred_element_type=jnp.float32),
            jnp.dot(rows_in, wu[r], preferred_element_type=jnp.float32),
        )
        return carry

    lax.fori_loop(OWN, CORE + 1, hidden_of, 0)

    next_odd = (e + 2) % devices
    next_even = (e + 1) % devices

    @pl.when(pair > 0)
    def _():
        remote(s_out, s_in, c_send.at[1], c_recv.at[1], (next_odd, t)).wait_recv()

    @pl.when(pair == 0)
    def _():
        s_in[...] = jnp.zeros_like(s_in)

    @pl.when(jnp.logical_and(odd == 1, pair < pairs - 1))
    def _():
        for h in range(heads):
            s_out[h] = (
                mm(pair_tot[h][:, :width], s_in[h].astype(jnp.float32)) + pair_tot[h][:, width:]
            ).astype(jnp.bfloat16)
        remote(s_out, s_in, c_send.at[1], c_recv.at[1], (next_odd, t)).start()
        remote(s_out, s_in, c_send.at[2], c_recv.at[1], (next_even, t)).start()

    @pl.when(odd == 1)
    def _():
        for h in range(heads):
            state_s[h] = mm(
                pair_in[h][:, :width].astype(jnp.float32), s_in[h].astype(jnp.float32)
            ) + pair_in[h][:, width:].astype(jnp.float32)

    @pl.when(odd == 0)
    def _():
        state_s[...] = s_in[...].astype(jnp.float32)

    for h in range(heads):
        out = mm(gs[h], state_s[h]) + zs[h]
        out = out * lax.rsqrt(jnp.mean(out * out, axis=-1, keepdims=True) + EPS)
        normed[:, h * width : (h + 1) * width] = (out * head_gain_ref[...]).astype(jnp.bfloat16)
    locals_[6].wait()
    for r, owner in enumerate((t, core_t, (t + 2) % 4, (core_t + 2) % 4)):
        mine = pl.ds(pl.multiple_of(owner * tokens, tokens), tokens)
        mx_part[r] = jnp.dot(
            normed[mine, :], mw[...], preferred_element_type=jnp.float32
        ).astype(jnp.bfloat16)
    reduce_start(1, mx_part, mx_in)
    forward(2, up_at)
    reduce_cross(1, mx_part, mx_in, mx_cross, mx_far)

    for i in (1, 2):
        remote(wg.at[FAR], wg.at[FAR], w_send.at[i, 2], w_recv.at[i, 2], core).wait_recv()
    lax.fori_loop(CROSS, FAR + 1, hidden_of, 0)

    def down_of(j, carry):
        place = down_at(j)
        forward(3 + j, place)
        take(3 + j, place)
        hidden = jnp.concatenate([hid[r] for r in range(4)], axis=1)
        weight = wd[:, :, cols(j)].reshape(4 * unit, cut)
        slot_out[:, :, cols(j)] = (
            jnp.dot(hidden, weight, preferred_element_type=jnp.float32)
            .astype(jnp.bfloat16)
            .reshape(devices, capacity, cut)
        )
        for o in range(1, devices):
            peer = (e + o) % devices
            remote(
                slot_out.at[peer, :, cols(j)],
                returned.at[e, :, cols(j)],
                r_send.at[j, o - 1],
                r_recv.at[j, o - 1],
                (peer, t),
            ).start()
        pltpu.make_async_copy(
            slot_out.at[e, :, cols(j)], returned.at[e, :, cols(j)], r_local.at[j]
        ).start()
        return carry

    lax.fori_loop(0, CUTS, down_of, 0)

    mix_ref[...] = reduce_finish(1, mx_part, mx_in, mx_cross, mx_far).astype(jnp.bfloat16)
    shared = reduce_finish(0, sh_part, sh_in, sh_cross, sh_far)

    for j in range(CUTS):
        for o in range(1, devices):
            remote(
                slot_out.at[e, :, cols(j)],
                returned.at[e, :, cols(j)],
                r_send.at[j, o - 1],
                r_recv.at[j, o - 1],
                (e, core_t),
            ).wait_recv()
        pltpu.make_async_copy(
            slot_out.at[e, :, cols(j)], returned.at[e, :, cols(j)], r_local.at[j]
        ).wait()
        back = returned[:, :, j * cut : (j + 1) * cut].reshape(slots, cut)
        routed = jnp.dot(coarse_ref[...], back, preferred_element_type=jnp.float32) + jnp.dot(
            fine_ref[...], back, preferred_element_type=jnp.float32
        )
        moe_ref[:, j * cut : (j + 1) * cut] = (
            shared[:, j * cut : (j + 1) * cut] + routed
        ).astype(jnp.bfloat16)

    remote(toks.at[CROSS], toks.at[CROSS], w_send.at[0, 0], w_recv.at[0, 0], cross).wait_send()
    remote(toks.at[CORE], toks.at[CORE], w_send.at[0, 1], w_recv.at[0, 1], core).wait_send()
    sent(1, gate_at)
    sent(2, up_at)
    for j in range(CUTS):
        sent(3 + j, down_at(j))
    for o in range(1, devices):
        remote(
            outgoing.at[e], arrived.at[e], d_send.at[o - 1], d_recv.at[o - 1], (e, core_t)
        ).wait_send()
        for j in range(CUTS):
            remote(
                slot_out.at[e, :, cols(j)],
                returned.at[e, :, cols(j)],
                r_send.at[j, o - 1],
                r_recv.at[j, o - 1],
                (e, core_t),
            ).wait_send()
    reduce_sent(0, sh_part, sh_in, sh_cross, sh_far)
    reduce_sent(1, mx_part, mx_in, mx_cross, mx_far)

    @pl.when(odd == 0)
    def _():
        to_odd.wait_send()

    @pl.when(jnp.logical_and(odd == 1, pair < pairs - 1))
    def _():
        remote(s_out, s_in, c_send.at[1], c_recv.at[1], (next_odd, t)).wait_send()
        remote(s_out, s_in, c_send.at[2], c_recv.at[1], (next_even, t)).wait_send()


def fused_shards(
    queries,
    keys,
    values,
    decay_gate_logits,
    correction_logits,
    head_decay_speed,
    position_log_decay,
    head_output_gain,
    mixer_output_weight,
    expert_input_tokens,
    expert_norm_gain,
    routes,
    chosen_expert_weight,
    routed_gate_weight,
    routed_up_weight,
    routed_down_weight,
    common_gate_weight,
    common_up_weight,
    common_down_weight,
):
    devices = lax.axis_size("ep")
    tokens, top_k = routes.shape
    model = expert_input_tokens.shape[1]
    length = queries.shape[0]
    heads = decay_gate_logits.shape[1]
    width = queries.shape[1] // heads
    count = length // SPAN
    unit = routed_gate_weight.shape[2]
    shared_unit = common_gate_weight.shape[1]
    capacity = 3 * tokens * top_k // (2 * devices)
    slot_count = devices * capacity
    slots = slot_layout(routes, capacity)
    numbers = jnp.arange(slot_count, dtype=jnp.int32)
    sends = sum(
        (slots[None, :, k] == numbers[:, None]).astype(jnp.bfloat16) for k in range(top_k)
    )
    weights = sum(
        jnp.where(
            slots[:, k : k + 1] == numbers[None, :], chosen_expert_weight[:, k : k + 1], 0.0
        )
        for k in range(top_k)
    )
    coarse = weights.astype(jnp.bfloat16)
    fine = (weights - coarse.astype(jnp.float32)).astype(jnp.bfloat16)
    bf, f32 = jnp.bfloat16, jnp.float32
    vmem = pl.BlockSpec(memory_space=pltpu.VMEM)
    anywhere = pl.BlockSpec(memory_space=pl.ANY)
    dma = pltpu.SemaphoreType.DMA
    quarter = (4, tokens, model)
    slot_shape = (devices, capacity, model)
    return pl.pallas_call(
        functools.partial(fused_kernel, devices),
        in_specs=[vmem] * 13 + [anywhere] * 7,
        out_specs=[vmem, vmem],
        out_shape=[jax.ShapeDtypeStruct((tokens, model), bf)] * 2,
        scratch_shapes=[
            pltpu.VMEM((4, model, unit), bf),
            pltpu.VMEM((4, model, unit), bf),
            pltpu.VMEM((4, unit, model), bf),
            pltpu.VMEM((model, shared_unit), bf),
            pltpu.VMEM((model, shared_unit), bf),
            pltpu.VMEM((shared_unit, model), bf),
            pltpu.VMEM(mixer_output_weight.shape, bf),
            pltpu.VMEM(quarter, bf),
            pltpu.VMEM(slot_shape, bf),
            pltpu.VMEM(slot_shape, bf),
            pltpu.VMEM((4, slot_count, unit), bf),
            pltpu.VMEM(slot_shape, bf),
            pltpu.VMEM(slot_shape, bf),
            pltpu.VMEM(quarter, bf),
            pltpu.VMEM((2, tokens, model), bf),
            pltpu.VMEM((tokens, model), bf),
            pltpu.VMEM((tokens, model), bf),
            pltpu.VMEM(quarter, bf),
            pltpu.VMEM((2, tokens, model), bf),
            pltpu.VMEM((tokens, model), bf),
            pltpu.VMEM((tokens, model), bf),
            pltpu.VMEM((heads, count, SPAN, 1), f32),
            pltpu.VMEM((heads, count, 1, SPAN), f32),
            pltpu.VMEM((heads, count, SPAN, 1), f32),
            pltpu.VMEM((heads, length, width), f32),
            pltpu.VMEM((heads, length, width), f32),
            pltpu.VMEM((heads, width, 2 * width), f32),
            pltpu.VMEM((heads, width, 2 * width), bf),
            pltpu.VMEM((heads, width, 2 * width), bf),
            pltpu.VMEM((heads, width, 2 * width), f32),
            pltpu.VMEM((heads, width, width), bf),
            pltpu.VMEM((heads, width, width), bf),
            pltpu.VMEM((heads, width, width), f32),
            pltpu.VMEM((length, heads * width), bf),
            dma((8,)),
            dma((3 + CUTS, 3)),
            dma((3 + CUTS, 3)),
            dma((devices - 1,)),
            dma((devices - 1,)),
            dma((CUTS, devices - 1)),
            dma((CUTS, devices - 1)),
            dma((CUTS,)),
            dma((2, 3)),
            dma((2, 3)),
            dma((3,)),
            dma((2,)),
        ],
        compiler_params=pltpu.CompilerParams(
            collective_id=0, has_side_effects=True, vmem_limit_bytes=62 << 20
        ),
    )(
        queries,
        keys,
        values,
        decay_gate_logits,
        correction_logits,
        head_decay_speed.reshape(1, heads),
        position_log_decay,
        head_output_gain.reshape(1, width),
        expert_input_tokens,
        expert_norm_gain.reshape(1, model),
        sends,
        coarse,
        fine,
        mixer_output_weight,
        routed_gate_weight[0],
        routed_up_weight[0],
        routed_down_weight[0],
        common_gate_weight,
        common_up_weight,
        common_down_weight,
    )


def shards(*args):
    devices, members = lax.axis_size("ep"), lax.axis_size("tp")
    routes, tokens = args[11], args[9]
    capacity = 3 * routes.shape[0] * routes.shape[1] // (2 * devices)
    whole_tiles = capacity % 16 == 0 and tokens.shape[1] % (128 * CUTS) == 0
    if members == 4 and devices % 2 == 0 and whole_tiles:
        return fused_shards(*args)
    return plain_shards(*args)


def solution(mesh):
    return jax.shard_map(
        shards,
        mesh=mesh,
        in_specs=(
            P("ep", "tp"),
            P("ep", "tp"),
            P("ep", "tp"),
            P("ep", "tp"),
            P("ep", "tp"),
            P("tp"),
            P("ep", "tp"),
            P(),
            P("tp", None),
            P(("ep", "tp"), None),
            P(),
            P(("ep", "tp"), None),
            P(("ep", "tp"), None),
            P("ep", None, "tp"),
            P("ep", None, "tp"),
            P("ep", "tp", None),
            P(None, "tp"),
            P(None, "tp"),
            P("tp", None),
        ),
        out_specs=(P(("ep", "tp"), None), P(("ep", "tp"), None)),
        check_vma=False,
    )
```

```python
import functools

import jax
import jax.numpy as jnp
from jax import lax
from jax.experimental import pallas as pl
from jax.experimental.pallas import tpu as pltpu
from jax.sharding import PartitionSpec as P


EPS = 1e-06


SPAN = 64


def halves(x):
    high = x.astype(jnp.bfloat16)
    return high, (x - high.astype(jnp.float32)).astype(jnp.bfloat16)


def product(left, right, numbers):
    left_high, left_low = halves(left)
    right_high, right_low = halves(right)

    def dot(x, y):
        return lax.dot_general(x, y, numbers, preferred_element_type=jnp.float32)

    return dot(left_high, right_high) + (dot(left_high, right_low) + dot(left_low, right_high))


def bmm(left, right, dims):
    return product(left, right, (dims, ((0,), (0,))))


def mm(left, right):
    return product(left, right, (((1,), (0,)), ((), ())))


def unit_lower_inverse(lower, rows, cols):
    inverse = jnp.where(rows == cols, 1.0, 0.0) - jnp.where(
        ((rows >> 1) == (cols >> 1)), lower, 0.0
    )
    level = 1
    while (1 << level) < SPAN:
        below = ((rows >> (level + 1)) == (cols >> (level + 1))) & (
            (rows >> level) != (cols >> level)
        )
        part = jnp.where(below, lower, 0.0)
        inverse = inverse - bmm(bmm(inverse, part, ((2,), (1,))), inverse, ((2,), (1,)))
        level += 1
    return inverse


def local_kernel(q_ref, k_ref, v_ref, ccol_ref, crow_ref, bcol_ref, g_ref, z_ref, total_ref):
    width = q_ref.shape[1]
    count = q_ref.shape[0] // SPAN
    shape = (count, SPAN, width)
    q = q_ref[...].astype(jnp.float32)
    k = k_ref[...].astype(jnp.float32)
    v = v_ref[...].astype(jnp.float32).reshape(shape)
    q = q * lax.rsqrt(jnp.sum(q * q, axis=-1, keepdims=True) + EPS) * width ** (-0.5)
    k = k * lax.rsqrt(jnp.sum(k * k, axis=-1, keepdims=True) + EPS)
    q = q.reshape(shape)
    k = k.reshape(shape)
    ccol = ccol_ref[0].reshape(count, SPAN, 1)
    crow = crow_ref[0]
    bcol = bcol_ref[0].reshape(count, SPAN, 1)
    rows = lax.broadcasted_iota(jnp.int32, (count, SPAN, SPAN), 1)
    cols = lax.broadcasted_iota(jnp.int32, (count, SPAN, SPAN), 2)
    decay = jnp.exp(jnp.where(rows >= cols, ccol - crow, -jnp.inf))
    keyed = k * bcol
    lower = jnp.where(rows > cols, bmm(keyed, k, ((2,), (2,))) * decay, 0.0)
    inverse = unit_lower_inverse(lower, rows, cols)
    grown = jnp.exp(ccol)
    solved = bmm(
        inverse, jnp.concatenate([keyed * grown, v * bcol], axis=-1), ((2,), (1,))
    )
    scores = bmm(q, k, ((2,), (2,))) * decay
    q_scaled = q * grown
    last = ccol[:, SPAN - 1 :, :]
    carried = k * jnp.exp(last - ccol)
    mixed = bmm(scores, solved, ((2,), (1,)))
    readout = q_scaled - mixed[:, :, :width]
    eye_r = lax.broadcasted_iota(jnp.int32, (width, width), 0)
    eye_c = lax.broadcasted_iota(jnp.int32, (width, width), 1)
    eye = jnp.where(eye_r == eye_c, 1.0, 0.0)
    state = jnp.concatenate([eye, jnp.zeros_like(eye)], axis=1)
    for n in range(count):
        seen = mm(readout[n], state)
        g_ref[0, n * SPAN : (n + 1) * SPAN, :] = seen[:, :width]
        z_ref[0, n * SPAN : (n + 1) * SPAN, :] = seen[:, width:] + mixed[n][:, width:]
        both = mm(carried[n].T, solved[n])
        trans = jnp.exp(last[n]) * eye - both[:, :width]
        state = mm(trans, state)
        state = jnp.concatenate([state[:, :width], state[:, width:] + both[:, width:]], axis=1)
    total_ref[0] = state.astype(jnp.bfloat16)


def finish_kernel(place_ref, gathered_ref, g_ref, z_ref, gain_ref, out_ref):
    width = g_ref.shape[2]

    def one(turn, state):
        both = gathered_ref[turn, 0].astype(jnp.float32)
        return mm(both[:, :width], state) + both[:, width:]

    state = lax.fori_loop(0, place_ref[0], one, jnp.zeros((width, width), jnp.float32))
    out = mm(g_ref[0], state) + z_ref[0]
    out = out * lax.rsqrt(jnp.mean(out * out, axis=-1, keepdims=True) + EPS) * gain_ref[...]
    out_ref[...] = out.astype(jnp.bfloat16)


def token_mixer_heads(
    queries,
    keys,
    values,
    decay_gate_logits,
    correction_logits,
    head_decay_speed,
    position_log_decay,
    head_output_gain,
):
    heads = decay_gate_logits.shape[1]
    length = queries.shape[0]
    width = queries.shape[1] // heads
    count = length // SPAN
    log_gate = -head_decay_speed * jax.nn.softplus(decay_gate_logits) + position_log_decay
    log_gate = log_gate.T.reshape(heads, count, SPAN)
    at = jnp.arange(SPAN)
    cum = jnp.sum(
        jnp.where(at[:, None] >= at[None, :], log_gate[:, :, None, :], 0.0), axis=-1
    )
    beta = jax.nn.sigmoid(correction_logits.astype(jnp.float32)).T.reshape(heads, length, 1)
    by_head = pl.BlockSpec((length, width), lambda h: (0, h))
    column = pl.BlockSpec((1, length, 1), lambda h: (h, 0, 0))
    whole = pl.BlockSpec((1, length, width), lambda h: (h, 0, 0))
    local_call = pl.pallas_call(
        local_kernel,
        grid=(heads,),
        in_specs=[
            by_head,
            by_head,
            by_head,
            column,
            pl.BlockSpec((1, count, 1, SPAN), lambda h: (h, 0, 0, 0)),
            column,
        ],
        out_specs=[whole, whole, pl.BlockSpec((1, width, 2 * width), lambda h: (h, 0, 0))],
        out_shape=[
            jax.ShapeDtypeStruct((heads, length, width), jnp.float32),
            jax.ShapeDtypeStruct((heads, length, width), jnp.float32),
            jax.ShapeDtypeStruct((heads, width, 2 * width), jnp.bfloat16),
        ],
        cost_estimate=pl.CostEstimate(
            flops=3_000_000_000, bytes_accessed=4_000_000, transcendentals=200_000
        ),
    )
    readout, local_out, total = local_call(
        queries,
        keys,
        values,
        cum.reshape(heads, length, 1),
        cum.reshape(heads, count, 1, SPAN),
        beta,
    )
    gathered = lax.all_gather(total, "ep")
    place = lax.axis_index("ep").astype(jnp.int32).reshape(1)
    devices = gathered.shape[0]
    return pl.pallas_call(
        finish_kernel,
        grid=(heads,),
        in_specs=[
            pl.BlockSpec(memory_space=pltpu.SMEM),
            pl.BlockSpec((devices, 1, width, 2 * width), lambda h: (0, h, 0, 0)),
            whole,
            whole,
            pl.BlockSpec((1, width), lambda h: (0, 0)),
        ],
        out_specs=by_head,
        out_shape=jax.ShapeDtypeStruct((length, heads * width), jnp.bfloat16),
        cost_estimate=pl.CostEstimate(
            flops=500_000_000, bytes_accessed=4_000_000, transcendentals=2_000
        ),
    )(place, gathered, readout, local_out, head_output_gain.reshape(1, width))


def norm_rows(expert_input_tokens, expert_norm_gain):
    rows_f = expert_input_tokens.astype(jnp.float32)
    scaled = (
        rows_f
        * lax.rsqrt(jnp.mean(rows_f * rows_f, axis=-1, keepdims=True) + EPS)
        * expert_norm_gain
    )
    return scaled.astype(jnp.bfloat16)


def gated_hidden(rows_in, w_gate, w_up):
    gate_val = jnp.dot(rows_in, w_gate, preferred_element_type=jnp.float32)
    up_val = jnp.dot(rows_in, w_up, preferred_element_type=jnp.float32)
    return (jax.nn.silu(gate_val) * up_val).astype(jnp.bfloat16)


def slot_layout(routes, capacity):
    flat = routes.reshape(-1)
    at = jnp.arange(flat.shape[0], dtype=jnp.int32)
    same = (flat[:, None] == flat[None, :]) & (at[None, :] < at[:, None])
    before = jnp.sum(same.astype(jnp.int32), axis=1)
    return (flat * capacity + before).reshape(routes.shape)


def plain_shards(
    queries,
    keys,
    values,
    decay_gate_logits,
    correction_logits,
    head_decay_speed,
    position_log_decay,
    head_output_gain,
    mixer_output_weight,
    expert_input_tokens,
    expert_norm_gain,
    routes,
    chosen_expert_weight,
    routed_gate_weight,
    routed_up_weight,
    routed_down_weight,
    common_gate_weight,
    common_up_weight,
    common_down_weight,
):
    normed = token_mixer_heads(
        queries,
        keys,
        values,
        decay_gate_logits,
        correction_logits,
        head_decay_speed,
        position_log_decay,
        head_output_gain,
    )
    mixer_out = lax.psum_scatter(
        jnp.dot(normed, mixer_output_weight, preferred_element_type=jnp.float32).astype(
            jnp.bfloat16
        ),
        "tp",
        scatter_dimension=0,
        tiled=True,
    )
    normed_in = norm_rows(expert_input_tokens, expert_norm_gain)
    tokens_own, top_k = routes.shape
    model_width = expert_input_tokens.shape[1]
    experts = lax.axis_size("ep")
    capacity = 3 * tokens_own * top_k // (2 * experts)
    slot_count = experts * capacity
    slots = slot_layout(routes, capacity)
    numbers = jnp.arange(slot_count, dtype=jnp.int32)
    sends = sum(
        (slots[None, :, k] == numbers[:, None]).astype(jnp.bfloat16) for k in range(top_k)
    )
    outgoing = jnp.dot(sends, normed_in, preferred_element_type=jnp.float32).astype(
        jnp.bfloat16
    )
    arrived = lax.all_to_all(
        outgoing.reshape(experts, capacity, model_width),
        "ep",
        split_axis=0,
        concat_axis=0,
        tiled=True,
    ).reshape(slot_count, model_width)
    gate_all = lax.all_gather(routed_gate_weight[0], "tp")
    up_all = lax.all_gather(routed_up_weight[0], "tp")
    down_all = lax.all_gather(routed_down_weight[0], "tp", axis=0, tiled=True)
    hidden = jnp.concatenate(
        [gated_hidden(arrived, gate_all[t], up_all[t]) for t in range(gate_all.shape[0])],
        axis=1,
    )
    slot_sums = jnp.dot(hidden, down_all, preferred_element_type=jnp.float32).astype(
        jnp.bfloat16
    )
    returned = lax.all_to_all(
        slot_sums.reshape(experts, capacity, model_width),
        "ep",
        split_axis=0,
        concat_axis=0,
        tiled=True,
    ).reshape(slot_count, model_width)
    shared_hidden = gated_hidden(
        lax.all_gather(normed_in, "tp", axis=0, tiled=True), common_gate_weight, common_up_weight
    )
    shared = lax.psum_scatter(
        jnp.dot(shared_hidden, common_down_weight, preferred_element_type=jnp.float32).astype(
            jnp.bfloat16
        ),
        "tp",
        scatter_dimension=0,
        tiled=True,
    ).astype(jnp.float32)
    weights = sum(
        jnp.where(
            slots[:, k : k + 1] == numbers[None, :], chosen_expert_weight[:, k : k + 1], 0.0
        )
        for k in range(top_k)
    )
    coarse = weights.astype(jnp.bfloat16)
    fine = (weights - coarse.astype(jnp.float32)).astype(jnp.bfloat16)
    routed = jnp.dot(coarse, returned, preferred_element_type=jnp.float32) + jnp.dot(
        fine, returned, preferred_element_type=jnp.float32
    )
    moe_out = (shared + routed).astype(jnp.bfloat16)
    return (mixer_out, moe_out)


MESH = pl.DeviceIdType.MESH
CUTS = 4
OWN, CORE, CROSS, FAR = range(4)


def scaled_rows(rows, gain):
    rows_f = rows.astype(jnp.float32)
    norm = lax.rsqrt(jnp.mean(rows_f * rows_f, axis=-1, keepdims=True) + EPS)
    return (rows_f * norm * gain).astype(jnp.bfloat16)


def silu_product(gate_val, up_val):
    return (gate_val / (1.0 + jnp.exp(-gate_val)) * up_val).astype(jnp.bfloat16)


def fused_kernel(
    devices,
    decay_ref,
    correct_ref,
    speed_ref,
    log_ref,
    head_gain_ref,
    gain_ref,
    routes_ref,
    chosen_ref,
    q_hbm,
    k_hbm,
    v_hbm,
    tok_hbm,
    mixw_hbm,
    rg_hbm,
    ru_hbm,
    rd_hbm,
    cg_hbm,
    cu_hbm,
    cd_hbm,
    mix_ref,
    moe_ref,
    wg,
    wu,
    wd,
    cg,
    cu,
    cd,
    mw,
    q_ref,
    k_ref,
    v_ref,
    tok_ref,
    hits_ref,
    weight_ref,
    lrow_s,
    brow_s,
    toks,
    outgoing,
    arrived,
    hid,
    slot_out,
    returned,
    sh_part,
    sh_in,
    sh_cross,
    sh_far,
    mx_part,
    mx_in,
    mx_cross,
    mx_far,
    ccol_s,
    crow_s,
    bcol_s,
    gs,
    zs,
    tot,
    tot_bf,
    pair_in,
    pair_tot,
    s_in,
    s_out,
    state_s,
    normed,
    local_sem,
    w_send,
    w_recv,
    d_send,
    d_recv,
    r_send,
    r_recv,
    r_local,
    rs_send,
    rs_recv,
    c_send,
    c_recv,
):
    e = lax.axis_index("ep")
    t = lax.axis_index("tp")
    heads = decay_ref.shape[0]
    width = q_ref.shape[1] // heads
    length = q_ref.shape[0]
    count = length // SPAN
    tokens, model = tok_ref.shape
    top_k = routes_ref.shape[0]
    capacity = arrived.shape[1]
    slots = devices * capacity
    unit = wg.shape[2]
    cut = model // CUTS
    core_t = t + 1 - 2 * (t % 2)
    core = (e, core_t)
    cross = (e, (t + 2) % 4)

    def remote(src, dst, send, recv, peer):
        return pltpu.make_async_remote_copy(
            src_ref=src,
            dst_ref=dst,
            send_sem=send,
            recv_sem=recv,
            device_id=peer,
            device_id_type=MESH,
        )

    early = [
        pltpu.make_async_copy(src, dst, local_sem.at[8 + n])
        for n, (src, dst) in enumerate(
            ((tok_hbm, tok_ref), (q_hbm, q_ref), (k_hbm, k_ref), (v_hbm, v_ref))
        )
    ]
    locals_ = [
        pltpu.make_async_copy(src, dst, local_sem.at[n])
        for n, (src, dst) in enumerate(
            (
                (cg_hbm, cg),
                (cu_hbm, cu),
                (cd_hbm, cd),
                (rg_hbm, wg.at[OWN]),
                (ru_hbm, wu.at[OWN]),
                (rd_hbm, wd.at[OWN]),
                (mixw_hbm, mw),
            )
        )
    ]
    for copy in early:
        copy.start()

    barrier = pltpu.get_barrier_semaphore()
    for o in range(1, devices):
        pl.semaphore_signal(
            barrier, inc=1, device_id=((e + o) % devices, t), device_id_type=MESH
        )
    for o in range(1, 4):
        pl.semaphore_signal(barrier, inc=1, device_id=(e, (t + o) % 4), device_id_type=MESH)

    expert = lax.broadcasted_iota(jnp.int32, (devices, tokens), 0)
    earlier = lax.broadcasted_iota(jnp.int32, (tokens, tokens), 0)
    earlier = jnp.where(
        earlier < lax.broadcasted_iota(jnp.int32, (tokens, tokens), 1), 1.0, 0.0
    ).astype(jnp.bfloat16)
    number = lax.broadcasted_iota(jnp.int32, (slots, tokens), 0).astype(jnp.float32)
    base = jnp.zeros((devices, 1), jnp.float32)
    sends = jnp.zeros((slots, tokens), jnp.bfloat16)
    token_a = lax.broadcasted_iota(jnp.int32, (tokens, tokens), 0)
    token_b = lax.broadcasted_iota(jnp.int32, (tokens, tokens), 1)
    for n in range(top_k):
        route = routes_ref[n : n + 1, :]
        chosen = jnp.where(expert == route, 1.0, 0.0)
        before = base + jnp.dot(
            chosen.astype(jnp.bfloat16), earlier, preferred_element_type=jnp.float32
        )
        base = base + jnp.sum(chosen, axis=1, keepdims=True)
        slot = route.astype(jnp.float32) * capacity + jnp.sum(
            chosen * before, axis=0, keepdims=True
        )
        hit = jnp.where(number == slot, 1.0, 0.0).astype(jnp.bfloat16)
        sends = sends + hit
        hits_ref[n] = hit
        weight_ref[n] = jnp.sum(
            jnp.where(token_a == token_b, chosen_ref[n : n + 1, :], 0.0), axis=1, keepdims=True
        )

    pl.semaphore_wait(barrier, devices + 2)

    def cols(j):
        return pl.ds(pl.multiple_of(j * cut, cut), cut)

    def spread(i, src, place):
        remote(src, place(CROSS), w_send.at[i, 0], w_recv.at[i, 0], cross).start()
        remote(src, place(CORE), w_send.at[i, 1], w_recv.at[i, 1], core).start()

    def forward(i, place):
        remote(place(CROSS), place(CROSS), w_send.at[i, 0], w_recv.at[i, 0], cross).wait_recv()
        remote(place(CROSS), place(FAR), w_send.at[i, 2], w_recv.at[i, 2], core).start()

    def take(i, place):
        remote(place(CORE), place(CORE), w_send.at[i, 1], w_recv.at[i, 1], core).wait_recv()
        remote(place(FAR), place(FAR), w_send.at[i, 2], w_recv.at[i, 2], core).wait_recv()

    def sent(i, place):
        remote(place(CROSS), place(CROSS), w_send.at[i, 0], w_recv.at[i, 0], cross).wait_send()
        remote(place(CORE), place(CORE), w_send.at[i, 1], w_recv.at[i, 1], core).wait_send()
        remote(place(FAR), place(FAR), w_send.at[i, 2], w_recv.at[i, 2], core).wait_send()

    def tok_at(r):
        return toks.at[r]

    def gate_at(r):
        return wg.at[r]

    def up_at(r):
        return wu.at[r]

    def down_at(j):
        return lambda r: wd.at[r, :, cols(j)]

    spread(0, tok_hbm, tok_at)
    spread(1, rg_hbm, gate_at)
    spread(2, ru_hbm, up_at)
    for j in range(CUTS):
        remote(
            rd_hbm.at[:, cols(j)], wd.at[CROSS, :, cols(j)], w_send.at[3 + j, 0], w_recv.at[3 + j, 0], cross
        ).start()
        remote(
            rd_hbm.at[:, cols(j)], wd.at[CORE, :, cols(j)], w_send.at[3 + j, 1], w_recv.at[3 + j, 1], core
        ).start()

    for copy in locals_:
        copy.start()

    early[0].wait()
    toks[OWN] = scaled_rows(tok_ref[...], gain_ref[...])
    outgoing[...] = (
        jnp.dot(sends, toks[OWN], preferred_element_type=jnp.float32)
        .astype(jnp.bfloat16)
        .reshape(outgoing.shape)
    )

    rows = lax.broadcasted_iota(jnp.int32, (count, SPAN, SPAN), 1)
    cols_at = lax.broadcasted_iota(jnp.int32, (count, SPAN, SPAN), 2)
    for h in range(heads):
        logit = decay_ref[h : h + 1, :]
        softplus = jnp.maximum(logit, 0.0) + jnp.log1p(jnp.exp(-jnp.abs(logit)))
        log_gate = -speed_ref[0:1, h : h + 1] * softplus + log_ref[h : h + 1, :]
        beta = 1.0 / (1.0 + jnp.exp(-correct_ref[h : h + 1, :].astype(jnp.float32)))
        for n in range(count):
            lrow_s[n] = log_gate[:, n * SPAN : (n + 1) * SPAN]
            brow_s[n] = beta[:, n * SPAN : (n + 1) * SPAN]
        ccol = jnp.sum(jnp.where(rows >= cols_at, lrow_s[...], 0.0), axis=2, keepdims=True)
        ccol_s[h] = ccol
        crow_s[h] = jnp.sum(jnp.where(rows == cols_at, ccol, 0.0), axis=1, keepdims=True)
        bcol_s[h] = jnp.sum(
            jnp.where(rows == cols_at, brow_s[...], 0.0), axis=2, keepdims=True
        )

    for o in range(1, devices):
        peer = (e + o) % devices
        remote(
            outgoing.at[peer], arrived.at[e], d_send.at[o - 1], d_recv.at[o - 1], (peer, t)
        ).start()
    own_rows = pltpu.make_async_copy(outgoing.at[e], arrived.at[e], local_sem.at[7])
    own_rows.start()

    def local_head(h, carry):
        at = pl.ds(pl.multiple_of(h * width, width), width)
        shape = (count, SPAN, width)
        q = q_ref[:, at].astype(jnp.float32)
        k = k_ref[:, at].astype(jnp.float32)
        v = v_ref[:, at].astype(jnp.float32).reshape(shape)
        q = q * lax.rsqrt(jnp.sum(q * q, axis=-1, keepdims=True) + EPS) * width ** (-0.5)
        k = k * lax.rsqrt(jnp.sum(k * k, axis=-1, keepdims=True) + EPS)
        q = q.reshape(shape)
        k = k.reshape(shape)
        ccol = ccol_s[h]
        crow = crow_s[h]
        bcol = bcol_s[h]
        decay = jnp.exp(jnp.where(rows >= cols_at, ccol - crow, -jnp.inf))
        keyed = k * bcol
        lower = jnp.where(rows > cols_at, bmm(keyed, k, ((2,), (2,))) * decay, 0.0)
        inverse = unit_lower_inverse(lower, rows, cols_at)
        grown = jnp.exp(ccol)
        solved = bmm(
            inverse, jnp.concatenate([keyed * grown, v * bcol], axis=-1), ((2,), (1,))
        )
        scores = bmm(q, k, ((2,), (2,))) * decay
        q_scaled = q * grown
        last = ccol[:, SPAN - 1 :, :]
        carried = k * jnp.exp(last - ccol)
        mixed = bmm(scores, solved, ((2,), (1,)))
        readout = q_scaled - mixed[:, :, :width]
        eye_r = lax.broadcasted_iota(jnp.int32, (width, width), 0)
        eye_c = lax.broadcasted_iota(jnp.int32, (width, width), 1)
        eye = jnp.where(eye_r == eye_c, 1.0, 0.0)
        state = jnp.concatenate([eye, jnp.zeros_like(eye)], axis=1)
        for n in range(count):
            seen = mm(readout[n], state)
            gs[h, n * SPAN : (n + 1) * SPAN, :] = seen[:, :width]
            zs[h, n * SPAN : (n + 1) * SPAN, :] = seen[:, width:] + mixed[n][:, width:]
            both = mm(carried[n].T, solved[n])
            trans = jnp.exp(last[n]) * eye - both[:, :width]
            state = mm(trans, state)
            state = jnp.concatenate([state[:, :width], state[:, width:] + both[:, width:]], axis=1)
        tot[h] = state
        tot_bf[h] = state.astype(jnp.bfloat16)
        return carry

    for copy in early[1:]:
        copy.wait()
    lax.fori_loop(0, heads, local_head, 0)

    odd = e % 2
    pair = e // 2
    pairs = devices // 2
    forward(0, tok_at)
    to_odd = remote(tot_bf, pair_in, c_send.at[0], c_recv.at[0], ((e + 1) % devices, t))

    @pl.when(odd == 0)
    def _():
        to_odd.start()

    take(0, tok_at)
    for n in range(3):
        locals_[n].wait()
    gain = gain_ref[...]
    for r in (CORE, CROSS, FAR):
        if r == CROSS:
            remote(tok_at(FAR), tok_at(FAR), w_send.at[0, 2], w_recv.at[0, 2], core).wait_send()
        toks[r] = scaled_rows(toks[r], gain)
    x_all = toks[...].reshape(4 * tokens, model)
    sh_hid = silu_product(
        jnp.dot(x_all, cg[...], preferred_element_type=jnp.float32),
        jnp.dot(x_all, cu[...], preferred_element_type=jnp.float32),
    )
    sh_part[...] = (
        jnp.dot(sh_hid, cd[...], preferred_element_type=jnp.float32)
        .astype(jnp.bfloat16)
        .reshape(sh_part.shape)
    )

    def reduce_start(n, part, inbox):
        for i, r in enumerate((FAR, CORE)):
            remote(
                part.at[r], inbox.at[1 - i], rs_send.at[n, i], rs_recv.at[n, i], core
            ).start()

    def reduce_cross(n, part, inbox, out, far):
        remote(part.at[FAR], inbox.at[1], rs_send.at[n, 0], rs_recv.at[n, 0], core).wait_recv()
        out[...] = (part[CROSS].astype(jnp.float32) + inbox[1].astype(jnp.float32)).astype(
            jnp.bfloat16
        )
        remote(out, far, rs_send.at[n, 2], rs_recv.at[n, 2], cross).start()

    def reduce_finish(n, part, inbox, out, far):
        remote(part.at[CORE], inbox.at[0], rs_send.at[n, 1], rs_recv.at[n, 1], core).wait_recv()
        remote(out, far, rs_send.at[n, 2], rs_recv.at[n, 2], cross).wait_recv()
        return (
            part[OWN].astype(jnp.float32)
            + inbox[0].astype(jnp.float32)
            + far[...].astype(jnp.float32)
        )

    def reduce_sent(n, part, inbox, out, far):
        remote(part.at[FAR], inbox.at[1], rs_send.at[n, 0], rs_recv.at[n, 0], core).wait_send()
        remote(part.at[CORE], inbox.at[0], rs_send.at[n, 1], rs_recv.at[n, 1], core).wait_send()
        remote(out, far, rs_send.at[n, 2], rs_recv.at[n, 2], cross).wait_send()

    reduce_start(0, sh_part, sh_in)

    @pl.when(odd == 1)
    def _():
        remote(tot_bf, pair_in, c_send.at[0], c_recv.at[0], ((e + 1) % devices, t)).wait_recv()
        for h in range(heads):
            both = mm(tot[h][:, :width], pair_in[h].astype(jnp.float32))
            pair_tot[h, :, :width] = both[:, :width]
            pair_tot[h, :, width:] = both[:, width:] + tot[h][:, width:]

    reduce_cross(0, sh_part, sh_in, sh_cross, sh_far)

    forward(1, gate_at)
    for n in range(3, 6):
        locals_[n].wait()
    for i in (1, 2):
        remote(
            wg.at[CORE], wg.at[CORE], w_send.at[i, 1], w_recv.at[i, 1], core
        ).wait_recv()
    own_rows.wait()
    for o in range(1, devices):
        remote(
            outgoing.at[e], arrived.at[e], d_send.at[o - 1], d_recv.at[o - 1], (e, core_t)
        ).wait_recv()

    def hidden_of(r, carry):
        rows_in = arrived[...].reshape(slots, model)
        hid[r] = silu_product(
            jnp.dot(rows_in, wg[r], preferred_element_type=jnp.float32),
            jnp.dot(rows_in, wu[r], preferred_element_type=jnp.float32),
        )
        return carry

    lax.fori_loop(OWN, CORE + 1, hidden_of, 0)

    next_odd = (e + 2) % devices
    next_even = (e + 1) % devices

    @pl.when(pair > 0)
    def _():
        remote(s_out, s_in, c_send.at[1], c_recv.at[1], (next_odd, t)).wait_recv()

    @pl.when(pair == 0)
    def _():
        s_in[...] = jnp.zeros_like(s_in)

    @pl.when(jnp.logical_and(odd == 1, pair < pairs - 1))
    def _():
        for h in range(heads):
            s_out[h] = (
                mm(pair_tot[h][:, :width], s_in[h].astype(jnp.float32)) + pair_tot[h][:, width:]
            ).astype(jnp.bfloat16)
        remote(s_out, s_in, c_send.at[1], c_recv.at[1], (next_odd, t)).start()
        remote(s_out, s_in, c_send.at[2], c_recv.at[1], (next_even, t)).start()

    @pl.when(odd == 1)
    def _():
        for h in range(heads):
            state_s[h] = mm(
                pair_in[h][:, :width].astype(jnp.float32), s_in[h].astype(jnp.float32)
            ) + pair_in[h][:, width:].astype(jnp.float32)

    @pl.when(odd == 0)
    def _():
        state_s[...] = s_in[...].astype(jnp.float32)

    for h in range(heads):
        out = mm(gs[h], state_s[h]) + zs[h]
        out = out * lax.rsqrt(jnp.mean(out * out, axis=-1, keepdims=True) + EPS)
        normed[:, h * width : (h + 1) * width] = (out * head_gain_ref[...]).astype(jnp.bfloat16)
    locals_[6].wait()
    for r, owner in enumerate((t, core_t, (t + 2) % 4, (core_t + 2) % 4)):
        mine = pl.ds(pl.multiple_of(owner * tokens, tokens), tokens)
        mx_part[r] = jnp.dot(
            normed[mine, :], mw[...], preferred_element_type=jnp.float32
        ).astype(jnp.bfloat16)
    reduce_start(1, mx_part, mx_in)
    forward(2, up_at)
    reduce_cross(1, mx_part, mx_in, mx_cross, mx_far)

    for i in (1, 2):
        remote(wg.at[FAR], wg.at[FAR], w_send.at[i, 2], w_recv.at[i, 2], core).wait_recv()
    lax.fori_loop(CROSS, FAR + 1, hidden_of, 0)

    def down_of(j, carry):
        place = down_at(j)
        forward(3 + j, place)
        take(3 + j, place)
        hidden = jnp.concatenate([hid[r] for r in range(4)], axis=1)
        weight = wd[:, :, cols(j)].reshape(4 * unit, cut)
        slot_out[:, :, cols(j)] = (
            jnp.dot(hidden, weight, preferred_element_type=jnp.float32)
            .astype(jnp.bfloat16)
            .reshape(devices, capacity, cut)
        )
        for o in range(1, devices):
            peer = (e + o) % devices
            remote(
                slot_out.at[peer, :, cols(j)],
                returned.at[e, :, cols(j)],
                r_send.at[j, o - 1],
                r_recv.at[j, o - 1],
                (peer, t),
            ).start()
        pltpu.make_async_copy(
            slot_out.at[e, :, cols(j)], returned.at[e, :, cols(j)], r_local.at[j]
        ).start()
        return carry

    lax.fori_loop(0, CUTS, down_of, 0)

    mix_ref[...] = reduce_finish(1, mx_part, mx_in, mx_cross, mx_far).astype(jnp.bfloat16)
    shared = reduce_finish(0, sh_part, sh_in, sh_cross, sh_far)

    for j in range(CUTS):
        for o in range(1, devices):
            remote(
                slot_out.at[e, :, cols(j)],
                returned.at[e, :, cols(j)],
                r_send.at[j, o - 1],
                r_recv.at[j, o - 1],
                (e, core_t),
            ).wait_recv()
        pltpu.make_async_copy(
            slot_out.at[e, :, cols(j)], returned.at[e, :, cols(j)], r_local.at[j]
        ).wait()
        back = returned[:, :, j * cut : (j + 1) * cut].reshape(slots, cut)
        routed = sum(
            weight_ref[n]
            * lax.dot_general(
                hits_ref[n], back, (((0,), (0,)), ((), ())), preferred_element_type=jnp.float32
            )
            for n in range(top_k)
        )
        moe_ref[:, j * cut : (j + 1) * cut] = (
            shared[:, j * cut : (j + 1) * cut] + routed
        ).astype(jnp.bfloat16)

    remote(toks.at[CROSS], toks.at[CROSS], w_send.at[0, 0], w_recv.at[0, 0], cross).wait_send()
    remote(toks.at[CORE], toks.at[CORE], w_send.at[0, 1], w_recv.at[0, 1], core).wait_send()
    sent(1, gate_at)
    sent(2, up_at)
    for j in range(CUTS):
        sent(3 + j, down_at(j))
    for o in range(1, devices):
        remote(
            outgoing.at[e], arrived.at[e], d_send.at[o - 1], d_recv.at[o - 1], (e, core_t)
        ).wait_send()
        for j in range(CUTS):
            remote(
                slot_out.at[e, :, cols(j)],
                returned.at[e, :, cols(j)],
                r_send.at[j, o - 1],
                r_recv.at[j, o - 1],
                (e, core_t),
            ).wait_send()
    reduce_sent(0, sh_part, sh_in, sh_cross, sh_far)
    reduce_sent(1, mx_part, mx_in, mx_cross, mx_far)

    @pl.when(odd == 0)
    def _():
        to_odd.wait_send()

    @pl.when(jnp.logical_and(odd == 1, pair < pairs - 1))
    def _():
        remote(s_out, s_in, c_send.at[1], c_recv.at[1], (next_odd, t)).wait_send()
        remote(s_out, s_in, c_send.at[2], c_recv.at[1], (next_even, t)).wait_send()


def hand_over(mixed_ref, routed_ref, mixer_out_ref, moe_out_ref):
    mixer_out_ref[...] = mixed_ref[...]
    moe_out_ref[...] = routed_ref[...]


def fused_shards(
    queries,
    keys,
    values,
    decay_gate_logits,
    correction_logits,
    head_decay_speed,
    position_log_decay,
    head_output_gain,
    mixer_output_weight,
    expert_input_tokens,
    expert_norm_gain,
    routes,
    chosen_expert_weight,
    routed_gate_weight,
    routed_up_weight,
    routed_down_weight,
    common_gate_weight,
    common_up_weight,
    common_down_weight,
):
    devices = lax.axis_size("ep")
    tokens, top_k = routes.shape
    model = expert_input_tokens.shape[1]
    length = queries.shape[0]
    heads = decay_gate_logits.shape[1]
    width = queries.shape[1] // heads
    count = length // SPAN
    unit = routed_gate_weight.shape[2]
    shared_unit = common_gate_weight.shape[1]
    capacity = 3 * tokens * top_k // (2 * devices)
    slot_count = devices * capacity
    bf, f32 = jnp.bfloat16, jnp.float32
    vmem = pl.BlockSpec(memory_space=pltpu.VMEM)
    anywhere = pl.BlockSpec(memory_space=pl.ANY)
    dma = pltpu.SemaphoreType.DMA
    quarter = (4, tokens, model)
    slot_shape = (devices, capacity, model)
    mixed, routed = pl.pallas_call(
        functools.partial(fused_kernel, devices),
        in_specs=[vmem] * 8 + [anywhere] * 11,
        out_specs=[vmem, vmem],
        out_shape=[jax.ShapeDtypeStruct((tokens, model), bf)] * 2,
        scratch_shapes=[
            pltpu.VMEM((4, model, unit), bf),
            pltpu.VMEM((4, model, unit), bf),
            pltpu.VMEM((4, unit, model), bf),
            pltpu.VMEM((model, shared_unit), bf),
            pltpu.VMEM((model, shared_unit), bf),
            pltpu.VMEM((shared_unit, model), bf),
            pltpu.VMEM(mixer_output_weight.shape, bf),
            pltpu.VMEM(queries.shape, bf),
            pltpu.VMEM(queries.shape, bf),
            pltpu.VMEM(queries.shape, bf),
            pltpu.VMEM((tokens, model), bf),
            pltpu.VMEM((top_k, slot_count, tokens), bf),
            pltpu.VMEM((top_k, tokens, 1), f32),
            pltpu.VMEM((count, 1, SPAN), f32),
            pltpu.VMEM((count, 1, SPAN), f32),
            pltpu.VMEM(quarter, bf),
            pltpu.VMEM(slot_shape, bf),
            pltpu.VMEM(slot_shape, bf),
            pltpu.VMEM((4, slot_count, unit), bf),
            pltpu.VMEM(slot_shape, bf),
            pltpu.VMEM(slot_shape, bf),
            pltpu.VMEM(quarter, bf),
            pltpu.VMEM((2, tokens, model), bf),
            pltpu.VMEM((tokens, model), bf),
            pltpu.VMEM((tokens, model), bf),
            pltpu.VMEM(quarter, bf),
            pltpu.VMEM((2, tokens, model), bf),
            pltpu.VMEM((tokens, model), bf),
            pltpu.VMEM((tokens, model), bf),
            pltpu.VMEM((heads, count, SPAN, 1), f32),
            pltpu.VMEM((heads, count, 1, SPAN), f32),
            pltpu.VMEM((heads, count, SPAN, 1), f32),
            pltpu.VMEM((heads, length, width), f32),
            pltpu.VMEM((heads, length, width), f32),
            pltpu.VMEM((heads, width, 2 * width), f32),
            pltpu.VMEM((heads, width, 2 * width), bf),
            pltpu.VMEM((heads, width, 2 * width), bf),
            pltpu.VMEM((heads, width, 2 * width), f32),
            pltpu.VMEM((heads, width, width), bf),
            pltpu.VMEM((heads, width, width), bf),
            pltpu.VMEM((heads, width, width), f32),
            pltpu.VMEM((length, heads * width), bf),
            dma((12,)),
            dma((3 + CUTS, 3)),
            dma((3 + CUTS, 3)),
            dma((devices - 1,)),
            dma((devices - 1,)),
            dma((CUTS, devices - 1)),
            dma((CUTS, devices - 1)),
            dma((CUTS,)),
            dma((2, 3)),
            dma((2, 3)),
            dma((3,)),
            dma((2,)),
        ],
        compiler_params=pltpu.CompilerParams(
            collective_id=0, has_side_effects=True, vmem_limit_bytes=62 << 20
        ),
    )(
        decay_gate_logits.T,
        correction_logits.T,
        head_decay_speed.reshape(1, heads),
        position_log_decay.T,
        head_output_gain.reshape(1, width),
        expert_norm_gain.reshape(1, model),
        routes.T,
        chosen_expert_weight.T,
        queries,
        keys,
        values,
        expert_input_tokens,
        mixer_output_weight,
        routed_gate_weight[0],
        routed_up_weight[0],
        routed_down_weight[0],
        common_gate_weight,
        common_up_weight,
        common_down_weight,
    )
    half = pl.BlockSpec((tokens // 2, model), lambda n: (n, 0))
    return pl.pallas_call(
        hand_over,
        grid=(2,),
        in_specs=[half, half],
        out_specs=[half, half],
        out_shape=[jax.ShapeDtypeStruct((tokens, model), bf)] * 2,
    )(mixed, routed)


def shards(*args):
    devices, members = lax.axis_size("ep"), lax.axis_size("tp")
    routes, tokens = args[11], args[9]
    capacity = 3 * routes.shape[0] * routes.shape[1] // (2 * devices)
    whole_tiles = capacity % 16 == 0 and tokens.shape[1] % (128 * CUTS) == 0
    if members == 4 and devices % 2 == 0 and whole_tiles:
        return fused_shards(*args)
    return plain_shards(*args)


def solution(mesh):
    return jax.shard_map(
        shards,
        mesh=mesh,
        in_specs=(
            P("ep", "tp"),
            P("ep", "tp"),
            P("ep", "tp"),
            P("ep", "tp"),
            P("ep", "tp"),
            P("tp"),
            P("ep", "tp"),
            P(),
            P("tp", None),
            P(("ep", "tp"), None),
            P(),
            P(("ep", "tp"), None),
            P(("ep", "tp"), None),
            P("ep", None, "tp"),
            P("ep", None, "tp"),
            P("ep", "tp", None),
            P(None, "tp"),
            P(None, "tp"),
            P("tp", None),
        ),
        out_specs=(P(("ep", "tp"), None), P(("ep", "tp"), None)),
        check_vma=False,
    )
```

```python
import functools

import jax
import jax.numpy as jnp
from jax import lax
from jax.experimental import pallas as pl
from jax.experimental.pallas import tpu as pltpu
from jax.sharding import PartitionSpec as P


EPS = 1e-06


SPAN = 64


def halves(x):
    high = x.astype(jnp.bfloat16)
    return high, (x - high.astype(jnp.float32)).astype(jnp.bfloat16)


def product(left, right, numbers):
    left_high, left_low = halves(left)
    right_high, right_low = halves(right)

    def dot(x, y):
        return lax.dot_general(x, y, numbers, preferred_element_type=jnp.float32)

    return dot(left_high, right_high) + (dot(left_high, right_low) + dot(left_low, right_high))


def bmm(left, right, dims):
    return product(left, right, (dims, ((0,), (0,))))


def mm(left, right):
    return product(left, right, (((1,), (0,)), ((), ())))


def unit_lower_inverse(lower, rows, cols):
    inverse = jnp.where(rows == cols, 1.0, 0.0) - jnp.where(
        ((rows >> 1) == (cols >> 1)), lower, 0.0
    )
    level = 1
    while (1 << level) < SPAN:
        below = ((rows >> (level + 1)) == (cols >> (level + 1))) & (
            (rows >> level) != (cols >> level)
        )
        part = jnp.where(below, lower, 0.0)
        inverse = inverse - bmm(bmm(inverse, part, ((2,), (1,))), inverse, ((2,), (1,)))
        level += 1
    return inverse


def local_kernel(q_ref, k_ref, v_ref, ccol_ref, crow_ref, bcol_ref, g_ref, z_ref, total_ref):
    width = q_ref.shape[1]
    count = q_ref.shape[0] // SPAN
    shape = (count, SPAN, width)
    q = q_ref[...].astype(jnp.float32)
    k = k_ref[...].astype(jnp.float32)
    v = v_ref[...].astype(jnp.float32).reshape(shape)
    q = q * lax.rsqrt(jnp.sum(q * q, axis=-1, keepdims=True) + EPS) * width ** (-0.5)
    k = k * lax.rsqrt(jnp.sum(k * k, axis=-1, keepdims=True) + EPS)
    q = q.reshape(shape)
    k = k.reshape(shape)
    ccol = ccol_ref[0].reshape(count, SPAN, 1)
    crow = crow_ref[0]
    bcol = bcol_ref[0].reshape(count, SPAN, 1)
    rows = lax.broadcasted_iota(jnp.int32, (count, SPAN, SPAN), 1)
    cols = lax.broadcasted_iota(jnp.int32, (count, SPAN, SPAN), 2)
    decay = jnp.exp(jnp.where(rows >= cols, ccol - crow, -jnp.inf))
    keyed = k * bcol
    lower = jnp.where(rows > cols, bmm(keyed, k, ((2,), (2,))) * decay, 0.0)
    inverse = unit_lower_inverse(lower, rows, cols)
    grown = jnp.exp(ccol)
    solved = bmm(
        inverse, jnp.concatenate([keyed * grown, v * bcol], axis=-1), ((2,), (1,))
    )
    scores = bmm(q, k, ((2,), (2,))) * decay
    q_scaled = q * grown
    last = ccol[:, SPAN - 1 :, :]
    carried = k * jnp.exp(last - ccol)
    mixed = bmm(scores, solved, ((2,), (1,)))
    readout = q_scaled - mixed[:, :, :width]
    eye_r = lax.broadcasted_iota(jnp.int32, (width, width), 0)
    eye_c = lax.broadcasted_iota(jnp.int32, (width, width), 1)
    eye = jnp.where(eye_r == eye_c, 1.0, 0.0)
    state = jnp.concatenate([eye, jnp.zeros_like(eye)], axis=1)
    for n in range(count):
        seen = mm(readout[n], state)
        g_ref[0, n * SPAN : (n + 1) * SPAN, :] = seen[:, :width]
        z_ref[0, n * SPAN : (n + 1) * SPAN, :] = seen[:, width:] + mixed[n][:, width:]
        both = mm(carried[n].T, solved[n])
        trans = jnp.exp(last[n]) * eye - both[:, :width]
        state = mm(trans, state)
        state = jnp.concatenate([state[:, :width], state[:, width:] + both[:, width:]], axis=1)
    total_ref[0] = state.astype(jnp.bfloat16)


def finish_kernel(place_ref, gathered_ref, g_ref, z_ref, gain_ref, out_ref):
    width = g_ref.shape[2]

    def one(turn, state):
        both = gathered_ref[turn, 0].astype(jnp.float32)
        return mm(both[:, :width], state) + both[:, width:]

    state = lax.fori_loop(0, place_ref[0], one, jnp.zeros((width, width), jnp.float32))
    out = mm(g_ref[0], state) + z_ref[0]
    out = out * lax.rsqrt(jnp.mean(out * out, axis=-1, keepdims=True) + EPS) * gain_ref[...]
    out_ref[...] = out.astype(jnp.bfloat16)


def token_mixer_heads(
    queries,
    keys,
    values,
    decay_gate_logits,
    correction_logits,
    head_decay_speed,
    position_log_decay,
    head_output_gain,
):
    heads = decay_gate_logits.shape[1]
    length = queries.shape[0]
    width = queries.shape[1] // heads
    count = length // SPAN
    log_gate = -head_decay_speed * jax.nn.softplus(decay_gate_logits) + position_log_decay
    log_gate = log_gate.T.reshape(heads, count, SPAN)
    at = jnp.arange(SPAN)
    cum = jnp.sum(
        jnp.where(at[:, None] >= at[None, :], log_gate[:, :, None, :], 0.0), axis=-1
    )
    beta = jax.nn.sigmoid(correction_logits.astype(jnp.float32)).T.reshape(heads, length, 1)
    by_head = pl.BlockSpec((length, width), lambda h: (0, h))
    column = pl.BlockSpec((1, length, 1), lambda h: (h, 0, 0))
    whole = pl.BlockSpec((1, length, width), lambda h: (h, 0, 0))
    local_call = pl.pallas_call(
        local_kernel,
        grid=(heads,),
        in_specs=[
            by_head,
            by_head,
            by_head,
            column,
            pl.BlockSpec((1, count, 1, SPAN), lambda h: (h, 0, 0, 0)),
            column,
        ],
        out_specs=[whole, whole, pl.BlockSpec((1, width, 2 * width), lambda h: (h, 0, 0))],
        out_shape=[
            jax.ShapeDtypeStruct((heads, length, width), jnp.float32),
            jax.ShapeDtypeStruct((heads, length, width), jnp.float32),
            jax.ShapeDtypeStruct((heads, width, 2 * width), jnp.bfloat16),
        ],
        cost_estimate=pl.CostEstimate(
            flops=3_000_000_000, bytes_accessed=4_000_000, transcendentals=200_000
        ),
    )
    readout, local_out, total = local_call(
        queries,
        keys,
        values,
        cum.reshape(heads, length, 1),
        cum.reshape(heads, count, 1, SPAN),
        beta,
    )
    gathered = lax.all_gather(total, "ep")
    place = lax.axis_index("ep").astype(jnp.int32).reshape(1)
    devices = gathered.shape[0]
    return pl.pallas_call(
        finish_kernel,
        grid=(heads,),
        in_specs=[
            pl.BlockSpec(memory_space=pltpu.SMEM),
            pl.BlockSpec((devices, 1, width, 2 * width), lambda h: (0, h, 0, 0)),
            whole,
            whole,
            pl.BlockSpec((1, width), lambda h: (0, 0)),
        ],
        out_specs=by_head,
        out_shape=jax.ShapeDtypeStruct((length, heads * width), jnp.bfloat16),
        cost_estimate=pl.CostEstimate(
            flops=500_000_000, bytes_accessed=4_000_000, transcendentals=2_000
        ),
    )(place, gathered, readout, local_out, head_output_gain.reshape(1, width))


def norm_rows(expert_input_tokens, expert_norm_gain):
    rows_f = expert_input_tokens.astype(jnp.float32)
    scaled = (
        rows_f
        * lax.rsqrt(jnp.mean(rows_f * rows_f, axis=-1, keepdims=True) + EPS)
        * expert_norm_gain
    )
    return scaled.astype(jnp.bfloat16)


def gated_hidden(rows_in, w_gate, w_up):
    gate_val = jnp.dot(rows_in, w_gate, preferred_element_type=jnp.float32)
    up_val = jnp.dot(rows_in, w_up, preferred_element_type=jnp.float32)
    return (jax.nn.silu(gate_val) * up_val).astype(jnp.bfloat16)


def slot_layout(routes, capacity):
    flat = routes.reshape(-1)
    at = jnp.arange(flat.shape[0], dtype=jnp.int32)
    same = (flat[:, None] == flat[None, :]) & (at[None, :] < at[:, None])
    before = jnp.sum(same.astype(jnp.int32), axis=1)
    return (flat * capacity + before).reshape(routes.shape)


def plain_shards(
    queries,
    keys,
    values,
    decay_gate_logits,
    correction_logits,
    head_decay_speed,
    position_log_decay,
    head_output_gain,
    mixer_output_weight,
    expert_input_tokens,
    expert_norm_gain,
    routes,
    chosen_expert_weight,
    routed_gate_weight,
    routed_up_weight,
    routed_down_weight,
    common_gate_weight,
    common_up_weight,
    common_down_weight,
):
    normed = token_mixer_heads(
        queries,
        keys,
        values,
        decay_gate_logits,
        correction_logits,
        head_decay_speed,
        position_log_decay,
        head_output_gain,
    )
    mixer_out = lax.psum_scatter(
        jnp.dot(normed, mixer_output_weight, preferred_element_type=jnp.float32).astype(
            jnp.bfloat16
        ),
        "tp",
        scatter_dimension=0,
        tiled=True,
    )
    normed_in = norm_rows(expert_input_tokens, expert_norm_gain)
    tokens_own, top_k = routes.shape
    model_width = expert_input_tokens.shape[1]
    experts = lax.axis_size("ep")
    capacity = 3 * tokens_own * top_k // (2 * experts)
    slot_count = experts * capacity
    slots = slot_layout(routes, capacity)
    numbers = jnp.arange(slot_count, dtype=jnp.int32)
    sends = sum(
        (slots[None, :, k] == numbers[:, None]).astype(jnp.bfloat16) for k in range(top_k)
    )
    outgoing = jnp.dot(sends, normed_in, preferred_element_type=jnp.float32).astype(
        jnp.bfloat16
    )
    arrived = lax.all_to_all(
        outgoing.reshape(experts, capacity, model_width),
        "ep",
        split_axis=0,
        concat_axis=0,
        tiled=True,
    ).reshape(slot_count, model_width)
    gate_all = lax.all_gather(routed_gate_weight[0], "tp")
    up_all = lax.all_gather(routed_up_weight[0], "tp")
    down_all = lax.all_gather(routed_down_weight[0], "tp", axis=0, tiled=True)
    hidden = jnp.concatenate(
        [gated_hidden(arrived, gate_all[t], up_all[t]) for t in range(gate_all.shape[0])],
        axis=1,
    )
    slot_sums = jnp.dot(hidden, down_all, preferred_element_type=jnp.float32).astype(
        jnp.bfloat16
    )
    returned = lax.all_to_all(
        slot_sums.reshape(experts, capacity, model_width),
        "ep",
        split_axis=0,
        concat_axis=0,
        tiled=True,
    ).reshape(slot_count, model_width)
    shared_hidden = gated_hidden(
        lax.all_gather(normed_in, "tp", axis=0, tiled=True), common_gate_weight, common_up_weight
    )
    shared = lax.psum_scatter(
        jnp.dot(shared_hidden, common_down_weight, preferred_element_type=jnp.float32).astype(
            jnp.bfloat16
        ),
        "tp",
        scatter_dimension=0,
        tiled=True,
    ).astype(jnp.float32)
    weights = sum(
        jnp.where(
            slots[:, k : k + 1] == numbers[None, :], chosen_expert_weight[:, k : k + 1], 0.0
        )
        for k in range(top_k)
    )
    coarse = weights.astype(jnp.bfloat16)
    fine = (weights - coarse.astype(jnp.float32)).astype(jnp.bfloat16)
    routed = jnp.dot(coarse, returned, preferred_element_type=jnp.float32) + jnp.dot(
        fine, returned, preferred_element_type=jnp.float32
    )
    moe_out = (shared + routed).astype(jnp.bfloat16)
    return (mixer_out, moe_out)


MESH = pl.DeviceIdType.MESH
CUTS = 8
OWN, CORE, CROSS, FAR = range(4)


def scaled_rows(rows, gain):
    rows_f = rows.astype(jnp.float32)
    norm = lax.rsqrt(jnp.mean(rows_f * rows_f, axis=-1, keepdims=True) + EPS)
    return (rows_f * norm * gain).astype(jnp.bfloat16)


def silu_product(gate_val, up_val):
    return (gate_val / (1.0 + jnp.exp(-gate_val)) * up_val).astype(jnp.bfloat16)


def fused_kernel(
    devices,
    decay_ref,
    correct_ref,
    speed_ref,
    log_ref,
    head_gain_ref,
    gain_ref,
    routes_ref,
    chosen_ref,
    q_hbm,
    k_hbm,
    v_hbm,
    tok_hbm,
    mixw_hbm,
    rg_hbm,
    ru_hbm,
    rd_hbm,
    cg_hbm,
    cu_hbm,
    cd_hbm,
    mix_ref,
    moe_ref,
    wg,
    wu,
    wd,
    cg,
    cu,
    dn,
    mw,
    q_ref,
    k_ref,
    v_ref,
    tok_ref,
    hits_ref,
    weight_ref,
    lrow_s,
    brow_s,
    toks,
    sh_hid,
    sh_in,
    outgoing,
    arrived,
    hid,
    slot_out,
    returned,
    shared,
    mx_part,
    mx_in,
    mx_cross,
    mx_far,
    ccol_s,
    crow_s,
    bcol_s,
    gs,
    zs,
    tot,
    tot_bf,
    pair_in,
    pair_tot,
    s_in,
    s_out,
    state_s,
    normed,
    local_sem,
    w_send,
    w_recv,
    d_send,
    d_recv,
    r_send,
    r_recv,
    r_local,
    rs_send,
    rs_recv,
    c_send,
    c_recv,
    sx_send,
    sx_recv,
    sc_send,
    sc_recv,
    z_send,
    z_recv,
    zf_send,
    y_send,
    y_recv,
    f_send,
    f_recv,
    h_send,
    h_recv,
    o_sem,
    mix_s,
    moe_s,
):
    e = lax.axis_index("ep")
    t = lax.axis_index("tp")
    heads = decay_ref.shape[0]
    width = q_ref.shape[1] // heads
    length = q_ref.shape[0]
    count = length // SPAN
    tokens, model = tok_ref.shape
    top_k = routes_ref.shape[0]
    capacity = arrived.shape[1]
    slots = devices * capacity
    unit = wg.shape[2]
    cut = model // CUTS
    core_t = t + 1 - 2 * (t % 2)
    core = (e, core_t)
    cross = (e, (t + 2) % 4)
    line = devices // 2
    half = line // 2
    z = e // 2
    y = e % 2
    inner = z % half
    mine = z - inner
    other = half - mine
    beside = (2 * z + 1 - y, t)

    def remote(src, dst, send, recv, peer):
        return pltpu.make_async_remote_copy(
            src_ref=src,
            dst_ref=dst,
            send_sem=send,
            recv_sem=recv,
            device_id=peer,
            device_id_type=MESH,
        )

    near = [
        2 * (mine + (inner + o) % half) + (y + d) % 2
        for o in range(half)
        for d in range(2)
        if (o, d) != (0, 0)
    ]
    distant = [
        2 * (other + (inner + o) % half) + (y + d) % 2 for o in range(half) for d in range(2)
    ]
    peers = distant + near

    early = [
        pltpu.make_async_copy(src, dst, local_sem.at[8 + n])
        for n, (src, dst) in enumerate(
            ((tok_hbm, tok_ref), (q_hbm, q_ref), (k_hbm, k_ref), (v_hbm, v_ref))
        )
    ]
    locals_ = [
        pltpu.make_async_copy(src, dst, local_sem.at[n])
        for n, (src, dst) in enumerate(
            (
                (cg_hbm, cg),
                (cu_hbm, cu),
                (cd_hbm, dn.at[OWN]),
                (rg_hbm, wg.at[OWN]),
                (ru_hbm, wu.at[OWN]),
                (rd_hbm, wd.at[OWN]),
                (mixw_hbm, mw),
            )
        )
    ]
    for copy in early:
        copy.start()

    barrier = pltpu.get_barrier_semaphore()
    for o in range(1, devices):
        pl.semaphore_signal(
            barrier, inc=1, device_id=((e + o) % devices, t), device_id_type=MESH
        )
    for o in range(1, 4):
        pl.semaphore_signal(barrier, inc=1, device_id=(e, (t + o) % 4), device_id_type=MESH)

    expert = lax.broadcasted_iota(jnp.int32, (devices, tokens), 0)
    earlier = lax.broadcasted_iota(jnp.int32, (tokens, tokens), 0)
    earlier = jnp.where(
        earlier < lax.broadcasted_iota(jnp.int32, (tokens, tokens), 1), 1.0, 0.0
    ).astype(jnp.bfloat16)
    number = lax.broadcasted_iota(jnp.int32, (slots, tokens), 0).astype(jnp.float32)
    base = jnp.zeros((devices, 1), jnp.float32)
    sends = jnp.zeros((slots, tokens), jnp.bfloat16)
    token_a = lax.broadcasted_iota(jnp.int32, (tokens, tokens), 0)
    token_b = lax.broadcasted_iota(jnp.int32, (tokens, tokens), 1)
    for n in range(top_k):
        route = routes_ref[n : n + 1, :]
        chosen = jnp.where(expert == route, 1.0, 0.0)
        before = base + jnp.dot(
            chosen.astype(jnp.bfloat16), earlier, preferred_element_type=jnp.float32
        )
        base = base + jnp.sum(chosen, axis=1, keepdims=True)
        slot = route.astype(jnp.float32) * capacity + jnp.sum(
            chosen * before, axis=0, keepdims=True
        )
        hit = jnp.where(number == slot, 1.0, 0.0).astype(jnp.bfloat16)
        sends = sends + hit
        hits_ref[n] = hit
        weight_ref[n] = jnp.sum(
            jnp.where(token_a == token_b, chosen_ref[n : n + 1, :], 0.0), axis=1, keepdims=True
        )

    pl.semaphore_wait(barrier, devices + 2)

    def cols(j):
        return pl.ds(pl.multiple_of(j * cut, cut), cut)

    def spread(i, src, place):
        remote(src, place(CROSS), w_send.at[i, 0], w_recv.at[i, 0], cross).start()
        remote(src, place(CORE), w_send.at[i, 1], w_recv.at[i, 1], core).start()

    def forward(i, place):
        remote(place(CROSS), place(CROSS), w_send.at[i, 0], w_recv.at[i, 0], cross).wait_recv()
        remote(place(CROSS), place(FAR), w_send.at[i, 2], w_recv.at[i, 2], core).start()

    def take(i, place):
        remote(place(CORE), place(CORE), w_send.at[i, 1], w_recv.at[i, 1], core).wait_recv()
        remote(place(FAR), place(FAR), w_send.at[i, 2], w_recv.at[i, 2], core).wait_recv()

    def sent(i, place):
        remote(place(CROSS), place(CROSS), w_send.at[i, 0], w_recv.at[i, 0], cross).wait_send()
        remote(place(CORE), place(CORE), w_send.at[i, 1], w_recv.at[i, 1], core).wait_send()
        remote(place(FAR), place(FAR), w_send.at[i, 2], w_recv.at[i, 2], core).wait_send()

    def gate_at(r):
        return wg.at[r]

    def up_at(r):
        return wu.at[r]

    def down_at(j):
        return lambda r: wd.at[r, :, cols(j)]

    def tok_at(r):
        return toks.at[r]

    slices = [remote(cd_hbm.at[e], dn.at[CROSS, e], sx_send, sx_recv, cross)]
    for copy in slices:
        copy.start()
    spread(0, rg_hbm, gate_at)
    spread(1, ru_hbm, up_at)

    def spread_down(j, carry):
        spread(2 + j, rd_hbm.at[:, cols(j)], down_at(j))
        return carry

    ahead = 5 * CUTS // 8
    lax.fori_loop(0, ahead, spread_down, 0)
    spread(2 + CUTS, tok_hbm, tok_at)
    lax.fori_loop(ahead, CUTS, spread_down, 0)
    shared_core = [remote(cd_hbm, dn.at[CORE], sc_send, sc_recv, core)]
    for copy in shared_core:
        copy.start()
    for copy in locals_:
        copy.start()

    early[0].wait()
    toks[OWN] = scaled_rows(tok_ref[...], gain_ref[...])
    outgoing[...] = (
        jnp.dot(sends, toks[OWN], preferred_element_type=jnp.float32)
        .astype(jnp.bfloat16)
        .reshape(outgoing.shape)
    )

    rows = lax.broadcasted_iota(jnp.int32, (count, SPAN, SPAN), 1)
    cols_at = lax.broadcasted_iota(jnp.int32, (count, SPAN, SPAN), 2)
    for h in range(heads):
        logit = decay_ref[h : h + 1, :]
        softplus = jnp.maximum(logit, 0.0) + jnp.log1p(jnp.exp(-jnp.abs(logit)))
        log_gate = -speed_ref[0:1, h : h + 1] * softplus + log_ref[h : h + 1, :]
        beta = 1.0 / (1.0 + jnp.exp(-correct_ref[h : h + 1, :].astype(jnp.float32)))
        for n in range(count):
            lrow_s[n] = log_gate[:, n * SPAN : (n + 1) * SPAN]
            brow_s[n] = beta[:, n * SPAN : (n + 1) * SPAN]
        ccol = jnp.sum(jnp.where(rows >= cols_at, lrow_s[...], 0.0), axis=2, keepdims=True)
        ccol_s[h] = ccol
        crow_s[h] = jnp.sum(jnp.where(rows == cols_at, ccol, 0.0), axis=1, keepdims=True)
        bcol_s[h] = jnp.sum(
            jnp.where(rows == cols_at, brow_s[...], 0.0), axis=2, keepdims=True
        )

    def dispatch(n):
        peer = peers[n]
        return remote(outgoing.at[peer], arrived.at[e], d_send.at[n], d_recv.at[n], (peer, t))

    for n in range(len(peers)):
        dispatch(n).start()
    own_rows = pltpu.make_async_copy(outgoing.at[e], arrived.at[e], local_sem.at[7])
    own_rows.start()

    def local_head(h, carry):
        at = pl.ds(pl.multiple_of(h * width, width), width)
        shape = (count, SPAN, width)
        q = q_ref[:, at].astype(jnp.float32)
        k = k_ref[:, at].astype(jnp.float32)
        v = v_ref[:, at].astype(jnp.float32).reshape(shape)
        q = q * lax.rsqrt(jnp.sum(q * q, axis=-1, keepdims=True) + EPS) * width ** (-0.5)
        k = k * lax.rsqrt(jnp.sum(k * k, axis=-1, keepdims=True) + EPS)
        q = q.reshape(shape)
        k = k.reshape(shape)
        ccol = ccol_s[h]
        crow = crow_s[h]
        bcol = bcol_s[h]
        decay = jnp.exp(jnp.where(rows >= cols_at, ccol - crow, -jnp.inf))
        keyed = k * bcol
        lower = jnp.where(rows > cols_at, bmm(keyed, k, ((2,), (2,))) * decay, 0.0)
        inverse = unit_lower_inverse(lower, rows, cols_at)
        grown = jnp.exp(ccol)
        solved = bmm(
            inverse, jnp.concatenate([keyed * grown, v * bcol], axis=-1), ((2,), (1,))
        )
        scores = bmm(q, k, ((2,), (2,))) * decay
        q_scaled = q * grown
        last = ccol[:, SPAN - 1 :, :]
        carried = k * jnp.exp(last - ccol)
        mixed = bmm(scores, solved, ((2,), (1,)))
        readout = q_scaled - mixed[:, :, :width]
        eye_r = lax.broadcasted_iota(jnp.int32, (width, width), 0)
        eye_c = lax.broadcasted_iota(jnp.int32, (width, width), 1)
        eye = jnp.where(eye_r == eye_c, 1.0, 0.0)
        state = jnp.concatenate([eye, jnp.zeros_like(eye)], axis=1)
        for n in range(count):
            seen = mm(readout[n], state)
            gs[h, n * SPAN : (n + 1) * SPAN, :] = seen[:, :width]
            zs[h, n * SPAN : (n + 1) * SPAN, :] = seen[:, width:] + mixed[n][:, width:]
            both = mm(carried[n].T, solved[n])
            trans = jnp.exp(last[n]) * eye - both[:, :width]
            state = mm(trans, state)
            state = jnp.concatenate([state[:, :width], state[:, width:] + both[:, width:]], axis=1)
        tot[h] = state
        tot_bf[h] = state.astype(jnp.bfloat16)
        return carry

    for copy in early[1:]:
        copy.wait()
    lax.fori_loop(0, heads, local_head, 0)

    def piece(i, r, send, recv, peer):
        return [remote(dn.at[CROSS, i], dn.at[r, i], send, recv, peer)]

    def along(at, n, place):
        i = 2 * at + y
        return piece(i, CROSS, z_send.at[n], z_recv.at[at], (2 * place + y, t))

    def hand_on(o, n, at):
        place = mine + (inner + o) % half
        return piece(
            2 * at + y,
            CROSS,
            zf_send.at[(o - 1) * half + n],
            z_recv.at[at],
            (2 * place + y, t),
        )

    def aside(at):
        return piece(2 * at + y, CROSS, y_send.at[at], y_recv.at[at], beside)

    def to_core(i):
        return piece(i, FAR, f_send.at[i], f_recv.at[i], core)

    def share(at):
        for copy in aside(at) + to_core(2 * at + y):
            copy.start()

    half_places = [mine + (inner + o) % half for o in range(half)]
    far_places = [other + (inner + o) % half for o in range(half)]
    middle = half - z // half
    is_middle = jnp.logical_or(z == half - 1, z == half)

    def line_copies():
        copies = along(z, 0, middle)
        for o in range(1, half):
            copies += along(z, o, half_places[o])
        return copies

    pair = z
    to_odd = remote(tot_bf, pair_in, c_send.at[0], c_recv.at[0], beside)
    next_odd = ((e + 2) % devices, t)
    next_even = ((e + 1) % devices, t)
    hands_on = jnp.logical_and(y == 1, pair < line - 1)
    to_next_odd = remote(s_out, s_in, c_send.at[1], c_recv.at[1], next_odd)
    to_next_even = remote(s_out, s_in, c_send.at[2], c_recv.at[1], next_even)

    @pl.when(y == 0)
    def _():
        to_odd.start()

    @pl.when(y == 1)
    def _():
        to_odd.wait_recv()
        for h in range(heads):
            both = mm(tot[h][:, :width], pair_in[h].astype(jnp.float32))
            pair_tot[h, :, :width] = both[:, :width]
            pair_tot[h, :, width:] = both[:, width:] + tot[h][:, width:]

    @pl.when(pair == 0)
    def _():
        s_in[...] = jnp.zeros_like(s_in)

    @pl.when(jnp.logical_and(hands_on, pair == 0))
    def _():
        s_out[...] = pair_tot[:, :, width:].astype(jnp.bfloat16)
        to_next_odd.start()
        to_next_even.start()

    late = jnp.logical_and(z > 0, z < half)
    for copy in slices:
        copy.wait_recv()
    share(z)

    @pl.when(jnp.logical_not(late))
    def _():
        for copy in line_copies():
            copy.start()

    forward(0, gate_at)
    for n in range(3, 6):
        locals_[n].wait()
    for i in (0, 1):
        remote(
            wg.at[CORE], wg.at[CORE], w_send.at[i, 1], w_recv.at[i, 1], core
        ).wait_recv()

    own_rows.wait()
    for n in range(len(peers)):
        dispatch(n).wait_recv()

    def hidden_of(r, carry):
        rows_in = arrived[...].reshape(slots, model)
        hid[r] = silu_product(
            jnp.dot(rows_in, wg[r], preferred_element_type=jnp.float32),
            jnp.dot(rows_in, wu[r], preferred_element_type=jnp.float32),
        )
        return carry

    lax.fori_loop(OWN, CORE + 1, hidden_of, 0)

    @pl.when(pair > 0)
    def _():
        to_next_odd.wait_recv()

    @pl.when(jnp.logical_and(hands_on, pair > 0))
    def _():
        for h in range(heads):
            s_out[h] = (
                mm(pair_tot[h][:, :width], s_in[h].astype(jnp.float32)) + pair_tot[h][:, width:]
            ).astype(jnp.bfloat16)
        to_next_odd.start()
        to_next_even.start()

    @pl.when(late)
    def _():
        for copy in line_copies():
            copy.start()

    @pl.when(y == 1)
    def _():
        for h in range(heads):
            state_s[h] = mm(
                pair_in[h][:, :width].astype(jnp.float32), s_in[h].astype(jnp.float32)
            ) + pair_in[h][:, width:].astype(jnp.float32)

    @pl.when(y == 0)
    def _():
        state_s[...] = s_in[...].astype(jnp.float32)

    for h in range(heads):
        out = mm(gs[h], state_s[h]) + zs[h]
        out = out * lax.rsqrt(jnp.mean(out * out, axis=-1, keepdims=True) + EPS)
        normed[:, h * width : (h + 1) * width] = (out * head_gain_ref[...]).astype(jnp.bfloat16)
    locals_[6].wait()
    for r, owner in enumerate((t, core_t, (t + 2) % 4, (core_t + 2) % 4)):
        block = pl.ds(pl.multiple_of(owner * tokens, tokens), tokens)
        mx_part[r] = jnp.dot(
            normed[block, :], mw[...], preferred_element_type=jnp.float32
        ).astype(jnp.bfloat16)
    to_peer = [
        remote(mx_part.at[r], mx_in.at[1 - i], rs_send.at[i], rs_recv.at[i], core)
        for i, r in enumerate((FAR, CORE))
    ]
    for copy in to_peer:
        copy.start()

    def line_wait(at):
        for copy in along(at, 0, z):
            copy.wait_recv()

    for o in range(1, half):
        line_wait(half_places[o])
        share(half_places[o])

    @pl.when(is_middle)
    def _():
        for n in range(half):
            line_wait(far_places[n])
            for o in range(1, half):
                for copy in hand_on(o, n, far_places[n]):
                    copy.start()
            share(far_places[n])

    forward(1, up_at)
    for i in (0, 1):
        remote(wg.at[FAR], wg.at[FAR], w_send.at[i, 2], w_recv.at[i, 2], core).wait_recv()
    lax.fori_loop(CROSS, FAR + 1, hidden_of, 0)

    def return_of(n, j):
        peer = peers[n]
        return remote(
            slot_out.at[peer, :, cols(j)],
            returned.at[e, :, cols(j)],
            r_send.at[j, n],
            r_recv.at[j, n],
            (peer, t),
        )

    def own_return(j):
        return pltpu.make_async_copy(
            slot_out.at[e, :, cols(j)], returned.at[e, :, cols(j)], r_local.at[j]
        )

    def down_of(j, carry):
        place = down_at(j)
        forward(2 + j, place)
        take(2 + j, place)
        hidden = jnp.concatenate([hid[r] for r in range(4)], axis=1)
        weight = wd[:, :, cols(j)].reshape(4 * unit, cut)
        slot_out[:, :, cols(j)] = (
            jnp.dot(hidden, weight, preferred_element_type=jnp.float32)
            .astype(jnp.bfloat16)
            .reshape(devices, capacity, cut)
        )
        for n in range(len(peers)):
            return_of(n, j).start()
        own_return(j).start()
        return carry

    lax.fori_loop(0 * CUTS // 8, 2 * CUTS // 8, down_of, 0)

    @pl.when(jnp.logical_not(is_middle))
    def _():
        for n in range(half):
            line_wait(far_places[n])
            share(far_places[n])

    lax.fori_loop(2 * CUTS // 8, ahead, down_of, 0)
    forward(2 + CUTS, tok_at)
    for n in range(2):
        locals_[n].wait()
    take(2 + CUTS, tok_at)
    remote(tok_at(FAR), tok_at(FAR), w_send.at[2 + CUTS, 2], w_recv.at[2 + CUTS, 2], core).wait_send()
    gain = gain_ref[...]
    for r in (CORE, CROSS, FAR):
        toks[r] = scaled_rows(toks[r], gain)
    x_all = toks[...].reshape(4 * tokens, model)
    sh_hid[...] = silu_product(
        jnp.dot(x_all, cg[...], preferred_element_type=jnp.float32),
        jnp.dot(x_all, cu[...], preferred_element_type=jnp.float32),
    ).reshape(sh_hid.shape)
    hidden_out = [
        remote(sh_hid.at[r], sh_in.at[r], h_send.at[r - 1], h_recv.at[r - 1], peer)
        for r, peer in ((CORE, core), (CROSS, cross), (FAR, (e, (core_t + 2) % 4)))
    ]
    for copy in hidden_out:
        copy.start()

    to_peer[0].wait_recv()
    mx_cross[...] = (mx_part[CROSS].astype(jnp.float32) + mx_in[1].astype(jnp.float32)).astype(
        jnp.bfloat16
    )
    over = remote(mx_cross, mx_far, rs_send.at[2], rs_recv.at[2], cross)
    over.start()
    for at in range(line):
        for copy in piece(2 * at + 1 - y, CROSS, y_send.at[at], y_recv.at[at], beside):
            copy.wait_recv()
        for copy in to_core(2 * at + 1 - y):
            copy.start()
    lax.fori_loop(ahead, CUTS, down_of, 0)

    def moe_out(j):
        return pltpu.make_async_copy(moe_s.at[:, cols(j)], moe_ref.at[:, cols(j)], o_sem.at[j])

    mix_out = pltpu.make_async_copy(mix_s, mix_ref, local_sem.at[12])

    def combine(j, carry):
        for n in range(len(peers)):
            return_of(n, j).wait_recv()
        own_return(j).wait()
        back = returned[:, :, cols(j)].reshape(slots, cut)
        routed = sum(
            weight_ref[n]
            * lax.dot_general(
                hits_ref[n], back, (((0,), (0,)), ((), ())), preferred_element_type=jnp.float32
            )
            for n in range(top_k)
        )
        moe_s[:, cols(j)] = (shared[:, cols(j)] + routed).astype(jnp.bfloat16)
        moe_out(j).start()
        return carry

    locals_[2].wait()
    shared_core[0].wait_recv()
    for i in range(devices):
        for copy in to_core(i):
            copy.wait_recv()
    for copy in hidden_out:
        copy.wait_recv()
    sh_in[OWN] = sh_hid[OWN]
    shared[...] = jnp.dot(
        jnp.concatenate([sh_in[r] for r in range(4)], axis=1),
        dn[...].reshape(4 * dn.shape[1] * dn.shape[2], model),
        preferred_element_type=jnp.float32,
    )

    lax.fori_loop(0, CUTS, combine, 0)
    to_peer[1].wait_recv()
    over.wait_recv()
    mix_s[...] = (
        mx_part[OWN].astype(jnp.float32)
        + mx_in[0].astype(jnp.float32)
        + mx_far[...].astype(jnp.float32)
    ).astype(jnp.bfloat16)
    mix_out.start()
    sent(0, gate_at)
    sent(1, up_at)
    remote(toks.at[CROSS], toks.at[CROSS], w_send.at[2 + CUTS, 0], w_recv.at[2 + CUTS, 0], cross).wait_send()
    remote(toks.at[CORE], toks.at[CORE], w_send.at[2 + CUTS, 1], w_recv.at[2 + CUTS, 1], core).wait_send()

    def down_sent(j, carry):
        sent(2 + j, down_at(j))
        for n in range(len(peers)):
            return_of(n, j).wait_send()
        moe_out(j).wait()
        return carry

    lax.fori_loop(0, CUTS, down_sent, 0)
    for n in range(len(peers)):
        dispatch(n).wait_send()
    for copy in slices + shared_core + to_peer + line_copies() + hidden_out + [over]:
        copy.wait_send()
    for at in range(line):
        for copy in aside(at):
            copy.wait_send()
    for i in range(devices):
        for copy in to_core(i):
            copy.wait_send()

    mix_out.wait()

    @pl.when(is_middle)
    def _():
        for n in range(half):
            for o in range(1, half):
                for copy in hand_on(o, n, far_places[n]):
                    copy.wait_send()

    @pl.when(y == 0)
    def _():
        to_odd.wait_send()

    @pl.when(hands_on)
    def _():
        to_next_odd.wait_send()
        to_next_even.wait_send()


def hand_over(mixed_hbm, routed_hbm, mixer_out_hbm, moe_out_hbm, held, in_sem, out_sem):
    pieces, rows = held.shape[0], held.shape[1]
    each = pieces // 2
    ins, outs = [], []
    for n in range(pieces):
        src, dst = ((mixed_hbm, mixer_out_hbm), (routed_hbm, moe_out_hbm))[n // each]
        at = pl.ds(n % each * rows, rows)
        ins.append(pltpu.make_async_copy(src.at[at], held.at[n], in_sem.at[n]))
        outs.append(pltpu.make_async_copy(held.at[n], dst.at[at], out_sem.at[n]))
    for copy in ins:
        copy.start()
    for taken, given in zip(ins, outs):
        taken.wait()
        given.start()
    for copy in outs:
        copy.wait()


def fused_shards(
    queries,
    keys,
    values,
    decay_gate_logits,
    correction_logits,
    head_decay_speed,
    position_log_decay,
    head_output_gain,
    mixer_output_weight,
    expert_input_tokens,
    expert_norm_gain,
    routes,
    chosen_expert_weight,
    routed_gate_weight,
    routed_up_weight,
    routed_down_weight,
    common_gate_weight,
    common_up_weight,
    common_down_weight,
):
    devices = lax.axis_size("ep")
    tokens, top_k = routes.shape
    model = expert_input_tokens.shape[1]
    length = queries.shape[0]
    heads = decay_gate_logits.shape[1]
    width = queries.shape[1] // heads
    count = length // SPAN
    unit = routed_gate_weight.shape[2]
    shared_unit = common_gate_weight.shape[1]
    capacity = 3 * tokens * top_k // (2 * devices)
    slot_count = devices * capacity
    bf, f32 = jnp.bfloat16, jnp.float32
    vmem = pl.BlockSpec(memory_space=pltpu.VMEM)
    anywhere = pl.BlockSpec(memory_space=pl.ANY)
    dma = pltpu.SemaphoreType.DMA
    line = devices // 2
    half = line // 2
    slot_shape = (devices, capacity, model)
    mixed, routed = pl.pallas_call(
        functools.partial(fused_kernel, devices),
        in_specs=[vmem] * 8 + [anywhere] * 11,
        out_specs=[anywhere, anywhere],
        out_shape=[jax.ShapeDtypeStruct((tokens, model), bf)] * 2,
        scratch_shapes=[
            pltpu.VMEM((4, model, unit), bf),
            pltpu.VMEM((4, model, unit), bf),
            pltpu.VMEM((4, unit, model), bf),
            pltpu.VMEM(common_gate_weight.shape, bf),
            pltpu.VMEM(common_up_weight.shape, bf),
            pltpu.VMEM((4, devices, shared_unit // devices, model), bf),
            pltpu.VMEM(mixer_output_weight.shape, bf),
            pltpu.VMEM(queries.shape, bf),
            pltpu.VMEM(queries.shape, bf),
            pltpu.VMEM(queries.shape, bf),
            pltpu.VMEM((tokens, model), bf),
            pltpu.VMEM((top_k, slot_count, tokens), bf),
            pltpu.VMEM((top_k, tokens, 1), f32),
            pltpu.VMEM((count, 1, SPAN), f32),
            pltpu.VMEM((count, 1, SPAN), f32),
            pltpu.VMEM((4, tokens, model), bf),
            pltpu.VMEM((4, tokens, shared_unit), bf),
            pltpu.VMEM((4, tokens, shared_unit), bf),
            pltpu.VMEM(slot_shape, bf),
            pltpu.VMEM(slot_shape, bf),
            pltpu.VMEM((4, slot_count, unit), bf),
            pltpu.VMEM(slot_shape, bf),
            pltpu.VMEM(slot_shape, bf),
            pltpu.VMEM((tokens, model), f32),
            pltpu.VMEM((4, tokens, model), bf),
            pltpu.VMEM((2, tokens, model), bf),
            pltpu.VMEM((tokens, model), bf),
            pltpu.VMEM((tokens, model), bf),
            pltpu.VMEM((heads, count, SPAN, 1), f32),
            pltpu.VMEM((heads, count, 1, SPAN), f32),
            pltpu.VMEM((heads, count, SPAN, 1), f32),
            pltpu.VMEM((heads, length, width), f32),
            pltpu.VMEM((heads, length, width), f32),
            pltpu.VMEM((heads, width, 2 * width), f32),
            pltpu.VMEM((heads, width, 2 * width), bf),
            pltpu.VMEM((heads, width, 2 * width), bf),
            pltpu.VMEM((heads, width, 2 * width), f32),
            pltpu.VMEM((heads, width, width), bf),
            pltpu.VMEM((heads, width, width), bf),
            pltpu.VMEM((heads, width, width), f32),
            pltpu.VMEM((length, heads * width), bf),
            dma((13,)),
            dma((3 + CUTS, 3)),
            dma((3 + CUTS, 3)),
            dma((devices - 1,)),
            dma((devices - 1,)),
            dma((CUTS, devices - 1)),
            dma((CUTS, devices - 1)),
            dma((CUTS,)),
            dma((3,)),
            dma((3,)),
            dma((3,)),
            dma((2,)),
            dma,
            dma,
            dma,
            dma,
            dma((half,)),
            dma((line,)),
            dma((half * half,)),
            dma((line,)),
            dma((line,)),
            dma((devices,)),
            dma((devices,)),
            dma((3,)),
            dma((3,)),
            dma((CUTS,)),
            pltpu.VMEM((tokens, model), bf),
            pltpu.VMEM((tokens, model), bf),
        ],
        compiler_params=pltpu.CompilerParams(
            collective_id=0, has_side_effects=True, vmem_limit_bytes=62 << 20
        ),
    )(
        decay_gate_logits.T,
        correction_logits.T,
        head_decay_speed.reshape(1, heads),
        position_log_decay.T,
        head_output_gain.reshape(1, width),
        expert_norm_gain.reshape(1, model),
        routes.T,
        chosen_expert_weight.T,
        queries,
        keys,
        values,
        expert_input_tokens,
        mixer_output_weight,
        routed_gate_weight[0],
        routed_up_weight[0],
        routed_down_weight[0],
        common_gate_weight,
        common_up_weight,
        common_down_weight.reshape(devices, shared_unit // devices, model),
    )
    return pl.pallas_call(
        hand_over,
        in_specs=[anywhere] * 2,
        out_specs=[anywhere] * 2,
        out_shape=[jax.ShapeDtypeStruct((tokens, model), bf)] * 2,
        scratch_shapes=[pltpu.VMEM((8, tokens // 4, model), bf), dma((8,)), dma((8,))],
    )(mixed, routed)


def shards(*args):
    devices, members = lax.axis_size("ep"), lax.axis_size("tp")
    routes, tokens = args[11], args[9]
    capacity = 3 * routes.shape[0] * routes.shape[1] // (2 * devices)
    whole_tiles = capacity % 16 == 0 and tokens.shape[1] % (128 * CUTS) == 0
    whole_tiles = whole_tiles and args[16].shape[1] % (16 * devices) == 0
    whole_tiles = whole_tiles and args[16].shape[1] == args[13].shape[2]
    if members == 4 and devices % 4 == 0 and whole_tiles:
        return fused_shards(*args)
    return plain_shards(*args)


def solution(mesh):
    return jax.shard_map(
        shards,
        mesh=mesh,
        in_specs=(
            P("ep", "tp"),
            P("ep", "tp"),
            P("ep", "tp"),
            P("ep", "tp"),
            P("ep", "tp"),
            P("tp"),
            P("ep", "tp"),
            P(),
            P("tp", None),
            P(("ep", "tp"), None),
            P(),
            P(("ep", "tp"), None),
            P(("ep", "tp"), None),
            P("ep", None, "tp"),
            P("ep", None, "tp"),
            P("ep", "tp", None),
            P(None, "tp"),
            P(None, "tp"),
            P("tp", None),
        ),
        out_specs=(P(("ep", "tp"), None), P(("ep", "tp"), None)),
        check_vma=False,
    )
```

```python
import functools

import jax
import jax.numpy as jnp
from jax import lax
from jax.experimental import pallas as pl
from jax.experimental.pallas import tpu as pltpu
from jax.sharding import PartitionSpec as P


EPS = 1e-06


SPAN = 64


def halves(x):
    high = x.astype(jnp.bfloat16)
    return high, (x - high.astype(jnp.float32)).astype(jnp.bfloat16)


def product(left, right, numbers):
    left_high, left_low = halves(left)
    right_high, right_low = halves(right)

    def dot(x, y):
        return lax.dot_general(x, y, numbers, preferred_element_type=jnp.float32)

    return dot(left_high, right_high) + (dot(left_high, right_low) + dot(left_low, right_high))


def bmm(left, right, dims):
    return product(left, right, (dims, ((0,), (0,))))


def mm(left, right):
    return product(left, right, (((1,), (0,)), ((), ())))


def unit_lower_inverse(lower, rows, cols):
    inverse = jnp.where(rows == cols, 1.0, 0.0) - jnp.where(
        ((rows >> 1) == (cols >> 1)), lower, 0.0
    )
    level = 1
    while (1 << level) < SPAN:
        below = ((rows >> (level + 1)) == (cols >> (level + 1))) & (
            (rows >> level) != (cols >> level)
        )
        part = jnp.where(below, lower, 0.0)
        inverse = inverse - bmm(bmm(inverse, part, ((2,), (1,))), inverse, ((2,), (1,)))
        level += 1
    return inverse


def local_kernel(q_ref, k_ref, v_ref, ccol_ref, crow_ref, bcol_ref, g_ref, z_ref, total_ref):
    width = q_ref.shape[1]
    count = q_ref.shape[0] // SPAN
    shape = (count, SPAN, width)
    q = q_ref[...].astype(jnp.float32)
    k = k_ref[...].astype(jnp.float32)
    v = v_ref[...].astype(jnp.float32).reshape(shape)
    q = q * lax.rsqrt(jnp.sum(q * q, axis=-1, keepdims=True) + EPS) * width ** (-0.5)
    k = k * lax.rsqrt(jnp.sum(k * k, axis=-1, keepdims=True) + EPS)
    q = q.reshape(shape)
    k = k.reshape(shape)
    ccol = ccol_ref[0].reshape(count, SPAN, 1)
    crow = crow_ref[0]
    bcol = bcol_ref[0].reshape(count, SPAN, 1)
    rows = lax.broadcasted_iota(jnp.int32, (count, SPAN, SPAN), 1)
    cols = lax.broadcasted_iota(jnp.int32, (count, SPAN, SPAN), 2)
    decay = jnp.exp(jnp.where(rows >= cols, ccol - crow, -jnp.inf))
    keyed = k * bcol
    lower = jnp.where(rows > cols, bmm(keyed, k, ((2,), (2,))) * decay, 0.0)
    inverse = unit_lower_inverse(lower, rows, cols)
    grown = jnp.exp(ccol)
    solved = bmm(
        inverse, jnp.concatenate([keyed * grown, v * bcol], axis=-1), ((2,), (1,))
    )
    scores = bmm(q, k, ((2,), (2,))) * decay
    q_scaled = q * grown
    last = ccol[:, SPAN - 1 :, :]
    carried = k * jnp.exp(last - ccol)
    mixed = bmm(scores, solved, ((2,), (1,)))
    readout = q_scaled - mixed[:, :, :width]
    eye_r = lax.broadcasted_iota(jnp.int32, (width, width), 0)
    eye_c = lax.broadcasted_iota(jnp.int32, (width, width), 1)
    eye = jnp.where(eye_r == eye_c, 1.0, 0.0)
    state = jnp.concatenate([eye, jnp.zeros_like(eye)], axis=1)
    for n in range(count):
        seen = mm(readout[n], state)
        g_ref[0, n * SPAN : (n + 1) * SPAN, :] = seen[:, :width]
        z_ref[0, n * SPAN : (n + 1) * SPAN, :] = seen[:, width:] + mixed[n][:, width:]
        both = mm(carried[n].T, solved[n])
        trans = jnp.exp(last[n]) * eye - both[:, :width]
        state = mm(trans, state)
        state = jnp.concatenate([state[:, :width], state[:, width:] + both[:, width:]], axis=1)
    total_ref[0] = state.astype(jnp.bfloat16)


def finish_kernel(place_ref, gathered_ref, g_ref, z_ref, gain_ref, out_ref):
    width = g_ref.shape[2]

    def one(turn, state):
        both = gathered_ref[turn, 0].astype(jnp.float32)
        return mm(both[:, :width], state) + both[:, width:]

    state = lax.fori_loop(0, place_ref[0], one, jnp.zeros((width, width), jnp.float32))
    out = mm(g_ref[0], state) + z_ref[0]
    out = out * lax.rsqrt(jnp.mean(out * out, axis=-1, keepdims=True) + EPS) * gain_ref[...]
    out_ref[...] = out.astype(jnp.bfloat16)


def token_mixer_heads(
    queries,
    keys,
    values,
    decay_gate_logits,
    correction_logits,
    head_decay_speed,
    position_log_decay,
    head_output_gain,
):
    heads = decay_gate_logits.shape[1]
    length = queries.shape[0]
    width = queries.shape[1] // heads
    count = length // SPAN
    log_gate = -head_decay_speed * jax.nn.softplus(decay_gate_logits) + position_log_decay
    log_gate = log_gate.T.reshape(heads, count, SPAN)
    at = jnp.arange(SPAN)
    cum = jnp.sum(
        jnp.where(at[:, None] >= at[None, :], log_gate[:, :, None, :], 0.0), axis=-1
    )
    beta = jax.nn.sigmoid(correction_logits.astype(jnp.float32)).T.reshape(heads, length, 1)
    by_head = pl.BlockSpec((length, width), lambda h: (0, h))
    column = pl.BlockSpec((1, length, 1), lambda h: (h, 0, 0))
    whole = pl.BlockSpec((1, length, width), lambda h: (h, 0, 0))
    local_call = pl.pallas_call(
        local_kernel,
        grid=(heads,),
        in_specs=[
            by_head,
            by_head,
            by_head,
            column,
            pl.BlockSpec((1, count, 1, SPAN), lambda h: (h, 0, 0, 0)),
            column,
        ],
        out_specs=[whole, whole, pl.BlockSpec((1, width, 2 * width), lambda h: (h, 0, 0))],
        out_shape=[
            jax.ShapeDtypeStruct((heads, length, width), jnp.float32),
            jax.ShapeDtypeStruct((heads, length, width), jnp.float32),
            jax.ShapeDtypeStruct((heads, width, 2 * width), jnp.bfloat16),
        ],
        cost_estimate=pl.CostEstimate(
            flops=3_000_000_000, bytes_accessed=4_000_000, transcendentals=200_000
        ),
    )
    readout, local_out, total = local_call(
        queries,
        keys,
        values,
        cum.reshape(heads, length, 1),
        cum.reshape(heads, count, 1, SPAN),
        beta,
    )
    gathered = lax.all_gather(total, "ep")
    place = lax.axis_index("ep").astype(jnp.int32).reshape(1)
    devices = gathered.shape[0]
    return pl.pallas_call(
        finish_kernel,
        grid=(heads,),
        in_specs=[
            pl.BlockSpec(memory_space=pltpu.SMEM),
            pl.BlockSpec((devices, 1, width, 2 * width), lambda h: (0, h, 0, 0)),
            whole,
            whole,
            pl.BlockSpec((1, width), lambda h: (0, 0)),
        ],
        out_specs=by_head,
        out_shape=jax.ShapeDtypeStruct((length, heads * width), jnp.bfloat16),
        cost_estimate=pl.CostEstimate(
            flops=500_000_000, bytes_accessed=4_000_000, transcendentals=2_000
        ),
    )(place, gathered, readout, local_out, head_output_gain.reshape(1, width))


def norm_rows(expert_input_tokens, expert_norm_gain):
    rows_f = expert_input_tokens.astype(jnp.float32)
    scaled = (
        rows_f
        * lax.rsqrt(jnp.mean(rows_f * rows_f, axis=-1, keepdims=True) + EPS)
        * expert_norm_gain
    )
    return scaled.astype(jnp.bfloat16)


def gated_hidden(rows_in, w_gate, w_up):
    gate_val = jnp.dot(rows_in, w_gate, preferred_element_type=jnp.float32)
    up_val = jnp.dot(rows_in, w_up, preferred_element_type=jnp.float32)
    return (jax.nn.silu(gate_val) * up_val).astype(jnp.bfloat16)


def slot_layout(routes, capacity):
    flat = routes.reshape(-1)
    at = jnp.arange(flat.shape[0], dtype=jnp.int32)
    same = (flat[:, None] == flat[None, :]) & (at[None, :] < at[:, None])
    before = jnp.sum(same.astype(jnp.int32), axis=1)
    return (flat * capacity + before).reshape(routes.shape)


def plain_shards(
    queries,
    keys,
    values,
    decay_gate_logits,
    correction_logits,
    head_decay_speed,
    position_log_decay,
    head_output_gain,
    mixer_output_weight,
    expert_input_tokens,
    expert_norm_gain,
    routes,
    chosen_expert_weight,
    routed_gate_weight,
    routed_up_weight,
    routed_down_weight,
    common_gate_weight,
    common_up_weight,
    common_down_weight,
):
    normed = token_mixer_heads(
        queries,
        keys,
        values,
        decay_gate_logits,
        correction_logits,
        head_decay_speed,
        position_log_decay,
        head_output_gain,
    )
    mixer_out = lax.psum_scatter(
        jnp.dot(normed, mixer_output_weight, preferred_element_type=jnp.float32).astype(
            jnp.bfloat16
        ),
        "tp",
        scatter_dimension=0,
        tiled=True,
    )
    normed_in = norm_rows(expert_input_tokens, expert_norm_gain)
    tokens_own, top_k = routes.shape
    model_width = expert_input_tokens.shape[1]
    experts = lax.axis_size("ep")
    capacity = 3 * tokens_own * top_k // (2 * experts)
    slot_count = experts * capacity
    slots = slot_layout(routes, capacity)
    numbers = jnp.arange(slot_count, dtype=jnp.int32)
    sends = sum(
        (slots[None, :, k] == numbers[:, None]).astype(jnp.bfloat16) for k in range(top_k)
    )
    outgoing = jnp.dot(sends, normed_in, preferred_element_type=jnp.float32).astype(
        jnp.bfloat16
    )
    arrived = lax.all_to_all(
        outgoing.reshape(experts, capacity, model_width),
        "ep",
        split_axis=0,
        concat_axis=0,
        tiled=True,
    ).reshape(slot_count, model_width)
    gate_all = lax.all_gather(routed_gate_weight[0], "tp")
    up_all = lax.all_gather(routed_up_weight[0], "tp")
    down_all = lax.all_gather(routed_down_weight[0], "tp", axis=0, tiled=True)
    hidden = jnp.concatenate(
        [gated_hidden(arrived, gate_all[t], up_all[t]) for t in range(gate_all.shape[0])],
        axis=1,
    )
    slot_sums = jnp.dot(hidden, down_all, preferred_element_type=jnp.float32).astype(
        jnp.bfloat16
    )
    returned = lax.all_to_all(
        slot_sums.reshape(experts, capacity, model_width),
        "ep",
        split_axis=0,
        concat_axis=0,
        tiled=True,
    ).reshape(slot_count, model_width)
    shared_hidden = gated_hidden(
        lax.all_gather(normed_in, "tp", axis=0, tiled=True), common_gate_weight, common_up_weight
    )
    shared = lax.psum_scatter(
        jnp.dot(shared_hidden, common_down_weight, preferred_element_type=jnp.float32).astype(
            jnp.bfloat16
        ),
        "tp",
        scatter_dimension=0,
        tiled=True,
    ).astype(jnp.float32)
    weights = sum(
        jnp.where(
            slots[:, k : k + 1] == numbers[None, :], chosen_expert_weight[:, k : k + 1], 0.0
        )
        for k in range(top_k)
    )
    coarse = weights.astype(jnp.bfloat16)
    fine = (weights - coarse.astype(jnp.float32)).astype(jnp.bfloat16)
    routed = jnp.dot(coarse, returned, preferred_element_type=jnp.float32) + jnp.dot(
        fine, returned, preferred_element_type=jnp.float32
    )
    moe_out = (shared + routed).astype(jnp.bfloat16)
    return (mixer_out, moe_out)


MESH = pl.DeviceIdType.MESH
CUTS = 8
OWN, CORE, CROSS, FAR = range(4)


def scaled_rows(rows, gain):
    rows_f = rows.astype(jnp.float32)
    norm = lax.rsqrt(jnp.mean(rows_f * rows_f, axis=-1, keepdims=True) + EPS)
    return (rows_f * norm * gain).astype(jnp.bfloat16)


def silu_product(gate_val, up_val):
    return (gate_val / (1.0 + jnp.exp(-gate_val)) * up_val).astype(jnp.bfloat16)


def fused_kernel(
    devices,
    decay_ref,
    correct_ref,
    speed_ref,
    log_ref,
    head_gain_ref,
    gain_ref,
    routes_ref,
    chosen_ref,
    q_hbm,
    k_hbm,
    v_hbm,
    tok_hbm,
    mixw_hbm,
    rg_hbm,
    ru_hbm,
    rd_hbm,
    cg_hbm,
    cu_hbm,
    cd_hbm,
    mix_ref,
    moe_ref,
    wg,
    wu,
    wd,
    cg,
    cu,
    dn,
    mw,
    q_ref,
    k_ref,
    v_ref,
    tok_ref,
    hits_ref,
    weight_ref,
    lrow_s,
    brow_s,
    toks,
    sh_hid,
    sh_in,
    outgoing,
    arrived,
    hid,
    slot_out,
    returned,
    shared,
    mx_part,
    mx_in,
    mx_cross,
    mx_far,
    ccol_s,
    crow_s,
    bcol_s,
    gs,
    zs,
    tot,
    tot_bf,
    pair_in,
    pair_tot,
    s_in,
    s_out,
    state_s,
    normed,
    local_sem,
    w_send,
    w_recv,
    p_recv,
    g_recv,
    d_send,
    d_recv,
    r_send,
    r_recv,
    rs_send,
    rs_recv,
    c_send,
    c_recv,
    sx_send,
    sx_recv,
    sc_send,
    sc_recv,
    z_send,
    z_recv,
    zf_send,
    y_send,
    y_recv,
    f_send,
    f_recv,
    h_send,
    h_recv,
    o_sem,
    here_sem,
    go_sem,
    mix_s,
    moe_s,
):
    e = lax.axis_index("ep")
    t = lax.axis_index("tp")
    heads = decay_ref.shape[0]
    width = q_ref.shape[1] // heads
    length = q_ref.shape[0]
    count = length // SPAN
    tokens, model = tok_ref.shape
    top_k = routes_ref.shape[0]
    capacity = arrived.shape[1]
    slots = devices * capacity
    unit = wg.shape[2]
    cut = model // CUTS
    core_t = t + 1 - 2 * (t % 2)
    core = (e, core_t)
    cross = (e, (t + 2) % 4)
    line = devices // 2
    half = line // 2
    z = e // 2
    y = e % 2
    inner = z % half
    mine = z - inner
    other = half - mine
    beside = (2 * z + 1 - y, t)

    def remote(src, dst, send, recv, peer):
        return pltpu.make_async_remote_copy(
            src_ref=src,
            dst_ref=dst,
            send_sem=send,
            recv_sem=recv,
            device_id=peer,
            device_id_type=MESH,
        )

    near = [
        2 * (mine + (inner + o) % half) + (y + d) % 2
        for o in range(half)
        for d in range(2)
        if (o, d) != (0, 0)
    ]
    distant = [
        2 * (other + (inner + o) % half) + (y + d) % 2 for o in range(half) for d in range(2)
    ]
    peers = distant + near

    early = [
        pltpu.make_async_copy(src, dst, local_sem.at[8 + n])
        for n, (src, dst) in enumerate(
            ((tok_hbm, tok_ref), (q_hbm, q_ref), (k_hbm, k_ref), (v_hbm, v_ref))
        )
    ]
    locals_ = [
        pltpu.make_async_copy(src, dst, local_sem.at[n])
        for n, (src, dst) in enumerate(
            (
                (cg_hbm, cg),
                (cu_hbm, cu),
                (cd_hbm, dn.at[OWN]),
                (rg_hbm, wg.at[OWN]),
                (ru_hbm, wu.at[OWN]),
                (rd_hbm, wd.at[OWN]),
                (mixw_hbm, mw),
            )
        )
    ]
    for copy in early:
        copy.start()

    barrier = pltpu.get_barrier_semaphore()
    speaker = t == 3
    for o in range(1, 4):
        member = (t + o) % 4

        @pl.when(member != 3)
        def _():
            pl.semaphore_signal(barrier, inc=1, device_id=(e, member), device_id_type=MESH)

    expert = lax.broadcasted_iota(jnp.int32, (devices, tokens), 0)
    earlier = lax.broadcasted_iota(jnp.int32, (tokens, tokens), 0)
    earlier = jnp.where(
        earlier < lax.broadcasted_iota(jnp.int32, (tokens, tokens), 1), 1.0, 0.0
    ).astype(jnp.bfloat16)
    number = lax.broadcasted_iota(jnp.int32, (slots, tokens), 0).astype(jnp.float32)
    base = jnp.zeros((devices, 1), jnp.float32)
    sends = jnp.zeros((slots, tokens), jnp.bfloat16)
    token_a = lax.broadcasted_iota(jnp.int32, (tokens, tokens), 0)
    token_b = lax.broadcasted_iota(jnp.int32, (tokens, tokens), 1)
    for n in range(top_k):
        route = routes_ref[n : n + 1, :]
        chosen = jnp.where(expert == route, 1.0, 0.0)
        before = base + jnp.dot(
            chosen.astype(jnp.bfloat16), earlier, preferred_element_type=jnp.float32
        )
        base = base + jnp.sum(chosen, axis=1, keepdims=True)
        slot = route.astype(jnp.float32) * capacity + jnp.sum(
            chosen * before, axis=0, keepdims=True
        )
        hit = jnp.where(number == slot, 1.0, 0.0).astype(jnp.bfloat16)
        sends = sends + hit
        hits_ref[n] = hit
        weight_ref[n] = jnp.sum(
            jnp.where(token_a == token_b, chosen_ref[n : n + 1, :], 0.0), axis=1, keepdims=True
        )

    @pl.when(jnp.logical_not(speaker))
    def _():
        pl.semaphore_wait(barrier, 3)
        pl.semaphore_signal(here_sem, inc=1, device_id=(e, 3), device_id_type=MESH)

    @pl.when(speaker)
    def _():
        pl.semaphore_wait(here_sem, 3)
        for o in range(1, devices):
            pl.semaphore_signal(
                barrier, inc=1, device_id=((e + o) % devices, t), device_id_type=MESH
            )


    def cols(j):
        return pl.ds(pl.multiple_of(j * cut, cut), cut)

    def spread(n, i, src, place):
        remote(src, place(CROSS), w_send.at[n], w_recv.at[i], cross).start()
        remote(src, place(CORE), w_send.at[n], p_recv.at[i], core).start()

    def forward(n, i, place):
        remote(place(CROSS), place(CROSS), w_send.at[n], w_recv.at[i], cross).wait_recv()
        remote(place(CROSS), place(FAR), w_send.at[n], p_recv.at[i], core).start()

    def take(i, both):
        remote(both, both, w_send.at[0], p_recv.at[i], core).wait_recv()

    def sent(n, all_of):
        remote(all_of, all_of, w_send.at[n], w_recv.at[0], core).wait_send()

    def gate_at(r):
        return wg.at[r]

    def down_at(j):
        return lambda r: wd.at[r, :, cols(j)]

    slices = [remote(cd_hbm.at[e], dn.at[CROSS, e], sx_send, sx_recv, cross)]
    for copy in slices:
        copy.start()
    spread(0, 0, rg_hbm, gate_at)
    hu = unit // 2
    up_index = (1, 3 + CUTS)
    for n in range(2):
        at = pl.ds(n * hu, hu)
        remote(
            ru_hbm.at[:, at], wu.at[CROSS, :, at], w_send.at[1], w_recv.at[up_index[n]], cross
        ).start()
    remote(ru_hbm, wu.at[CORE], w_send.at[1], p_recv.at[1], core).start()

    def spread_down(j, carry):
        spread(2, 2 + j, rd_hbm.at[:, cols(j)], down_at(j))
        return carry

    ahead = 5 * CUTS // 8
    lax.fori_loop(0, ahead, spread_down, 0)
    remote(tok_hbm, toks.at[CROSS], w_send.at[3], w_recv.at[2 + CUTS], cross).start()
    remote(tok_hbm, toks.at[CORE], w_send.at[3], p_recv.at[2 + CUTS], core).start()
    lax.fori_loop(ahead, CUTS, spread_down, 0)
    shared_core = [remote(cd_hbm, dn.at[CORE], sc_send, sc_recv, core)]
    for copy in shared_core:
        copy.start()
    for copy in locals_:
        copy.start()

    early[0].wait()
    toks[OWN] = scaled_rows(tok_ref[...], gain_ref[...])
    outgoing[...] = (
        jnp.dot(sends, toks[OWN], preferred_element_type=jnp.float32)
        .astype(jnp.bfloat16)
        .reshape(outgoing.shape)
    )

    rows = lax.broadcasted_iota(jnp.int32, (count, SPAN, SPAN), 1)
    cols_at = lax.broadcasted_iota(jnp.int32, (count, SPAN, SPAN), 2)
    for h in range(heads):
        logit = decay_ref[h : h + 1, :]
        softplus = jnp.maximum(logit, 0.0) + jnp.log1p(jnp.exp(-jnp.abs(logit)))
        log_gate = -speed_ref[0:1, h : h + 1] * softplus + log_ref[h : h + 1, :]
        beta = 1.0 / (1.0 + jnp.exp(-correct_ref[h : h + 1, :].astype(jnp.float32)))
        for n in range(count):
            lrow_s[n] = log_gate[:, n * SPAN : (n + 1) * SPAN]
            brow_s[n] = beta[:, n * SPAN : (n + 1) * SPAN]
        ccol = jnp.sum(jnp.where(rows >= cols_at, lrow_s[...], 0.0), axis=2, keepdims=True)
        ccol_s[h] = ccol
        crow_s[h] = jnp.sum(jnp.where(rows == cols_at, ccol, 0.0), axis=1, keepdims=True)
        bcol_s[h] = jnp.sum(
            jnp.where(rows == cols_at, brow_s[...], 0.0), axis=2, keepdims=True
        )

    def dispatch(n):
        peer = peers[n]
        return remote(outgoing.at[peer], arrived.at[e], d_send, d_recv, (peer, t))

    @pl.when(speaker)
    def _():
        pl.semaphore_wait(barrier, devices - 1)
        for o in range(3):
            pl.semaphore_signal(go_sem, inc=1, device_id=(e, o), device_id_type=MESH)

    @pl.when(jnp.logical_not(speaker))
    def _():
        pl.semaphore_wait(go_sem, 1)

    for n in range(len(peers)):
        dispatch(n).start()
    own_rows = pltpu.make_async_copy(outgoing.at[e], arrived.at[e], d_recv)
    own_rows.start()

    def local_head(h, carry):
        at = pl.ds(pl.multiple_of(h * width, width), width)
        shape = (count, SPAN, width)
        q = q_ref[:, at].astype(jnp.float32)
        k = k_ref[:, at].astype(jnp.float32)
        v = v_ref[:, at].astype(jnp.float32).reshape(shape)
        q = q * lax.rsqrt(jnp.sum(q * q, axis=-1, keepdims=True) + EPS) * width ** (-0.5)
        k = k * lax.rsqrt(jnp.sum(k * k, axis=-1, keepdims=True) + EPS)
        q = q.reshape(shape)
        k = k.reshape(shape)
        ccol = ccol_s[h]
        crow = crow_s[h]
        bcol = bcol_s[h]
        decay = jnp.exp(jnp.where(rows >= cols_at, ccol - crow, -jnp.inf))
        keyed = k * bcol
        lower = jnp.where(rows > cols_at, bmm(keyed, k, ((2,), (2,))) * decay, 0.0)
        inverse = unit_lower_inverse(lower, rows, cols_at)
        grown = jnp.exp(ccol)
        solved = bmm(
            inverse, jnp.concatenate([keyed * grown, v * bcol], axis=-1), ((2,), (1,))
        )
        scores = bmm(q, k, ((2,), (2,))) * decay
        q_scaled = q * grown
        last = ccol[:, SPAN - 1 :, :]
        carried = k * jnp.exp(last - ccol)
        mixed = bmm(scores, solved, ((2,), (1,)))
        readout = q_scaled - mixed[:, :, :width]
        eye_r = lax.broadcasted_iota(jnp.int32, (width, width), 0)
        eye_c = lax.broadcasted_iota(jnp.int32, (width, width), 1)
        eye = jnp.where(eye_r == eye_c, 1.0, 0.0)
        state = jnp.concatenate([eye, jnp.zeros_like(eye)], axis=1)
        for n in range(count):
            seen = mm(readout[n], state)
            gs[h, n * SPAN : (n + 1) * SPAN, :] = seen[:, :width]
            zs[h, n * SPAN : (n + 1) * SPAN, :] = seen[:, width:] + mixed[n][:, width:]
            both = mm(carried[n].T, solved[n])
            trans = jnp.exp(last[n]) * eye - both[:, :width]
            state = mm(trans, state)
            state = jnp.concatenate([state[:, :width], state[:, width:] + both[:, width:]], axis=1)
        tot[h] = state
        tot_bf[h] = state.astype(jnp.bfloat16)
        return carry

    for copy in early[1:]:
        copy.wait()
    lax.fori_loop(0, heads, local_head, 0)

    def piece(i, r, send, recv, peer):
        return [remote(dn.at[CROSS, i], dn.at[r, i], send, recv, peer)]

    def along(at, place):
        i = 2 * at + y
        return piece(i, CROSS, z_send, z_recv.at[at], (2 * place + y, t))

    def hand_on(o, at):
        place = mine + (inner + o) % half
        return piece(
            2 * at + y,
            CROSS,
            zf_send,
            z_recv.at[at],
            (2 * place + y, t),
        )

    def aside(at):
        return piece(2 * at + y, CROSS, y_send, y_recv.at[at], beside)

    def to_core(i):
        return piece(i, FAR, f_send, f_recv, core)

    def share(at):
        for copy in aside(at) + to_core(2 * at + y):
            copy.start()

    half_places = [mine + (inner + o) % half for o in range(half)]
    far_places = [other + (inner + o) % half for o in range(half)]
    middle = half - z // half
    is_middle = jnp.logical_or(z == half - 1, z == half)

    def line_copies():
        copies = along(z, middle)
        for o in range(1, half):
            copies += along(z, half_places[o])
        return copies

    pair = z
    to_odd = remote(tot_bf, pair_in, c_send.at[0], c_recv.at[0], beside)
    next_odd = ((e + 2) % devices, t)
    next_even = ((e + 1) % devices, t)
    hands_on = jnp.logical_and(y == 1, pair < line - 1)
    to_next_odd = remote(s_out, s_in, c_send.at[1], c_recv.at[1], next_odd)
    to_next_even = remote(s_out, s_in, c_send.at[2], c_recv.at[1], next_even)

    @pl.when(y == 0)
    def _():
        to_odd.start()

    @pl.when(y == 1)
    def _():
        to_odd.wait_recv()
        for h in range(heads):
            both = mm(tot[h][:, :width], pair_in[h].astype(jnp.float32))
            pair_tot[h, :, :width] = both[:, :width]
            pair_tot[h, :, width:] = both[:, width:] + tot[h][:, width:]

    @pl.when(pair == 0)
    def _():
        s_in[...] = jnp.zeros_like(s_in)

    @pl.when(jnp.logical_and(hands_on, pair == 0))
    def _():
        s_out[...] = pair_tot[:, :, width:].astype(jnp.bfloat16)
        to_next_odd.start()
        to_next_even.start()

    for copy in slices:
        copy.wait_recv()
    share(z)

    for copy in line_copies():
        copy.start()

    remote(wg.at[CROSS], wg.at[CROSS], w_send.at[0], w_recv.at[0], cross).wait_recv()
    remote(wg.at[CROSS], wg.at[FAR], w_send.at[0], g_recv.at[0], core).start()
    for n in range(3, 6):
        locals_[n].wait()
    take(0, wg.at[CORE])
    take(1, wu.at[CORE])

    remote(arrived, arrived, d_send, d_recv, core).wait_recv()

    def hidden_of(r, carry):
        rows_in = arrived[...].reshape(slots, model)
        hid[r] = silu_product(
            jnp.dot(rows_in, wg[r], preferred_element_type=jnp.float32),
            jnp.dot(rows_in, wu[r], preferred_element_type=jnp.float32),
        )
        return carry

    lax.fori_loop(OWN, CORE + 1, hidden_of, 0)

    def hidden_half(n):
        at = slice(n * hu, (n + 1) * hu)
        rows_in = arrived[...].reshape(slots, model)
        value = silu_product(
            *(
                jnp.dot(
                    rows_in,
                    jnp.concatenate([bank[CROSS, :, at], bank[FAR, :, at]], axis=1),
                    preferred_element_type=jnp.float32,
                )
                for bank in (wg, wu)
            )
        )
        hid[CROSS, :, at] = value[:, :hu]
        hid[FAR, :, at] = value[:, hu:]

    def far_half(n):
        at = pl.ds(n * hu, hu)
        there, here = wu.at[CROSS, :, at], wu.at[FAR, :, at]
        remote(there, there, w_send.at[1], w_recv.at[up_index[n]], cross).wait_recv()
        remote(there, here, w_send.at[1], g_recv.at[1 + n], core).start()
        if n == 0:
            remote(wg.at[FAR], wg.at[FAR], w_send.at[0], g_recv.at[0], core).wait_recv()
        remote(here, here, w_send.at[1], g_recv.at[1 + n], core).wait_recv()
        hidden_half(n)

    far_half(0)

    @pl.when(jnp.logical_and(hands_on, pair > 0))
    def _():
        to_next_odd.wait_recv()
        for h in range(heads):
            s_out[h] = (
                mm(pair_tot[h][:, :width], s_in[h].astype(jnp.float32)) + pair_tot[h][:, width:]
            ).astype(jnp.bfloat16)
        to_next_odd.start()
        to_next_even.start()

    def line_wait(at):
        for copy in along(at, z):
            copy.wait_recv()

    for o in range(1, half):
        line_wait(half_places[o])
        share(half_places[o])

    @pl.when(is_middle)
    def _():
        for n in range(half):
            line_wait(far_places[n])
            for o in range(1, half):
                for copy in hand_on(o, far_places[n]):
                    copy.start()
            share(far_places[n])

    far_half(1)

    def return_of(n, j):
        peer = peers[n]
        return remote(
            slot_out.at[peer, :, cols(j)],
            returned.at[e, :, cols(j)],
            r_send,
            r_recv.at[j],
            (peer, t),
        )

    def own_return(j):
        return pltpu.make_async_copy(
            slot_out.at[e, :, cols(j)], returned.at[e, :, cols(j)], r_recv.at[j]
        )

    def down_of(j, carry):
        place = down_at(j)
        forward(2, 2 + j, place)
        take(2 + j, wd.at[pl.ds(0, 2), :, cols(j)])
        hidden = jnp.concatenate([hid[r] for r in range(4)], axis=1)
        weight = wd[:, :, cols(j)].reshape(4 * unit, cut)
        slot_out[:, :, cols(j)] = (
            jnp.dot(hidden, weight, preferred_element_type=jnp.float32)
            .astype(jnp.bfloat16)
            .reshape(devices, capacity, cut)
        )
        for n in range(len(peers)):
            return_of(n, j).start()
        own_return(j).start()
        return carry

    lax.fori_loop(0 * CUTS // 8, 2 * CUTS // 8, down_of, 0)
    lax.fori_loop(2 * CUTS // 8, ahead, down_of, 0)

    @pl.when(jnp.logical_and(jnp.logical_not(hands_on), pair > 0))
    def _():
        to_next_odd.wait_recv()

    @pl.when(y == 1)
    def _():
        for h in range(heads):
            state_s[h] = mm(
                pair_in[h][:, :width].astype(jnp.float32), s_in[h].astype(jnp.float32)
            ) + pair_in[h][:, width:].astype(jnp.float32)

    @pl.when(y == 0)
    def _():
        state_s[...] = s_in[...].astype(jnp.float32)

    for h in range(heads):
        out = mm(gs[h], state_s[h]) + zs[h]
        out = out * lax.rsqrt(jnp.mean(out * out, axis=-1, keepdims=True) + EPS)
        normed[:, h * width : (h + 1) * width] = (out * head_gain_ref[...]).astype(jnp.bfloat16)
    locals_[6].wait()
    for r, owner in enumerate((t, core_t, (t + 2) % 4, (core_t + 2) % 4)):
        block = pl.ds(pl.multiple_of(owner * tokens, tokens), tokens)
        mx_part[r] = jnp.dot(
            normed[block, :], mw[...], preferred_element_type=jnp.float32
        ).astype(jnp.bfloat16)
    to_peer = [
        remote(mx_part.at[r], mx_in.at[1 - i], rs_send.at[i], rs_recv.at[i], core)
        for i, r in enumerate((FAR, CORE))
    ]
    for copy in to_peer:
        copy.start()

    @pl.when(jnp.logical_not(is_middle))
    def _():
        for n in range(half):
            line_wait(far_places[n])
            share(far_places[n])

    remote(tok_hbm, toks.at[CROSS], w_send.at[3], w_recv.at[2 + CUTS], cross).wait_recv()
    toks_on = remote(toks.at[CROSS], toks.at[FAR], w_send.at[4], p_recv.at[2 + CUTS], core)
    toks_on.start()
    for n in range(2):
        locals_[n].wait()
    take(2 + CUTS, toks.at[pl.ds(0, 2)])
    toks_on.wait_send()
    gain = gain_ref[...]
    for r in (CORE, CROSS, FAR):
        toks[r] = scaled_rows(toks[r], gain)
    x_all = toks[...].reshape(4 * tokens, model)
    sh_hid[...] = silu_product(
        jnp.dot(x_all, cg[...], preferred_element_type=jnp.float32),
        jnp.dot(x_all, cu[...], preferred_element_type=jnp.float32),
    ).reshape(sh_hid.shape)
    hidden_out = [
        remote(sh_hid.at[r], sh_in.at[r], h_send, h_recv, peer)
        for r, peer in ((CORE, core), (CROSS, cross), (FAR, (e, (core_t + 2) % 4)))
    ]
    for copy in hidden_out:
        copy.start()

    to_peer[0].wait_recv()
    mx_cross[...] = (mx_part[CROSS].astype(jnp.float32) + mx_in[1].astype(jnp.float32)).astype(
        jnp.bfloat16
    )
    over = remote(mx_cross, mx_far, rs_send.at[2], rs_recv.at[2], cross)
    over.start()
    for at in range(line):
        for copy in piece(2 * at + 1 - y, CROSS, y_send, y_recv.at[at], beside):
            copy.wait_recv()
        for copy in to_core(2 * at + 1 - y):
            copy.start()
    lax.fori_loop(ahead, CUTS, down_of, 0)

    def moe_out(j):
        return pltpu.make_async_copy(moe_s.at[:, cols(j)], moe_ref.at[:, cols(j)], o_sem)

    mix_out = pltpu.make_async_copy(mix_s, mix_ref, local_sem.at[12])

    def combine(j, carry):
        whole = returned.at[:, :, cols(j)]
        remote(whole, whole, r_send, r_recv.at[j], core).wait_recv()
        back = returned[:, :, cols(j)].reshape(slots, cut)
        routed = sum(
            weight_ref[n]
            * lax.dot_general(
                hits_ref[n], back, (((0,), (0,)), ((), ())), preferred_element_type=jnp.float32
            )
            for n in range(top_k)
        )
        moe_s[:, cols(j)] = (shared[:, cols(j)] + routed).astype(jnp.bfloat16)
        moe_out(j).start()
        return carry

    locals_[2].wait()
    shared_core[0].wait_recv()
    remote(dn.at[FAR], dn.at[FAR], f_send, f_recv, core).wait_recv()
    others = sh_in.at[pl.ds(CORE, 3)]
    remote(others, others, h_send, h_recv, core).wait_recv()
    sh_in[OWN] = sh_hid[OWN]
    shared[...] = jnp.dot(
        jnp.concatenate([sh_in[r] for r in range(4)], axis=1),
        dn[...].reshape(4 * dn.shape[1] * dn.shape[2], model),
        preferred_element_type=jnp.float32,
    )

    lax.fori_loop(0, CUTS, combine, 0)
    to_peer[1].wait_recv()
    over.wait_recv()
    mix_s[...] = (
        mx_part[OWN].astype(jnp.float32)
        + mx_in[0].astype(jnp.float32)
        + mx_far[...].astype(jnp.float32)
    ).astype(jnp.bfloat16)
    mix_out.start()

    def gone(all_of, semaphore):
        remote(all_of, all_of, semaphore, d_recv, core).wait_send()

    sent(0, wg.at[pl.ds(0, 3)])
    sent(1, wu.at[pl.ds(0, 3)])
    sent(2, wd.at[pl.ds(0, 3)])
    sent(3, toks.at[pl.ds(0, 2)])
    gone(arrived.at[pl.ds(1, devices - 1)], d_send)
    gone(slot_out.at[pl.ds(1, devices - 1)], r_send)
    gone(dn.at[FAR, pl.ds(0, half)], z_send)
    gone(dn.at[FAR, pl.ds(0, line)], y_send)
    gone(dn.at[FAR], f_send)
    gone(sh_in.at[pl.ds(CORE, 3)], h_send)
    for copy in slices + shared_core + to_peer + [over]:
        copy.wait_send()
    pltpu.make_async_copy(moe_s, moe_ref, o_sem).wait()
    mix_out.wait()

    @pl.when(is_middle)
    def _():
        gone(dn.at[FAR, pl.ds(0, half * (half - 1))], zf_send)

    @pl.when(y == 0)
    def _():
        to_odd.wait_send()

    @pl.when(hands_on)
    def _():
        to_next_odd.wait_send()
        to_next_even.wait_send()


def hand_over(mixed_hbm, routed_hbm, mixer_out_hbm, moe_out_hbm, held, in_sem, out_sem):
    pieces, rows = held.shape[0], held.shape[1]
    each = pieces // 2
    ins, outs = [], []
    for n in range(pieces):
        src, dst = ((mixed_hbm, mixer_out_hbm), (routed_hbm, moe_out_hbm))[n // each]
        at = pl.ds(n % each * rows, rows)
        ins.append(pltpu.make_async_copy(src.at[at], held.at[n], in_sem.at[n]))
        outs.append(pltpu.make_async_copy(held.at[n], dst.at[at], out_sem.at[n]))
    for copy in ins:
        copy.start()
    for taken, given in zip(ins, outs):
        taken.wait()
        given.start()
    for copy in outs:
        copy.wait()


def fused_shards(
    queries,
    keys,
    values,
    decay_gate_logits,
    correction_logits,
    head_decay_speed,
    position_log_decay,
    head_output_gain,
    mixer_output_weight,
    expert_input_tokens,
    expert_norm_gain,
    routes,
    chosen_expert_weight,
    routed_gate_weight,
    routed_up_weight,
    routed_down_weight,
    common_gate_weight,
    common_up_weight,
    common_down_weight,
):
    devices = lax.axis_size("ep")
    tokens, top_k = routes.shape
    model = expert_input_tokens.shape[1]
    length = queries.shape[0]
    heads = decay_gate_logits.shape[1]
    width = queries.shape[1] // heads
    count = length // SPAN
    unit = routed_gate_weight.shape[2]
    shared_unit = common_gate_weight.shape[1]
    capacity = 3 * tokens * top_k // (2 * devices)
    slot_count = devices * capacity
    bf, f32 = jnp.bfloat16, jnp.float32
    vmem = pl.BlockSpec(memory_space=pltpu.VMEM)
    anywhere = pl.BlockSpec(memory_space=pl.ANY)
    dma = pltpu.SemaphoreType.DMA
    line = devices // 2
    slot_shape = (devices, capacity, model)
    mixed, routed = pl.pallas_call(
        functools.partial(fused_kernel, devices),
        in_specs=[vmem] * 8 + [anywhere] * 11,
        out_specs=[anywhere, anywhere],
        out_shape=[jax.ShapeDtypeStruct((tokens, model), bf)] * 2,
        scratch_shapes=[
            pltpu.VMEM((4, model, unit), bf),
            pltpu.VMEM((4, model, unit), bf),
            pltpu.VMEM((4, unit, model), bf),
            pltpu.VMEM(common_gate_weight.shape, bf),
            pltpu.VMEM(common_up_weight.shape, bf),
            pltpu.VMEM((4, devices, shared_unit // devices, model), bf),
            pltpu.VMEM(mixer_output_weight.shape, bf),
            pltpu.VMEM(queries.shape, bf),
            pltpu.VMEM(queries.shape, bf),
            pltpu.VMEM(queries.shape, bf),
            pltpu.VMEM((tokens, model), bf),
            pltpu.VMEM((top_k, slot_count, tokens), bf),
            pltpu.VMEM((top_k, tokens, 1), f32),
            pltpu.VMEM((count, 1, SPAN), f32),
            pltpu.VMEM((count, 1, SPAN), f32),
            pltpu.VMEM((4, tokens, model), bf),
            pltpu.VMEM((4, tokens, shared_unit), bf),
            pltpu.VMEM((4, tokens, shared_unit), bf),
            pltpu.VMEM(slot_shape, bf),
            pltpu.VMEM(slot_shape, bf),
            pltpu.VMEM((4, slot_count, unit), bf),
            pltpu.VMEM(slot_shape, bf),
            pltpu.VMEM(slot_shape, bf),
            pltpu.VMEM((tokens, model), f32),
            pltpu.VMEM((4, tokens, model), bf),
            pltpu.VMEM((2, tokens, model), bf),
            pltpu.VMEM((tokens, model), bf),
            pltpu.VMEM((tokens, model), bf),
            pltpu.VMEM((heads, count, SPAN, 1), f32),
            pltpu.VMEM((heads, count, 1, SPAN), f32),
            pltpu.VMEM((heads, count, SPAN, 1), f32),
            pltpu.VMEM((heads, length, width), f32),
            pltpu.VMEM((heads, length, width), f32),
            pltpu.VMEM((heads, width, 2 * width), f32),
            pltpu.VMEM((heads, width, 2 * width), bf),
            pltpu.VMEM((heads, width, 2 * width), bf),
            pltpu.VMEM((heads, width, 2 * width), f32),
            pltpu.VMEM((heads, width, width), bf),
            pltpu.VMEM((heads, width, width), bf),
            pltpu.VMEM((heads, width, width), f32),
            pltpu.VMEM((length, heads * width), bf),
            dma((13,)),
            dma((5,)),
            dma((4 + CUTS,)),
            dma((3 + CUTS,)),
            dma((3,)),
            dma,
            dma,
            dma,
            dma((CUTS,)),
            dma((3,)),
            dma((3,)),
            dma((3,)),
            dma((2,)),
            dma,
            dma,
            dma,
            dma,
            dma,
            dma((line,)),
            dma,
            dma,
            dma((line,)),
            dma,
            dma,
            dma,
            dma,
            dma,
            pltpu.SemaphoreType.REGULAR,
            pltpu.SemaphoreType.REGULAR,
            pltpu.VMEM((tokens, model), bf),
            pltpu.VMEM((tokens, model), bf),
        ],
        compiler_params=pltpu.CompilerParams(
            collective_id=0, has_side_effects=True, vmem_limit_bytes=62 << 20
        ),
    )(
        decay_gate_logits.T,
        correction_logits.T,
        head_decay_speed.reshape(1, heads),
        position_log_decay.T,
        head_output_gain.reshape(1, width),
        expert_norm_gain.reshape(1, model),
        routes.T,
        chosen_expert_weight.T,
        queries,
        keys,
        values,
        expert_input_tokens,
        mixer_output_weight,
        routed_gate_weight[0],
        routed_up_weight[0],
        routed_down_weight[0],
        common_gate_weight,
        common_up_weight,
        common_down_weight.reshape(devices, shared_unit // devices, model),
    )
    return pl.pallas_call(
        hand_over,
        in_specs=[anywhere] * 2,
        out_specs=[anywhere] * 2,
        out_shape=[jax.ShapeDtypeStruct((tokens, model), bf)] * 2,
        scratch_shapes=[pltpu.VMEM((8, tokens // 4, model), bf), dma((8,)), dma((8,))],
    )(mixed, routed)


def shards(*args):
    devices, members = lax.axis_size("ep"), lax.axis_size("tp")
    routes, tokens = args[11], args[9]
    capacity = 3 * routes.shape[0] * routes.shape[1] // (2 * devices)
    whole_tiles = capacity % 16 == 0 and tokens.shape[1] % (128 * CUTS) == 0
    whole_tiles = whole_tiles and args[16].shape[1] % (16 * devices) == 0
    whole_tiles = whole_tiles and args[16].shape[1] == args[13].shape[2]
    whole_tiles = whole_tiles and args[13].shape[2] % 256 == 0
    if members == 4 and devices % 4 == 0 and whole_tiles:
        return fused_shards(*args)
    return plain_shards(*args)


def solution(mesh):
    return jax.shard_map(
        shards,
        mesh=mesh,
        in_specs=(
            P("ep", "tp"),
            P("ep", "tp"),
            P("ep", "tp"),
            P("ep", "tp"),
            P("ep", "tp"),
            P("tp"),
            P("ep", "tp"),
            P(),
            P("tp", None),
            P(("ep", "tp"), None),
            P(),
            P(("ep", "tp"), None),
            P(("ep", "tp"), None),
            P("ep", None, "tp"),
            P("ep", None, "tp"),
            P("ep", "tp", None),
            P(None, "tp"),
            P(None, "tp"),
            P("tp", None),
        ),
        out_specs=(P(("ep", "tp"), None), P(("ep", "tp"), None)),
        check_vma=False,
    )
```

```python
import functools

import jax
import jax.numpy as jnp
from jax import lax
from jax.experimental import pallas as pl
from jax.experimental.pallas import tpu as pltpu
from jax.sharding import PartitionSpec as P


EPS = 1e-06


SPAN = 64


def halves(x):
    high = x.astype(jnp.bfloat16)
    return high, (x - high.astype(jnp.float32)).astype(jnp.bfloat16)


def product(left, right, numbers):
    left_high, left_low = halves(left)
    right_high, right_low = halves(right)

    def dot(x, y):
        return lax.dot_general(x, y, numbers, preferred_element_type=jnp.float32)

    return dot(left_high, right_high) + (dot(left_high, right_low) + dot(left_low, right_high))


def bmm(left, right, dims):
    return product(left, right, (dims, ((0,), (0,))))


def mm(left, right):
    return product(left, right, (((1,), (0,)), ((), ())))


def unit_lower_inverse(lower, rows, cols):
    inverse = jnp.where(rows == cols, 1.0, 0.0) - jnp.where(
        ((rows >> 1) == (cols >> 1)), lower, 0.0
    )
    level = 1
    while (1 << level) < SPAN:
        below = ((rows >> (level + 1)) == (cols >> (level + 1))) & (
            (rows >> level) != (cols >> level)
        )
        part = jnp.where(below, lower, 0.0)
        inverse = inverse - bmm(bmm(inverse, part, ((2,), (1,))), inverse, ((2,), (1,)))
        level += 1
    return inverse


def local_kernel(q_ref, k_ref, v_ref, ccol_ref, crow_ref, bcol_ref, g_ref, z_ref, total_ref):
    width = q_ref.shape[1]
    count = q_ref.shape[0] // SPAN
    shape = (count, SPAN, width)
    q = q_ref[...].astype(jnp.float32)
    k = k_ref[...].astype(jnp.float32)
    v = v_ref[...].astype(jnp.float32).reshape(shape)
    q = q * lax.rsqrt(jnp.sum(q * q, axis=-1, keepdims=True) + EPS) * width ** (-0.5)
    k = k * lax.rsqrt(jnp.sum(k * k, axis=-1, keepdims=True) + EPS)
    q = q.reshape(shape)
    k = k.reshape(shape)
    ccol = ccol_ref[0].reshape(count, SPAN, 1)
    crow = crow_ref[0]
    bcol = bcol_ref[0].reshape(count, SPAN, 1)
    rows = lax.broadcasted_iota(jnp.int32, (count, SPAN, SPAN), 1)
    cols = lax.broadcasted_iota(jnp.int32, (count, SPAN, SPAN), 2)
    decay = jnp.exp(jnp.where(rows >= cols, ccol - crow, -jnp.inf))
    keyed = k * bcol
    lower = jnp.where(rows > cols, bmm(keyed, k, ((2,), (2,))) * decay, 0.0)
    inverse = unit_lower_inverse(lower, rows, cols)
    grown = jnp.exp(ccol)
    solved = bmm(
        inverse, jnp.concatenate([keyed * grown, v * bcol], axis=-1), ((2,), (1,))
    )
    scores = bmm(q, k, ((2,), (2,))) * decay
    q_scaled = q * grown
    last = ccol[:, SPAN - 1 :, :]
    carried = k * jnp.exp(last - ccol)
    mixed = bmm(scores, solved, ((2,), (1,)))
    readout = q_scaled - mixed[:, :, :width]
    eye_r = lax.broadcasted_iota(jnp.int32, (width, width), 0)
    eye_c = lax.broadcasted_iota(jnp.int32, (width, width), 1)
    eye = jnp.where(eye_r == eye_c, 1.0, 0.0)
    state = jnp.concatenate([eye, jnp.zeros_like(eye)], axis=1)
    for n in range(count):
        seen = mm(readout[n], state)
        g_ref[0, n * SPAN : (n + 1) * SPAN, :] = seen[:, :width]
        z_ref[0, n * SPAN : (n + 1) * SPAN, :] = seen[:, width:] + mixed[n][:, width:]
        both = mm(carried[n].T, solved[n])
        trans = jnp.exp(last[n]) * eye - both[:, :width]
        state = mm(trans, state)
        state = jnp.concatenate([state[:, :width], state[:, width:] + both[:, width:]], axis=1)
    total_ref[0] = state.astype(jnp.bfloat16)


def finish_kernel(place_ref, gathered_ref, g_ref, z_ref, gain_ref, out_ref):
    width = g_ref.shape[2]

    def one(turn, state):
        both = gathered_ref[turn, 0].astype(jnp.float32)
        return mm(both[:, :width], state) + both[:, width:]

    state = lax.fori_loop(0, place_ref[0], one, jnp.zeros((width, width), jnp.float32))
    out = mm(g_ref[0], state) + z_ref[0]
    out = out * lax.rsqrt(jnp.mean(out * out, axis=-1, keepdims=True) + EPS) * gain_ref[...]
    out_ref[...] = out.astype(jnp.bfloat16)


def token_mixer_heads(
    queries,
    keys,
    values,
    decay_gate_logits,
    correction_logits,
    head_decay_speed,
    position_log_decay,
    head_output_gain,
):
    heads = decay_gate_logits.shape[1]
    length = queries.shape[0]
    width = queries.shape[1] // heads
    count = length // SPAN
    log_gate = -head_decay_speed * jax.nn.softplus(decay_gate_logits) + position_log_decay
    log_gate = log_gate.T.reshape(heads, count, SPAN)
    at = jnp.arange(SPAN)
    cum = jnp.sum(
        jnp.where(at[:, None] >= at[None, :], log_gate[:, :, None, :], 0.0), axis=-1
    )
    beta = jax.nn.sigmoid(correction_logits.astype(jnp.float32)).T.reshape(heads, length, 1)
    by_head = pl.BlockSpec((length, width), lambda h: (0, h))
    column = pl.BlockSpec((1, length, 1), lambda h: (h, 0, 0))
    whole = pl.BlockSpec((1, length, width), lambda h: (h, 0, 0))
    local_call = pl.pallas_call(
        local_kernel,
        grid=(heads,),
        in_specs=[
            by_head,
            by_head,
            by_head,
            column,
            pl.BlockSpec((1, count, 1, SPAN), lambda h: (h, 0, 0, 0)),
            column,
        ],
        out_specs=[whole, whole, pl.BlockSpec((1, width, 2 * width), lambda h: (h, 0, 0))],
        out_shape=[
            jax.ShapeDtypeStruct((heads, length, width), jnp.float32),
            jax.ShapeDtypeStruct((heads, length, width), jnp.float32),
            jax.ShapeDtypeStruct((heads, width, 2 * width), jnp.bfloat16),
        ],
        cost_estimate=pl.CostEstimate(
            flops=3_000_000_000, bytes_accessed=4_000_000, transcendentals=200_000
        ),
    )
    readout, local_out, total = local_call(
        queries,
        keys,
        values,
        cum.reshape(heads, length, 1),
        cum.reshape(heads, count, 1, SPAN),
        beta,
    )
    gathered = lax.all_gather(total, "ep")
    place = lax.axis_index("ep").astype(jnp.int32).reshape(1)
    devices = gathered.shape[0]
    return pl.pallas_call(
        finish_kernel,
        grid=(heads,),
        in_specs=[
            pl.BlockSpec(memory_space=pltpu.SMEM),
            pl.BlockSpec((devices, 1, width, 2 * width), lambda h: (0, h, 0, 0)),
            whole,
            whole,
            pl.BlockSpec((1, width), lambda h: (0, 0)),
        ],
        out_specs=by_head,
        out_shape=jax.ShapeDtypeStruct((length, heads * width), jnp.bfloat16),
        cost_estimate=pl.CostEstimate(
            flops=500_000_000, bytes_accessed=4_000_000, transcendentals=2_000
        ),
    )(place, gathered, readout, local_out, head_output_gain.reshape(1, width))


def norm_rows(expert_input_tokens, expert_norm_gain):
    rows_f = expert_input_tokens.astype(jnp.float32)
    scaled = (
        rows_f
        * lax.rsqrt(jnp.mean(rows_f * rows_f, axis=-1, keepdims=True) + EPS)
        * expert_norm_gain
    )
    return scaled.astype(jnp.bfloat16)


def gated_hidden(rows_in, w_gate, w_up):
    gate_val = jnp.dot(rows_in, w_gate, preferred_element_type=jnp.float32)
    up_val = jnp.dot(rows_in, w_up, preferred_element_type=jnp.float32)
    return (jax.nn.silu(gate_val) * up_val).astype(jnp.bfloat16)


def slot_layout(routes, capacity):
    flat = routes.reshape(-1)
    at = jnp.arange(flat.shape[0], dtype=jnp.int32)
    same = (flat[:, None] == flat[None, :]) & (at[None, :] < at[:, None])
    before = jnp.sum(same.astype(jnp.int32), axis=1)
    return (flat * capacity + before).reshape(routes.shape)


def plain_shards(
    queries,
    keys,
    values,
    decay_gate_logits,
    correction_logits,
    head_decay_speed,
    position_log_decay,
    head_output_gain,
    mixer_output_weight,
    expert_input_tokens,
    expert_norm_gain,
    routes,
    chosen_expert_weight,
    routed_gate_weight,
    routed_up_weight,
    routed_down_weight,
    common_gate_weight,
    common_up_weight,
    common_down_weight,
):
    normed = token_mixer_heads(
        queries,
        keys,
        values,
        decay_gate_logits,
        correction_logits,
        head_decay_speed,
        position_log_decay,
        head_output_gain,
    )
    mixer_out = lax.psum_scatter(
        jnp.dot(normed, mixer_output_weight, preferred_element_type=jnp.float32).astype(
            jnp.bfloat16
        ),
        "tp",
        scatter_dimension=0,
        tiled=True,
    )
    normed_in = norm_rows(expert_input_tokens, expert_norm_gain)
    tokens_own, top_k = routes.shape
    model_width = expert_input_tokens.shape[1]
    experts = lax.axis_size("ep")
    capacity = 3 * tokens_own * top_k // (2 * experts)
    slot_count = experts * capacity
    slots = slot_layout(routes, capacity)
    numbers = jnp.arange(slot_count, dtype=jnp.int32)
    sends = sum(
        (slots[None, :, k] == numbers[:, None]).astype(jnp.bfloat16) for k in range(top_k)
    )
    outgoing = jnp.dot(sends, normed_in, preferred_element_type=jnp.float32).astype(
        jnp.bfloat16
    )
    arrived = lax.all_to_all(
        outgoing.reshape(experts, capacity, model_width),
        "ep",
        split_axis=0,
        concat_axis=0,
        tiled=True,
    ).reshape(slot_count, model_width)
    gate_all = lax.all_gather(routed_gate_weight[0], "tp")
    up_all = lax.all_gather(routed_up_weight[0], "tp")
    down_all = lax.all_gather(routed_down_weight[0], "tp", axis=0, tiled=True)
    hidden = jnp.concatenate(
        [gated_hidden(arrived, gate_all[t], up_all[t]) for t in range(gate_all.shape[0])],
        axis=1,
    )
    slot_sums = jnp.dot(hidden, down_all, preferred_element_type=jnp.float32).astype(
        jnp.bfloat16
    )
    returned = lax.all_to_all(
        slot_sums.reshape(experts, capacity, model_width),
        "ep",
        split_axis=0,
        concat_axis=0,
        tiled=True,
    ).reshape(slot_count, model_width)
    shared_hidden = gated_hidden(
        lax.all_gather(normed_in, "tp", axis=0, tiled=True), common_gate_weight, common_up_weight
    )
    shared = lax.psum_scatter(
        jnp.dot(shared_hidden, common_down_weight, preferred_element_type=jnp.float32).astype(
            jnp.bfloat16
        ),
        "tp",
        scatter_dimension=0,
        tiled=True,
    ).astype(jnp.float32)
    weights = sum(
        jnp.where(
            slots[:, k : k + 1] == numbers[None, :], chosen_expert_weight[:, k : k + 1], 0.0
        )
        for k in range(top_k)
    )
    coarse = weights.astype(jnp.bfloat16)
    fine = (weights - coarse.astype(jnp.float32)).astype(jnp.bfloat16)
    routed = jnp.dot(coarse, returned, preferred_element_type=jnp.float32) + jnp.dot(
        fine, returned, preferred_element_type=jnp.float32
    )
    moe_out = (shared + routed).astype(jnp.bfloat16)
    return (mixer_out, moe_out)


MESH = pl.DeviceIdType.MESH
CUTS = 8
OWN, CORE, CROSS, FAR = range(4)


def scaled_rows(rows, gain):
    rows_f = rows.astype(jnp.float32)
    norm = lax.rsqrt(jnp.mean(rows_f * rows_f, axis=-1, keepdims=True) + EPS)
    return (rows_f * norm * gain).astype(jnp.bfloat16)


def silu_product(gate_val, up_val):
    return (gate_val / (1.0 + jnp.exp(-gate_val)) * up_val).astype(jnp.bfloat16)


def fused_kernel(
    devices,
    decay_hbm,
    correct_hbm,
    speed_hbm,
    log_hbm,
    head_gain_hbm,
    gain_hbm,
    routes_hbm,
    chosen_hbm,
    q_hbm,
    k_hbm,
    v_hbm,
    tok_hbm,
    mixw_hbm,
    rg_hbm,
    ru_hbm,
    rd_hbm,
    cg_hbm,
    cu_hbm,
    cd_hbm,
    mix_ref,
    moe_ref,
    wg,
    wu,
    wd,
    cg,
    cu,
    dn,
    mw,
    q_ref,
    k_ref,
    v_ref,
    tok_ref,
    hits_ref,
    weight_ref,
    lrow_s,
    brow_s,
    decay_ref,
    correct_ref,
    speed_ref,
    log_ref,
    head_gain_ref,
    gain_ref,
    routes_ref,
    chosen_ref,
    thin_sem,
    toks,
    sh_hid,
    sh_in,
    outgoing,
    arrived,
    hid,
    slot_out,
    returned,
    shared,
    mx_part,
    mx_in,
    mx_cross,
    mx_far,
    ccol_s,
    crow_s,
    bcol_s,
    gs,
    zs,
    tot,
    tot_bf,
    pair_in,
    pair_tot,
    s_in,
    s_out,
    state_s,
    normed,
    local_sem,
    w_send,
    w_recv,
    p_recv,
    g_recv,
    d_send,
    d_recv,
    r_send,
    r_recv,
    rs_send,
    rs_recv,
    c_send,
    c_recv,
    sx_send,
    sx_recv,
    sc_send,
    sc_recv,
    z_send,
    z_recv,
    zf_send,
    y_send,
    y_recv,
    f_send,
    f_recv,
    h_send,
    h_recv,
    o_sem,
    here_sem,
    go_sem,
    mix_s,
    moe_s,
):
    e = lax.axis_index("ep")
    t = lax.axis_index("tp")
    heads = decay_ref.shape[0]
    width = q_ref.shape[1] // heads
    length = q_ref.shape[0]
    count = length // SPAN
    tokens, model = tok_ref.shape
    top_k = routes_ref.shape[0]
    capacity = arrived.shape[1]
    slots = devices * capacity
    unit = wg.shape[2]
    cut = model // CUTS
    core_t = t + 1 - 2 * (t % 2)
    core = (e, core_t)
    cross = (e, (t + 2) % 4)
    line = devices // 2
    half = line // 2
    z = e // 2
    y = e % 2
    inner = z % half
    mine = z - inner
    other = half - mine
    beside = (2 * z + 1 - y, t)

    def remote(src, dst, send, recv, peer):
        return pltpu.make_async_remote_copy(
            src_ref=src,
            dst_ref=dst,
            send_sem=send,
            recv_sem=recv,
            device_id=peer,
            device_id_type=MESH,
        )

    near = [
        2 * (mine + (inner + o) % half) + (y + d) % 2
        for o in range(half)
        for d in range(2)
        if (o, d) != (0, 0)
    ]
    distant = [
        2 * (other + (inner + o) % half) + (y + d) % 2 for o in range(half) for d in range(2)
    ]
    peers = distant + near

    early = [
        pltpu.make_async_copy(src, dst, local_sem.at[8 + n])
        for n, (src, dst) in enumerate(
            ((tok_hbm, tok_ref), (q_hbm, q_ref), (k_hbm, k_ref), (v_hbm, v_ref))
        )
    ]
    locals_ = [
        pltpu.make_async_copy(src, dst, local_sem.at[n])
        for n, (src, dst) in enumerate(
            (
                (cg_hbm, cg),
                (cu_hbm, cu),
                (cd_hbm, dn.at[OWN]),
                (rg_hbm, wg.at[OWN]),
                (ru_hbm, wu.at[OWN]),
                (rd_hbm, wd.at[OWN]),
                (mixw_hbm, mw),
            )
        )
    ]
    thin = [
        pltpu.make_async_copy(src, dst, thin_sem.at[n])
        for n, (src, dst) in enumerate(
            (
                (routes_hbm, routes_ref),
                (chosen_hbm, chosen_ref),
                (gain_hbm, gain_ref),
                (decay_hbm, decay_ref),
                (correct_hbm, correct_ref),
                (speed_hbm, speed_ref),
                (log_hbm, log_ref),
                (head_gain_hbm, head_gain_ref),
            )
        )
    ]

    barrier = pltpu.get_barrier_semaphore()
    speaker = t == 3
    for o in range(1, 4):
        member = (t + o) % 4

        @pl.when(member != 3)
        def _():
            pl.semaphore_signal(barrier, inc=1, device_id=(e, member), device_id_type=MESH)

    for copy in thin + early:
        copy.start()
    for copy in thin:
        copy.wait()

    expert = lax.broadcasted_iota(jnp.int32, (devices, tokens), 0)
    earlier = lax.broadcasted_iota(jnp.int32, (tokens, tokens), 0)
    earlier = jnp.where(
        earlier < lax.broadcasted_iota(jnp.int32, (tokens, tokens), 1), 1.0, 0.0
    ).astype(jnp.bfloat16)
    number = lax.broadcasted_iota(jnp.int32, (slots, tokens), 0).astype(jnp.float32)
    base = jnp.zeros((devices, 1), jnp.float32)
    sends = jnp.zeros((slots, tokens), jnp.bfloat16)
    token_a = lax.broadcasted_iota(jnp.int32, (tokens, tokens), 0)
    token_b = lax.broadcasted_iota(jnp.int32, (tokens, tokens), 1)
    for n in range(top_k):
        route = routes_ref[n : n + 1, :]
        chosen = jnp.where(expert == route, 1.0, 0.0)
        before = base + jnp.dot(
            chosen.astype(jnp.bfloat16), earlier, preferred_element_type=jnp.float32
        )
        base = base + jnp.sum(chosen, axis=1, keepdims=True)
        slot = route.astype(jnp.float32) * capacity + jnp.sum(
            chosen * before, axis=0, keepdims=True
        )
        hit = jnp.where(number == slot, 1.0, 0.0).astype(jnp.bfloat16)
        sends = sends + hit
        hits_ref[n] = hit
        weight_ref[n] = jnp.sum(
            jnp.where(token_a == token_b, chosen_ref[n : n + 1, :], 0.0), axis=1, keepdims=True
        )

    @pl.when(jnp.logical_not(speaker))
    def _():
        pl.semaphore_wait(barrier, 3)
        pl.semaphore_signal(here_sem, inc=1, device_id=(e, 3), device_id_type=MESH)

    @pl.when(speaker)
    def _():
        pl.semaphore_wait(here_sem, 3)
        for o in range(1, devices):
            pl.semaphore_signal(
                barrier, inc=1, device_id=((e + o) % devices, t), device_id_type=MESH
            )


    def cols(j):
        return pl.ds(pl.multiple_of(j * cut, cut), cut)

    def spread(n, i, src, place):
        remote(src, place(CROSS), w_send.at[n], w_recv.at[i], cross).start()
        remote(src, place(CORE), w_send.at[n], p_recv.at[i], core).start()

    def forward(n, i, place):
        remote(place(CROSS), place(CROSS), w_send.at[n], w_recv.at[i], cross).wait_recv()
        remote(place(CROSS), place(FAR), w_send.at[n], p_recv.at[i], core).start()

    def take(i, both):
        remote(both, both, w_send.at[0], p_recv.at[i], core).wait_recv()

    def sent(n, all_of):
        remote(all_of, all_of, w_send.at[n], w_recv.at[0], core).wait_send()

    def gate_at(r):
        return wg.at[r]

    def down_at(j):
        return lambda r: wd.at[r, :, cols(j)]

    slices = [remote(cd_hbm.at[e], dn.at[CROSS, e], sx_send, sx_recv, cross)]
    for copy in slices:
        copy.start()
    spread(0, 0, rg_hbm, gate_at)
    hu = unit // 2
    up_index = (1, 3 + CUTS)
    for n in range(2):
        at = pl.ds(n * hu, hu)
        remote(
            ru_hbm.at[:, at], wu.at[CROSS, :, at], w_send.at[1], w_recv.at[up_index[n]], cross
        ).start()
    remote(ru_hbm, wu.at[CORE], w_send.at[1], p_recv.at[1], core).start()

    def spread_down(j, carry):
        spread(2, 2 + j, rd_hbm.at[:, cols(j)], down_at(j))
        return carry

    ahead = 5 * CUTS // 8
    lax.fori_loop(0, ahead, spread_down, 0)
    remote(tok_hbm, toks.at[CROSS], w_send.at[3], w_recv.at[2 + CUTS], cross).start()
    remote(tok_hbm, toks.at[CORE], w_send.at[3], p_recv.at[2 + CUTS], core).start()
    lax.fori_loop(ahead, CUTS, spread_down, 0)
    shared_core = [remote(cd_hbm, dn.at[CORE], sc_send, sc_recv, core)]
    for copy in shared_core:
        copy.start()
    for copy in locals_:
        copy.start()

    early[0].wait()
    toks[OWN] = scaled_rows(tok_ref[...], gain_ref[...])
    outgoing[...] = (
        jnp.dot(sends, toks[OWN], preferred_element_type=jnp.float32)
        .astype(jnp.bfloat16)
        .reshape(outgoing.shape)
    )

    rows = lax.broadcasted_iota(jnp.int32, (count, SPAN, SPAN), 1)
    cols_at = lax.broadcasted_iota(jnp.int32, (count, SPAN, SPAN), 2)
    for h in range(heads):
        logit = decay_ref[h : h + 1, :]
        softplus = jnp.maximum(logit, 0.0) + jnp.log1p(jnp.exp(-jnp.abs(logit)))
        log_gate = -speed_ref[0:1, h : h + 1] * softplus + log_ref[h : h + 1, :]
        beta = 1.0 / (1.0 + jnp.exp(-correct_ref[h : h + 1, :].astype(jnp.float32)))
        for n in range(count):
            lrow_s[n] = log_gate[:, n * SPAN : (n + 1) * SPAN]
            brow_s[n] = beta[:, n * SPAN : (n + 1) * SPAN]
        ccol = jnp.sum(jnp.where(rows >= cols_at, lrow_s[...], 0.0), axis=2, keepdims=True)
        ccol_s[h] = ccol
        crow_s[h] = jnp.sum(jnp.where(rows == cols_at, ccol, 0.0), axis=1, keepdims=True)
        bcol_s[h] = jnp.sum(
            jnp.where(rows == cols_at, brow_s[...], 0.0), axis=2, keepdims=True
        )

    def dispatch(n):
        peer = peers[n]
        return remote(outgoing.at[peer], arrived.at[e], d_send, d_recv, (peer, t))

    @pl.when(speaker)
    def _():
        pl.semaphore_wait(barrier, devices - 1)
        for o in range(3):
            pl.semaphore_signal(go_sem, inc=1, device_id=(e, o), device_id_type=MESH)

    @pl.when(jnp.logical_not(speaker))
    def _():
        pl.semaphore_wait(go_sem, 1)

    for n in range(len(peers)):
        dispatch(n).start()
    own_rows = pltpu.make_async_copy(outgoing.at[e], arrived.at[e], d_recv)
    own_rows.start()

    def local_head(h, carry):
        at = pl.ds(pl.multiple_of(h * width, width), width)
        shape = (count, SPAN, width)
        q = q_ref[:, at].astype(jnp.float32)
        k = k_ref[:, at].astype(jnp.float32)
        v = v_ref[:, at].astype(jnp.float32).reshape(shape)
        q = q * lax.rsqrt(jnp.sum(q * q, axis=-1, keepdims=True) + EPS) * width ** (-0.5)
        k = k * lax.rsqrt(jnp.sum(k * k, axis=-1, keepdims=True) + EPS)
        q = q.reshape(shape)
        k = k.reshape(shape)
        ccol = ccol_s[h]
        crow = crow_s[h]
        bcol = bcol_s[h]
        decay = jnp.exp(jnp.where(rows >= cols_at, ccol - crow, -jnp.inf))
        keyed = k * bcol
        lower = jnp.where(rows > cols_at, bmm(keyed, k, ((2,), (2,))) * decay, 0.0)
        inverse = unit_lower_inverse(lower, rows, cols_at)
        grown = jnp.exp(ccol)
        solved = bmm(
            inverse, jnp.concatenate([keyed * grown, v * bcol], axis=-1), ((2,), (1,))
        )
        scores = bmm(q, k, ((2,), (2,))) * decay
        q_scaled = q * grown
        last = ccol[:, SPAN - 1 :, :]
        carried = k * jnp.exp(last - ccol)
        mixed = bmm(scores, solved, ((2,), (1,)))
        readout = q_scaled - mixed[:, :, :width]
        eye_r = lax.broadcasted_iota(jnp.int32, (width, width), 0)
        eye_c = lax.broadcasted_iota(jnp.int32, (width, width), 1)
        eye = jnp.where(eye_r == eye_c, 1.0, 0.0)
        state = jnp.concatenate([eye, jnp.zeros_like(eye)], axis=1)
        for n in range(count):
            seen = mm(readout[n], state)
            gs[h, n * SPAN : (n + 1) * SPAN, :] = seen[:, :width]
            zs[h, n * SPAN : (n + 1) * SPAN, :] = seen[:, width:] + mixed[n][:, width:]
            both = mm(carried[n].T, solved[n])
            trans = jnp.exp(last[n]) * eye - both[:, :width]
            state = mm(trans, state)
            state = jnp.concatenate([state[:, :width], state[:, width:] + both[:, width:]], axis=1)
        tot[h] = state
        tot_bf[h] = state.astype(jnp.bfloat16)
        return carry

    for copy in early[1:]:
        copy.wait()
    lax.fori_loop(0, heads, local_head, 0)

    def piece(i, r, send, recv, peer):
        return [remote(dn.at[CROSS, i], dn.at[r, i], send, recv, peer)]

    def along(at, place):
        i = 2 * at + y
        return piece(i, CROSS, z_send, z_recv.at[at], (2 * place + y, t))

    def hand_on(o, at):
        place = mine + (inner + o) % half
        return piece(
            2 * at + y,
            CROSS,
            zf_send,
            z_recv.at[at],
            (2 * place + y, t),
        )

    def aside(at):
        return piece(2 * at + y, CROSS, y_send, y_recv.at[at], beside)

    def to_core(i):
        return piece(i, FAR, f_send, f_recv, core)

    def share(at):
        for copy in aside(at) + to_core(2 * at + y):
            copy.start()

    half_places = [mine + (inner + o) % half for o in range(half)]
    far_places = [other + (inner + o) % half for o in range(half)]
    middle = half - z // half
    is_middle = jnp.logical_or(z == half - 1, z == half)

    def line_copies():
        copies = along(z, middle)
        for o in range(1, half):
            copies += along(z, half_places[o])
        return copies

    pair = z
    to_odd = remote(tot_bf, pair_in, c_send.at[0], c_recv.at[0], beside)
    next_odd = ((e + 2) % devices, t)
    next_even = ((e + 1) % devices, t)
    hands_on = jnp.logical_and(y == 1, pair < line - 1)
    to_next_odd = remote(s_out, s_in, c_send.at[1], c_recv.at[1], next_odd)
    to_next_even = remote(s_out, s_in, c_send.at[2], c_recv.at[1], next_even)

    @pl.when(y == 0)
    def _():
        to_odd.start()

    @pl.when(y == 1)
    def _():
        to_odd.wait_recv()
        for h in range(heads):
            both = mm(tot[h][:, :width], pair_in[h].astype(jnp.float32))
            pair_tot[h, :, :width] = both[:, :width]
            pair_tot[h, :, width:] = both[:, width:] + tot[h][:, width:]

    @pl.when(pair == 0)
    def _():
        s_in[...] = jnp.zeros_like(s_in)

    @pl.when(jnp.logical_and(hands_on, pair == 0))
    def _():
        s_out[...] = pair_tot[:, :, width:].astype(jnp.bfloat16)
        to_next_odd.start()
        to_next_even.start()

    for copy in slices:
        copy.wait_recv()
    share(z)

    for copy in line_copies():
        copy.start()

    remote(wg.at[CROSS], wg.at[CROSS], w_send.at[0], w_recv.at[0], cross).wait_recv()
    remote(wg.at[CROSS], wg.at[FAR], w_send.at[0], g_recv.at[0], core).start()
    for n in range(3, 6):
        locals_[n].wait()
    take(0, wg.at[CORE])
    take(1, wu.at[CORE])

    remote(arrived, arrived, d_send, d_recv, core).wait_recv()

    def hidden_of(r, carry):
        rows_in = arrived[...].reshape(slots, model)
        hid[r] = silu_product(
            jnp.dot(rows_in, wg[r], preferred_element_type=jnp.float32),
            jnp.dot(rows_in, wu[r], preferred_element_type=jnp.float32),
        )
        return carry

    lax.fori_loop(OWN, CORE + 1, hidden_of, 0)

    def hidden_half(n):
        at = slice(n * hu, (n + 1) * hu)
        rows_in = arrived[...].reshape(slots, model)
        value = silu_product(
            *(
                jnp.dot(
                    rows_in,
                    jnp.concatenate([bank[CROSS, :, at], bank[FAR, :, at]], axis=1),
                    preferred_element_type=jnp.float32,
                )
                for bank in (wg, wu)
            )
        )
        hid[CROSS, :, at] = value[:, :hu]
        hid[FAR, :, at] = value[:, hu:]

    def far_half(n):
        at = pl.ds(n * hu, hu)
        there, here = wu.at[CROSS, :, at], wu.at[FAR, :, at]
        remote(there, there, w_send.at[1], w_recv.at[up_index[n]], cross).wait_recv()
        remote(there, here, w_send.at[1], g_recv.at[1 + n], core).start()
        if n == 0:
            remote(wg.at[FAR], wg.at[FAR], w_send.at[0], g_recv.at[0], core).wait_recv()
        remote(here, here, w_send.at[1], g_recv.at[1 + n], core).wait_recv()
        hidden_half(n)

    far_half(0)

    @pl.when(jnp.logical_and(hands_on, pair > 0))
    def _():
        to_next_odd.wait_recv()
        for h in range(heads):
            s_out[h] = (
                mm(pair_tot[h][:, :width], s_in[h].astype(jnp.float32)) + pair_tot[h][:, width:]
            ).astype(jnp.bfloat16)
        to_next_odd.start()
        to_next_even.start()

    def line_wait(at):
        for copy in along(at, z):
            copy.wait_recv()

    for o in range(1, half):
        line_wait(half_places[o])
        share(half_places[o])

    @pl.when(is_middle)
    def _():
        for n in range(half):
            line_wait(far_places[n])
            for o in range(1, half):
                for copy in hand_on(o, far_places[n]):
                    copy.start()
            share(far_places[n])

    far_half(1)

    def return_of(n, j):
        peer = peers[n]
        return remote(
            slot_out.at[peer, :, cols(j)],
            returned.at[e, :, cols(j)],
            r_send,
            r_recv.at[j],
            (peer, t),
        )

    def own_return(j):
        return pltpu.make_async_copy(
            slot_out.at[e, :, cols(j)], returned.at[e, :, cols(j)], r_recv.at[j]
        )

    def down_of(j, carry):
        place = down_at(j)
        forward(2, 2 + j, place)
        take(2 + j, wd.at[pl.ds(0, 2), :, cols(j)])
        hidden = jnp.concatenate([hid[r] for r in range(4)], axis=1)
        weight = wd[:, :, cols(j)].reshape(4 * unit, cut)
        slot_out[:, :, cols(j)] = (
            jnp.dot(hidden, weight, preferred_element_type=jnp.float32)
            .astype(jnp.bfloat16)
            .reshape(devices, capacity, cut)
        )
        for n in range(len(peers)):
            return_of(n, j).start()
        own_return(j).start()
        return carry

    lax.fori_loop(0 * CUTS // 8, 2 * CUTS // 8, down_of, 0)
    lax.fori_loop(2 * CUTS // 8, ahead, down_of, 0)

    @pl.when(jnp.logical_and(jnp.logical_not(hands_on), pair > 0))
    def _():
        to_next_odd.wait_recv()

    @pl.when(y == 1)
    def _():
        for h in range(heads):
            state_s[h] = mm(
                pair_in[h][:, :width].astype(jnp.float32), s_in[h].astype(jnp.float32)
            ) + pair_in[h][:, width:].astype(jnp.float32)

    @pl.when(y == 0)
    def _():
        state_s[...] = s_in[...].astype(jnp.float32)

    for h in range(heads):
        out = mm(gs[h], state_s[h]) + zs[h]
        out = out * lax.rsqrt(jnp.mean(out * out, axis=-1, keepdims=True) + EPS)
        normed[:, h * width : (h + 1) * width] = (out * head_gain_ref[...]).astype(jnp.bfloat16)
    locals_[6].wait()
    for r, owner in enumerate((t, core_t, (t + 2) % 4, (core_t + 2) % 4)):
        block = pl.ds(pl.multiple_of(owner * tokens, tokens), tokens)
        mx_part[r] = jnp.dot(
            normed[block, :], mw[...], preferred_element_type=jnp.float32
        ).astype(jnp.bfloat16)
    to_peer = [
        remote(mx_part.at[r], mx_in.at[1 - i], rs_send.at[i], rs_recv.at[i], core)
        for i, r in enumerate((FAR, CORE))
    ]
    for copy in to_peer:
        copy.start()

    @pl.when(jnp.logical_not(is_middle))
    def _():
        for n in range(half):
            line_wait(far_places[n])
            share(far_places[n])

    remote(tok_hbm, toks.at[CROSS], w_send.at[3], w_recv.at[2 + CUTS], cross).wait_recv()
    toks_on = remote(toks.at[CROSS], toks.at[FAR], w_send.at[4], p_recv.at[2 + CUTS], core)
    toks_on.start()
    for n in range(2):
        locals_[n].wait()
    take(2 + CUTS, toks.at[pl.ds(0, 2)])
    toks_on.wait_send()
    gain = gain_ref[...]
    for r in (CORE, CROSS, FAR):
        toks[r] = scaled_rows(toks[r], gain)
    x_all = toks[...].reshape(4 * tokens, model)
    sh_hid[...] = silu_product(
        jnp.dot(x_all, cg[...], preferred_element_type=jnp.float32),
        jnp.dot(x_all, cu[...], preferred_element_type=jnp.float32),
    ).reshape(sh_hid.shape)
    hidden_out = [
        remote(sh_hid.at[r], sh_in.at[r], h_send, h_recv, peer)
        for r, peer in ((CORE, core), (CROSS, cross), (FAR, (e, (core_t + 2) % 4)))
    ]
    for copy in hidden_out:
        copy.start()

    to_peer[0].wait_recv()
    mx_cross[...] = (mx_part[CROSS].astype(jnp.float32) + mx_in[1].astype(jnp.float32)).astype(
        jnp.bfloat16
    )
    over = remote(mx_cross, mx_far, rs_send.at[2], rs_recv.at[2], cross)
    over.start()
    for at in range(line):
        for copy in piece(2 * at + 1 - y, CROSS, y_send, y_recv.at[at], beside):
            copy.wait_recv()
        for copy in to_core(2 * at + 1 - y):
            copy.start()
    lax.fori_loop(ahead, CUTS, down_of, 0)

    def moe_out(j):
        return pltpu.make_async_copy(moe_s.at[:, cols(j)], moe_ref.at[:, cols(j)], o_sem)

    mix_out = pltpu.make_async_copy(mix_s, mix_ref, local_sem.at[12])

    def combine(j, carry):
        whole = returned.at[:, :, cols(j)]
        remote(whole, whole, r_send, r_recv.at[j], core).wait_recv()
        back = returned[:, :, cols(j)].reshape(slots, cut)
        routed = sum(
            weight_ref[n]
            * lax.dot_general(
                hits_ref[n], back, (((0,), (0,)), ((), ())), preferred_element_type=jnp.float32
            )
            for n in range(top_k)
        )
        moe_s[:, cols(j)] = (shared[:, cols(j)] + routed).astype(jnp.bfloat16)
        moe_out(j).start()
        return carry

    locals_[2].wait()
    shared_core[0].wait_recv()
    remote(dn.at[FAR], dn.at[FAR], f_send, f_recv, core).wait_recv()
    others = sh_in.at[pl.ds(CORE, 3)]
    remote(others, others, h_send, h_recv, core).wait_recv()
    sh_in[OWN] = sh_hid[OWN]
    shared[...] = jnp.dot(
        jnp.concatenate([sh_in[r] for r in range(4)], axis=1),
        dn[...].reshape(4 * dn.shape[1] * dn.shape[2], model),
        preferred_element_type=jnp.float32,
    )

    lax.fori_loop(0, CUTS, combine, 0)
    to_peer[1].wait_recv()
    over.wait_recv()
    mix_s[...] = (
        mx_part[OWN].astype(jnp.float32)
        + mx_in[0].astype(jnp.float32)
        + mx_far[...].astype(jnp.float32)
    ).astype(jnp.bfloat16)
    mix_out.start()

    def gone(all_of, semaphore):
        remote(all_of, all_of, semaphore, d_recv, core).wait_send()

    sent(0, wg.at[pl.ds(0, 3)])
    sent(1, wu.at[pl.ds(0, 3)])
    sent(2, wd.at[pl.ds(0, 3)])
    sent(3, toks.at[pl.ds(0, 2)])
    gone(arrived.at[pl.ds(1, devices - 1)], d_send)
    gone(slot_out.at[pl.ds(1, devices - 1)], r_send)
    gone(dn.at[FAR, pl.ds(0, half)], z_send)
    gone(dn.at[FAR, pl.ds(0, line)], y_send)
    gone(dn.at[FAR], f_send)
    gone(sh_in.at[pl.ds(CORE, 3)], h_send)
    for copy in slices + shared_core + to_peer + [over]:
        copy.wait_send()
    pltpu.make_async_copy(moe_s, moe_ref, o_sem).wait()
    mix_out.wait()

    @pl.when(is_middle)
    def _():
        gone(dn.at[FAR, pl.ds(0, half * (half - 1))], zf_send)

    @pl.when(y == 0)
    def _():
        to_odd.wait_send()

    @pl.when(hands_on)
    def _():
        to_next_odd.wait_send()
        to_next_even.wait_send()


def hand_over(mixed_hbm, routed_hbm, mixer_out_hbm, moe_out_hbm, held, in_sem, out_sem):
    pieces, rows = held.shape[0], held.shape[1]
    each = pieces // 2
    ins, outs = [], []
    for n in range(pieces):
        src, dst = ((mixed_hbm, mixer_out_hbm), (routed_hbm, moe_out_hbm))[n // each]
        at = pl.ds(n % each * rows, rows)
        ins.append(pltpu.make_async_copy(src.at[at], held.at[n], in_sem.at[n]))
        outs.append(pltpu.make_async_copy(held.at[n], dst.at[at], out_sem.at[n]))
    for copy in ins:
        copy.start()
    for taken, given in zip(ins, outs):
        taken.wait()
        given.start()
    for copy in outs:
        copy.wait()


def fused_shards(
    queries,
    keys,
    values,
    decay_gate_logits,
    correction_logits,
    head_decay_speed,
    position_log_decay,
    head_output_gain,
    mixer_output_weight,
    expert_input_tokens,
    expert_norm_gain,
    routes,
    chosen_expert_weight,
    routed_gate_weight,
    routed_up_weight,
    routed_down_weight,
    common_gate_weight,
    common_up_weight,
    common_down_weight,
):
    devices = lax.axis_size("ep")
    tokens, top_k = routes.shape
    model = expert_input_tokens.shape[1]
    length = queries.shape[0]
    heads = decay_gate_logits.shape[1]
    width = queries.shape[1] // heads
    count = length // SPAN
    unit = routed_gate_weight.shape[2]
    shared_unit = common_gate_weight.shape[1]
    capacity = 3 * tokens * top_k // (2 * devices)
    slot_count = devices * capacity
    bf, f32 = jnp.bfloat16, jnp.float32
    anywhere = pl.BlockSpec(memory_space=pl.ANY)
    dma = pltpu.SemaphoreType.DMA
    line = devices // 2
    slot_shape = (devices, capacity, model)
    mixed, routed = pl.pallas_call(
        functools.partial(fused_kernel, devices),
        in_specs=[anywhere] * 19,
        out_specs=[anywhere, anywhere],
        out_shape=[jax.ShapeDtypeStruct((tokens, model), bf)] * 2,
        scratch_shapes=[
            pltpu.VMEM((4, model, unit), bf),
            pltpu.VMEM((4, model, unit), bf),
            pltpu.VMEM((4, unit, model), bf),
            pltpu.VMEM(common_gate_weight.shape, bf),
            pltpu.VMEM(common_up_weight.shape, bf),
            pltpu.VMEM((4, devices, shared_unit // devices, model), bf),
            pltpu.VMEM(mixer_output_weight.shape, bf),
            pltpu.VMEM(queries.shape, bf),
            pltpu.VMEM(queries.shape, bf),
            pltpu.VMEM(queries.shape, bf),
            pltpu.VMEM((tokens, model), bf),
            pltpu.VMEM((top_k, slot_count, tokens), bf),
            pltpu.VMEM((top_k, tokens, 1), f32),
            pltpu.VMEM((count, 1, SPAN), f32),
            pltpu.VMEM((count, 1, SPAN), f32),
            pltpu.VMEM((heads, length), f32),
            pltpu.VMEM((heads, length), correction_logits.dtype),
            pltpu.VMEM((1, heads), f32),
            pltpu.VMEM((heads, length), f32),
            pltpu.VMEM((1, width), f32),
            pltpu.VMEM((1, model), f32),
            pltpu.VMEM((top_k, tokens), routes.dtype),
            pltpu.VMEM((top_k, tokens), f32),
            dma((8,)),
            pltpu.VMEM((4, tokens, model), bf),
            pltpu.VMEM((4, tokens, shared_unit), bf),
            pltpu.VMEM((4, tokens, shared_unit), bf),
            pltpu.VMEM(slot_shape, bf),
            pltpu.VMEM(slot_shape, bf),
            pltpu.VMEM((4, slot_count, unit), bf),
            pltpu.VMEM(slot_shape, bf),
            pltpu.VMEM(slot_shape, bf),
            pltpu.VMEM((tokens, model), f32),
            pltpu.VMEM((4, tokens, model), bf),
            pltpu.VMEM((2, tokens, model), bf),
            pltpu.VMEM((tokens, model), bf),
            pltpu.VMEM((tokens, model), bf),
            pltpu.VMEM((heads, count, SPAN, 1), f32),
            pltpu.VMEM((heads, count, 1, SPAN), f32),
            pltpu.VMEM((heads, count, SPAN, 1), f32),
            pltpu.VMEM((heads, length, width), f32),
            pltpu.VMEM((heads, length, width), f32),
            pltpu.VMEM((heads, width, 2 * width), f32),
            pltpu.VMEM((heads, width, 2 * width), bf),
            pltpu.VMEM((heads, width, 2 * width), bf),
            pltpu.VMEM((heads, width, 2 * width), f32),
            pltpu.VMEM((heads, width, width), bf),
            pltpu.VMEM((heads, width, width), bf),
            pltpu.VMEM((heads, width, width), f32),
            pltpu.VMEM((length, heads * width), bf),
            dma((13,)),
            dma((5,)),
            dma((4 + CUTS,)),
            dma((3 + CUTS,)),
            dma((3,)),
            dma,
            dma,
            dma,
            dma((CUTS,)),
            dma((3,)),
            dma((3,)),
            dma((3,)),
            dma((2,)),
            dma,
            dma,
            dma,
            dma,
            dma,
            dma((line,)),
            dma,
            dma,
            dma((line,)),
            dma,
            dma,
            dma,
            dma,
            dma,
            pltpu.SemaphoreType.REGULAR,
            pltpu.SemaphoreType.REGULAR,
            pltpu.VMEM((tokens, model), bf),
            pltpu.VMEM((tokens, model), bf),
        ],
        compiler_params=pltpu.CompilerParams(
            collective_id=0, has_side_effects=True, vmem_limit_bytes=62 << 20
        ),
    )(
        decay_gate_logits.T,
        correction_logits.T,
        head_decay_speed.reshape(1, heads),
        position_log_decay.T,
        head_output_gain.reshape(1, width),
        expert_norm_gain.reshape(1, model),
        routes.T,
        chosen_expert_weight.T,
        queries,
        keys,
        values,
        expert_input_tokens,
        mixer_output_weight,
        routed_gate_weight[0],
        routed_up_weight[0],
        routed_down_weight[0],
        common_gate_weight,
        common_up_weight,
        common_down_weight.reshape(devices, shared_unit // devices, model),
    )
    return pl.pallas_call(
        hand_over,
        in_specs=[anywhere] * 2,
        out_specs=[anywhere] * 2,
        out_shape=[jax.ShapeDtypeStruct((tokens, model), bf)] * 2,
        scratch_shapes=[pltpu.VMEM((8, tokens // 4, model), bf), dma((8,)), dma((8,))],
    )(mixed, routed)


def shards(*args):
    devices, members = lax.axis_size("ep"), lax.axis_size("tp")
    routes, tokens = args[11], args[9]
    capacity = 3 * routes.shape[0] * routes.shape[1] // (2 * devices)
    whole_tiles = capacity % 16 == 0 and tokens.shape[1] % (128 * CUTS) == 0
    whole_tiles = whole_tiles and args[16].shape[1] % (16 * devices) == 0
    whole_tiles = whole_tiles and args[16].shape[1] == args[13].shape[2]
    whole_tiles = whole_tiles and args[13].shape[2] % 256 == 0
    if members == 4 and devices % 4 == 0 and whole_tiles:
        return fused_shards(*args)
    return plain_shards(*args)


def solution(mesh):
    return jax.shard_map(
        shards,
        mesh=mesh,
        in_specs=(
            P("ep", "tp"),
            P("ep", "tp"),
            P("ep", "tp"),
            P("ep", "tp"),
            P("ep", "tp"),
            P("tp"),
            P("ep", "tp"),
            P(),
            P("tp", None),
            P(("ep", "tp"), None),
            P(),
            P(("ep", "tp"), None),
            P(("ep", "tp"), None),
            P("ep", None, "tp"),
            P("ep", None, "tp"),
            P("ep", "tp", None),
            P(None, "tp"),
            P(None, "tp"),
            P("tp", None),
        ),
        out_specs=(P(("ep", "tp"), None), P(("ep", "tp"), None)),
        check_vma=False,
    )
```
